128 devices in a mesh: kv: 16 (over z, y), tp: 8 (over x, core).
Axes of the slice: x: 4, y: 4, z: 4, core: 2. Of those that a mesh axis runs over, the one named last changes fastest.
Arguments:
- tokens: bfloat16 [512, 4096], P(None, ('kv', 'tp')), may hold values from -60 to 60
- past_state: float32 [512, 16, 128, 128], P('kv', 'tp'), may hold values from -4 to 4
- pre_gain: float32 [4096], replicated, may hold values from 0.1 to 1.9
- pre_gate: bfloat16 [4096, 11264], P(None, ('kv', 'tp')), may hold values from -0.09375 to 0.09375
- pre_up: bfloat16 [4096, 11264], P(None, ('kv', 'tp')), may hold values from -0.09375 to 0.09375
- pre_down: bfloat16 [11264, 4096], P(('kv', 'tp')), may hold values from -0.21875 to 0.21875
- mix_gain: float32 [4096], replicated, may hold values from 0.1 to 1.9
- query_weight: bfloat16 [4096, 2048], P('kv', 'tp'), may hold values from -0.09375 to 0.09375
- forget_weight: bfloat16 [4096, 2048], P('kv', 'tp'), may hold values from -0.09375 to 0.09375
- value_weight: bfloat16 [4096, 2048], P('kv', 'tp'), may hold values from -0.09375 to 0.09375
- output_gate_weight: bfloat16 [4096, 2048], P('kv', 'tp'), may hold values from -0.09375 to 0.09375
- forget_floor: float32 [2048], P('tp'), may hold values from 0.02 to 0.9
- head_gain: float32 [128], replicated, may hold values from 0.1 to 1.9
- proj_out: bfloat16 [2048, 4096], P('tp', 'kv'), may hold values from -0.125 to 0.125
- post_gain: float32 [4096], replicated, may hold values from 0.1 to 1.9
- post_gate: bfloat16 [4096, 11264], P(None, ('kv', 'tp')), may hold values from -0.09375 to 0.09375
- post_up: bfloat16 [4096, 11264], P(None, ('kv', 'tp')), may hold values from -0.09375 to 0.09375
- post_down: bfloat16 [11264, 4096], P(('kv', 'tp')), may hold values from -0.21875 to 0.21875
Outputs:
- result: bfloat16 [512, 4096], P(None, ('kv', 'tp'))
- new_state: float32 [512, 16, 128, 128], P('kv', 'tp')
The draws below stay inside these ranges and needn't reach their ends.
All inputs are finite; a program needn't handle non-finite values.
Results may differ from the reference program's by a relative error of at most 0.014.
Values may be sent and summed in bfloat16 or wider, within the bound.
No kernel may reach another device: no remote copies, remote signals or barrier semaphores. Data moves between devices by JAX's collectives and lax.ppermute only.
A program may use at most 128 MiB of HBM per device.

```python
import math
import jax
import jax.numpy as jnp
from jax import lax

D = 4096
FF = 11264
HEADS = 16
HEAD_DIM = 128
INNER = 2048
SEQS = 512
N_TP = 8


def draw_tokens(key, part):
    key_base = jax.random.fold_in(key, 11)
    key_rows = jax.random.fold_in(key, 12)
    key_cols = jax.random.fold_in(key, 13)
    column_pos = jnp.arange(D, dtype=jnp.float32) / D
    jitter = jax.random.uniform(key_cols, (1, D), jnp.float32, 0.7, 1.3)
    rising = 0.5 * jnp.exp(column_pos * jnp.log(4.0))
    row_scales = jnp.exp(jax.random.uniform(key_rows, (SEQS, 1), jnp.float32, jnp.log(0.5), jnp.log(5.0)))
    base_vals = jnp.clip(jax.random.normal(key_base, (SEQS, D), jnp.float32), -4.0, 4.0)
    return (base_vals * rising[None, :] * jitter * row_scales).astype(jnp.bfloat16)


def spiked(values, stream_key, source, target, parts, factor):
    def block_of(dim):
        return (jnp.arange(values.shape[dim]) // (values.shape[dim] // parts)).reshape((-1,) + (1,) * (values.ndim - 1 - dim))

    near = jax.random.permutation(stream_key, parts)[block_of(target)]
    second = (block_of(target) + parts // 2) % parts
    return jnp.where((block_of(source) == near) | (block_of(source) == second), factor * values, values)


def shard_levels(stream_key, dims, cuts, smallest, high):
    level, own = 1.0, jax.random.fold_in(stream_key, 6)
    for position, parts in cuts:
        steps = jnp.exp(jax.random.uniform(jax.random.fold_in(own, position), (parts,), jnp.float32, smallest / len(cuts), high / len(cuts)))
        level = level * jnp.repeat(steps, dims[position] // parts).reshape([-1 if axis == position else 1 for axis in range(len(dims))])
    return level


def scatter_about(rng, dims, scale, bound, split=(), kind=jnp.bfloat16):
    level = shard_levels(rng, dims, split, -0.22, 0.18) if split else 1.0
    values = jax.random.normal(rng, dims, jnp.float32) * scale * level
    return jnp.minimum(jnp.maximum(values, -bound), bound).astype(kind)


def bell_draw_with(own_key, extent, deviation, limit, cuts, heavy, kind=jnp.bfloat16):
    entries = deviation * jax.random.normal(own_key, extent, jnp.float32)
    if cuts:
        entries = entries * shard_levels(own_key, extent, cuts, -0.22, 0.18)
    return jnp.clip(spiked(entries, jax.random.fold_in(own_key, 3), *heavy), -limit, limit).astype(kind)


def setup_inputs(seed: int = 0) -> dict:
    keys = jax.random.split(jax.random.key(seed), 19)
    return {
        "tokens": draw_tokens(jax.random.fold_in(keys[18], 71), 0),
        "past_state": scatter_about(keys[1], (SEQS, HEADS, HEAD_DIM, HEAD_DIM), 0.3, 4.0, ((0, 16), (1, 8)), jnp.float32),
        "pre_gain": jnp.clip(1.0 + 0.18 * jax.random.normal(keys[2], (D,), jnp.float32), 0.1, 1.9),
        "pre_gate": scatter_about(keys[3], (D, FF), D ** -0.5, 0.09375, ((1, 128),)),
        "pre_up": scatter_about(keys[4], (D, FF), D ** -0.5, 0.09375, ((1, 128),)),
        "pre_down": bell_draw_with(keys[5], (FF, D), FF ** -0.5, 0.21875, ((0, 128),), (0, 1, 128, 5.5)),
        "mix_gain": jnp.clip(1.0 + 0.18 * jax.random.normal(keys[6], (D,), jnp.float32), 0.1, 1.9),
        "query_weight": scatter_about(keys[7], (D, INNER), D ** -0.5, 0.09375, ((0, 16), (1, 8))),
        "forget_weight": scatter_about(keys[8], (D, INNER), D ** -0.5, 0.09375, ((0, 16), (1, 8))),
        "value_weight": scatter_about(keys[9], (D, INNER), D ** -0.5, 0.09375, ((0, 16), (1, 8))),
        "output_gate_weight": scatter_about(keys[10], (D, INNER), D ** -0.5, 0.09375, ((0, 16), (1, 8))),
        "forget_floor": jnp.clip(jnp.exp(math.log(0.9) - 3.8066625 * jax.random.uniform(keys[11], (INNER,), jnp.float32) ** shard_levels(keys[11], (INNER,), ((0, 8),), -0.2, 0.2)), 0.02, 0.9),
        "head_gain": jnp.clip(1.0 + 0.18 * jax.random.normal(keys[12], (HEAD_DIM,), jnp.float32), 0.1, 1.9),
        "proj_out": scatter_about(keys[13], (INNER, D), INNER ** -0.5, 0.125, ((0, 8), (1, 16))),
        "post_gain": jnp.clip(1.0 + 0.18 * jax.random.normal(keys[14], (D,), jnp.float32), 0.1, 1.9),
        "post_gate": scatter_about(keys[15], (D, FF), D ** -0.5, 0.09375, ((1, 128),)),
        "post_up": scatter_about(keys[16], (D, FF), D ** -0.5, 0.09375, ((1, 128),)),
        "post_down": bell_draw_with(keys[17], (FF, D), FF ** -0.5, 0.21875, ((0, 128),), (0, 1, 128, 5.5)),
    }


epsilon = 1e-06

def half_step(activations, gain, w_gate, w_up, w_down):
    x_float = activations.astype(jnp.float32)
    row_scale = lax.rsqrt(lax.optimization_barrier(jnp.mean(x_float * x_float, axis=1, keepdims=True)) + epsilon)
    normed = (x_float * gain).astype(jnp.bfloat16)
    gate_pre = row_scale * jnp.dot(normed, w_gate, preferred_element_type=jnp.float32)
    up_pre = row_scale * jnp.dot(normed, w_up, preferred_element_type=jnp.float32)
    hidden = (jax.nn.silu(gate_pre) * up_pre).astype(jnp.bfloat16)
    down_out = jnp.dot(hidden, w_down, preferred_element_type=jnp.float32)
    return (x_float + 0.5 * down_out).astype(jnp.bfloat16)

def reference(tokens, past_state, pre_gain, pre_gate, pre_up, pre_down, mix_gain, query_weight, forget_weight, value_weight, output_gate_weight, forget_floor, head_gain, proj_out, post_gain, post_gate, post_up, post_down):
    after_first = half_step(tokens, pre_gain, pre_gate, pre_up, pre_down)
    first_float = after_first.astype(jnp.float32)
    row_scale = lax.rsqrt(lax.optimization_barrier(jnp.mean(first_float * first_float, axis=1, keepdims=True)) + epsilon)
    normed = (first_float * mix_gain).astype(jnp.bfloat16)
    row_count = tokens.shape[0]
    head_shape = (row_count, HEADS, HEAD_DIM)
    pre_query = row_scale * jnp.dot(normed, query_weight, preferred_element_type=jnp.float32)
    pre_forget = row_scale * jnp.dot(normed, forget_weight, preferred_element_type=jnp.float32)
    pre_value = row_scale * jnp.dot(normed, value_weight, preferred_element_type=jnp.float32)
    pre_gate_out = row_scale * jnp.dot(normed, output_gate_weight, preferred_element_type=jnp.float32)
    floors = forget_floor.reshape(HEADS, HEAD_DIM)
    forget_heads = pre_forget.reshape(head_shape)
    forget = floors + (1.0 - floors) * jax.nn.sigmoid(forget_heads)
    written = (1.0 - floors) * jax.nn.sigmoid(-forget_heads)
    query_act = jax.nn.silu(pre_query.reshape(head_shape))
    value_act = pre_value.reshape(head_shape)
    new_state = forget[:, :, :, None] * past_state + written[:, :, :, None] * value_act[:, :, None, :]
    readout = jnp.einsum('bhkv,bhk->bhv', new_state, query_act, precision=lax.Precision.HIGHEST)
    readout = readout * lax.rsqrt(lax.optimization_barrier(jnp.mean(readout * readout, axis=2, keepdims=True)) + epsilon) * head_gain
    mixed_in = (readout.reshape(row_count, INNER) * jax.nn.silu(pre_gate_out)).astype(jnp.bfloat16)
    per_group = INNER // N_TP
    total_sum = jnp.zeros((row_count, D), jnp.float32)
    for head_block in range(N_TP):
        lower = head_block * per_group
        partial_out = jnp.dot(mixed_in[:, lower:lower + per_group], proj_out[lower:lower + per_group], preferred_element_type=jnp.float32).astype(jnp.bfloat16)
        total_sum = total_sum + partial_out.astype(jnp.float32)
    second = (first_float + total_sum).astype(jnp.bfloat16)
    result = half_step(second, post_gain, post_gate, post_up, post_down)
    return (result, new_state)
```

```python
import jax
import jax.numpy as jnp
from jax import lax
from jax.sharding import Mesh
from jax.sharding import PartitionSpec as P

D = 4096
ALL = ("z", "y", "x", "c")
KV = ("z", "y")
TP = ("x", "c")
SAME_CORE = ("z", "y", "x")
epsilon = 1e-06
f32 = jnp.float32
bf16 = jnp.bfloat16


def copy_for_each(value, axes):
    copies = jnp.broadcast_to(value, (lax.axis_size(axes), *value.shape))
    return lax.all_to_all(copies, axes, split_axis=0, concat_axis=0, tiled=True)


def exchange(pieces, axes):
    return lax.all_to_all(pieces, axes, split_axis=0, concat_axis=0, tiled=True)


def other_core(value):
    return lax.ppermute(value, "c", [(0, 1), (1, 0)])


def dot_t(left, right):
    return lax.dot_general(left, right, (((1,), (0,)), ((), ())), preferred_element_type=f32)


def half_step(own, gain, gate, up, down, gate_far, up_far, down_far):
    core = lax.axis_index("c")
    chips = lax.axis_size(SAME_CORE)
    width, rows = own.shape
    units = gate.shape[0]
    pieces = copy_for_each(own, SAME_CORE).astype(f32)
    squares = jnp.sum(pieces * pieces, axis=(0, 1))
    parity = lax.broadcasted_iota(jnp.int32, (1, 2, 1, 1), 1)
    gains = gain.reshape(chips, 2, width, 1)
    normed = jnp.where(parity == core, pieces[:, None] * gains, 0.0).astype(bf16)
    normed = normed.reshape(chips * 2 * width, rows)
    parts = [dot_t(w, normed) for w in (gate, up, gate_far, up_far)]
    sent = jnp.concatenate([*parts, jnp.broadcast_to(squares, (8, rows))], axis=0)
    got = other_core(sent)
    g_own = parts[0] + got[2 * units : 3 * units]
    u_own = parts[1] + got[3 * units : 4 * units]
    g_far = parts[2] + got[:units]
    u_far = parts[3] + got[units : 2 * units]
    scale = lax.rsqrt((squares + got[4 * units]) / D + epsilon)[None, :]
    hidden = jnp.concatenate(
        [
            (jax.nn.silu(scale * g_own) * (scale * u_own)).astype(bf16),
            (jax.nn.silu(scale * g_far) * (scale * u_far)).astype(bf16),
        ],
        axis=0,
    )
    weights = jnp.concatenate([down, down_far], axis=0)
    out = lax.dot_general(weights, hidden, (((0,), (0,)), ((), ())), preferred_element_type=f32)
    out = out.astype(bf16).reshape(chips, 2, width, rows)
    out = jnp.where(core == 0, out[:, 0], out[:, 1])
    total = jnp.sum(exchange(out, SAME_CORE).astype(f32), axis=0)
    return (own.astype(f32) + 0.5 * total).astype(bf16)


def per_device(
    tokens,
    past_state,
    pre_gain,
    pre_gate,
    pre_up,
    pre_down,
    mix_gain,
    query_weight,
    forget_weight,
    value_weight,
    output_gate_weight,
    forget_floor,
    head_gain,
    proj_out,
    post_gain,
    post_gate,
    post_up,
    post_down,
):
    pre = [pre_gate.T, pre_up.T, pre_down]
    post = [post_gate.T, post_up.T, post_down]
    first = half_step(tokens.T, pre_gain, *pre, *[other_core(w) for w in pre])

    block = copy_for_each(first, TP)
    block = block.reshape(-1, block.shape[2])
    width, rows = block.shape
    own_rows, local_heads, head_width, _ = past_state.shape
    block_float = block.astype(f32)
    gains = lax.dynamic_slice_in_dim(mix_gain, lax.axis_index(KV) * width, width, 0)
    squares = jnp.sum(block_float * block_float, axis=0)
    square_high = squares.astype(bf16)
    square_low = (squares - square_high.astype(f32)).astype(bf16)
    normed = (block_float * gains[:, None]).astype(bf16).T
    weight_list = (query_weight, forget_weight, value_weight, output_gate_weight)
    parts = [jnp.dot(normed, w, preferred_element_type=f32).astype(bf16) for w in weight_list]
    parts += [
        jnp.broadcast_to(square_high[:, None], (rows, 128)),
        jnp.broadcast_to(square_low[:, None], (rows, 128)),
    ]
    sent = jnp.concatenate(parts, axis=1).reshape(-1, own_rows, 4 * width + 256)
    projected = jnp.sum(exchange(sent, KV).astype(f32), axis=0)
    own_squares = projected[:, 4 * width] + projected[:, 4 * width + 128]
    projected = projected[:, : 4 * width] * lax.rsqrt(own_squares / D + epsilon)[:, None]
    pre_query, pre_forget, pre_value, pre_gate_out = jnp.split(projected, 4, axis=1)
    head_shape = (own_rows, local_heads, head_width)
    floors = forget_floor.reshape(local_heads, head_width)
    forget_heads = pre_forget.reshape(head_shape)
    forget = floors + (1.0 - floors) * jax.nn.sigmoid(forget_heads)
    written = (1.0 - floors) * jax.nn.sigmoid(-forget_heads)
    query_act = jax.nn.silu(pre_query.reshape(head_shape))
    value_act = pre_value.reshape(head_shape)
    new_state = (
        forget[:, :, :, None] * past_state + written[:, :, :, None] * value_act[:, :, None, :]
    )
    readout = jnp.einsum("bhkv,bhk->bhv", new_state, query_act, precision=lax.Precision.HIGHEST)
    readout = (
        readout
        * lax.rsqrt(jnp.mean(readout * readout, axis=2, keepdims=True) + epsilon)
        * head_gain
    )
    mixed_in = (
        readout.reshape(own_rows, local_heads * head_width) * jax.nn.silu(pre_gate_out)
    ).astype(bf16)
    gathered = copy_for_each(mixed_in, KV).reshape(rows, local_heads * head_width)
    partials = lax.dot_general(
        proj_out, gathered, (((0,), (1,)), ((), ())), preferred_element_type=f32
    ).astype(bf16)
    mixed_sum = jnp.sum(exchange(partials.reshape(-1, *first.shape), TP).astype(f32), axis=0)
    second = (first.astype(f32) + mixed_sum).astype(bf16)
    result = half_step(second, post_gain, *post, *[other_core(w) for w in post])
    return (result.T, new_state)


def solution(mesh):
    torus = Mesh(mesh.devices.reshape(4, 4, 4, 2), ALL)
    return jax.shard_map(
        per_device,
        mesh=torus,
        in_specs=(
            P(None, ALL),
            P(KV, TP, None, None),
            P(),
            P(None, ALL),
            P(None, ALL),
            P(ALL, None),
            P(),
            P(KV, TP),
            P(KV, TP),
            P(KV, TP),
            P(KV, TP),
            P(TP),
            P(),
            P(TP, KV),
            P(),
            P(None, ALL),
            P(None, ALL),
            P(ALL, None),
        ),
        out_specs=(P(None, ALL), P(KV, TP, None, None)),
        check_vma=False,
    )
```

```python
import jax
import jax.numpy as jnp
from jax import lax
from jax.sharding import Mesh
from jax.sharding import PartitionSpec as P

D = 4096
ALL = ("z", "y", "x", "c")
KV = ("z", "y")
TP = ("x", "c")
epsilon = 1e-06
f32 = jnp.float32
bf16 = jnp.bfloat16


def copy_for_each(value, axes):
    copies = jnp.broadcast_to(value, (lax.axis_size(axes), *value.shape))
    return lax.all_to_all(copies, axes, split_axis=0, concat_axis=0, tiled=True)


def exchange(pieces, axes):
    return lax.all_to_all(pieces, axes, split_axis=0, concat_axis=0, tiled=True)


def other_core(value):
    return lax.ppermute(value, "c", [(0, 1), (1, 0)])


def dot_t(left, right):
    return lax.dot_general(left, right, (((1,), (0,)), ((), ())), preferred_element_type=f32)


def device(z, y, x, c):
    return ((z % 4 * 4 + y % 4) * 4 + x % 4) * 2 + c


PLACES = [(z, y, x, c) for z in range(4) for y in range(4) for x in range(4) for c in range(2)]
PLANES = [[device(z, m, x, 0) for z in range(4) for m in range(4)] for x in range(4)] + [
    [device(z, y, m, 1) for z in range(4) for m in range(4)] for y in range(4)
]


def shift(value, steps):
    pairs = [
        (device(z, y, x, c), device(z, y, x + steps, c) if c == 0 else device(z, y + steps, x, c))
        for z, y, x, c in PLACES
    ]
    return lax.ppermute(value, ALL, pairs)


def plane_exchange(pieces):
    return lax.all_to_all(
        pieces, ALL, split_axis=0, concat_axis=0, axis_index_groups=PLANES, tiled=True
    )


def selection():
    core = lax.axis_index("c")
    out = lax.broadcasted_iota(jnp.int32, (1, 512), 1)
    chunk, place, column = out // 128, out // 32 % 4, out % 32
    far_x = (lax.axis_index("x") + chunk) % 4
    far_y = (lax.axis_index("y") + chunk) % 4
    source = jnp.where(
        core == 0, place * 256 + far_x * 64, far_y * 256 + place * 64 + 32
    ) + column
    return source == lax.broadcasted_iota(jnp.int32, (1024, 512), 0)


def chunked(weights, chosen):
    by_z = [
        jnp.dot(weights[:, 1024 * z : 1024 * (z + 1)], chosen, preferred_element_type=f32).astype(
            bf16
        )
        for z in range(4)
    ]
    return [
        jnp.concatenate([w[:, 128 * k : 128 * (k + 1)] for w in by_z], axis=1) for k in range(4)
    ]


def prepare(gain, gate, up, down, chosen):
    far = [other_core(w) for w in (gate, up, down)]
    wide = chunked(jnp.concatenate([gate, up, far[0], far[1]], axis=0), chosen)
    deep = chunked(jnp.concatenate([down, far[2]], axis=0), chosen)
    gains = jnp.dot(gain.reshape(4, 1024), chosen.astype(f32), precision=lax.Precision.HIGHEST)
    gains = [gains[:, 128 * k : 128 * (k + 1)].reshape(512, 1) for k in range(4)]
    return wide, deep, gains


def half_step(own, wide, deep, gains):
    width, rows = own.shape
    units = deep[0].shape[0] // 2
    near = plane_exchange(jnp.broadcast_to(own, (16, width, rows))).reshape(16 * width, rows)
    chunks = {0: near}
    for k in (2, 1, 3):
        chunks[k] = shift(near, -k)
    acc = squares = 0.0
    for k in (0, 1, 3, 2):
        piece = chunks[k].astype(f32)
        squares = squares + jnp.sum(piece * piece, axis=0)
        acc = acc + dot_t(wide[k], (piece * gains[k]).astype(bf16))
    sent = jnp.concatenate([acc, jnp.broadcast_to(squares, (8, rows))], axis=0)
    got = other_core(sent)
    scale = lax.rsqrt((squares + got[4 * units]) / D + epsilon)[None, :]
    own_acc = acc[: 2 * units] + got[2 * units : 4 * units]
    far_acc = acc[2 * units :] + got[: 2 * units]
    hidden = jnp.concatenate(
        [
            (jax.nn.silu(scale * a[:units]) * (scale * a[units:])).astype(bf16)
            for a in (own_acc, far_acc)
        ],
        axis=0,
    )
    sums = {
        k: lax.dot_general(
            deep[k], hidden, (((0,), (0,)), ((), ())), preferred_element_type=f32
        ).astype(bf16)
        for k in (2, 1, 3, 0)
    }
    arrived = [shift(sums[k], k) for k in (2, 1, 3)]
    total = sums[0].astype(f32)
    for piece in arrived:
        total = total + piece.astype(f32)
    total = plane_exchange(total.astype(bf16).reshape(16, width, rows)).astype(f32).sum(axis=0)
    return (own.astype(f32) + 0.5 * total).astype(bf16)


def per_device(
    tokens,
    past_state,
    pre_gain,
    pre_gate,
    pre_up,
    pre_down,
    mix_gain,
    query_weight,
    forget_weight,
    value_weight,
    output_gate_weight,
    forget_floor,
    head_gain,
    proj_out,
    post_gain,
    post_gate,
    post_up,
    post_down,
):
    chosen = selection().astype(bf16)
    pre = prepare(pre_gain, pre_gate.T, pre_up.T, pre_down, chosen)
    post = prepare(post_gain, post_gate.T, post_up.T, post_down, chosen)
    first = half_step(tokens.T, *pre)

    block = copy_for_each(first, TP)
    block = block.reshape(-1, block.shape[2])
    width, rows = block.shape
    own_rows, local_heads, head_width, _ = past_state.shape
    block_float = block.astype(f32)
    gains = lax.dynamic_slice_in_dim(mix_gain, lax.axis_index(KV) * width, width, 0)
    squares = jnp.sum(block_float * block_float, axis=0)
    square_high = squares.astype(bf16)
    square_low = (squares - square_high.astype(f32)).astype(bf16)
    normed = (block_float * gains[:, None]).astype(bf16).T
    weight_list = (query_weight, forget_weight, value_weight, output_gate_weight)
    parts = [jnp.dot(normed, w, preferred_element_type=f32).astype(bf16) for w in weight_list]
    parts.append(jnp.broadcast_to(square_high[:, None], (rows, 64)))
    parts.append(jnp.broadcast_to(square_low[:, None], (rows, 64)))
    sent = jnp.concatenate(parts, axis=1).reshape(-1, own_rows, 4 * width + 128)
    projected = jnp.sum(exchange(sent, KV).astype(f32), axis=0)
    own_squares = projected[:, 4 * width] + projected[:, 4 * width + 64]
    projected = projected[:, : 4 * width] * lax.rsqrt(own_squares / D + epsilon)[:, None]
    pre_query, pre_forget, pre_value, pre_gate_out = jnp.split(projected, 4, axis=1)
    head_shape = (own_rows, local_heads, head_width)
    floors = forget_floor.reshape(local_heads, head_width)
    forget_heads = pre_forget.reshape(head_shape)
    forget = floors + (1.0 - floors) * jax.nn.sigmoid(forget_heads)
    written = (1.0 - floors) * jax.nn.sigmoid(-forget_heads)
    query_act = jax.nn.silu(pre_query.reshape(head_shape))
    value_act = pre_value.reshape(head_shape)
    new_state = (
        forget[:, :, :, None] * past_state + written[:, :, :, None] * value_act[:, :, None, :]
    )
    readout = jnp.einsum("bhkv,bhk->bhv", new_state, query_act, precision=lax.Precision.HIGHEST)
    readout = (
        readout
        * lax.rsqrt(jnp.mean(readout * readout, axis=2, keepdims=True) + epsilon)
        * head_gain
    )
    mixed_in = (
        readout.reshape(own_rows, local_heads * head_width) * jax.nn.silu(pre_gate_out)
    ).astype(bf16)
    gathered = copy_for_each(mixed_in, KV).reshape(rows, local_heads * head_width)
    partials = lax.dot_general(
        proj_out, gathered, (((0,), (1,)), ((), ())), preferred_element_type=f32
    ).astype(bf16)
    mixed_sum = jnp.sum(exchange(partials.reshape(-1, *first.shape), TP).astype(f32), axis=0)
    second = (first.astype(f32) + mixed_sum).astype(bf16)
    result = half_step(second, *post)
    return (result.T, new_state)


def solution(mesh):
    torus = Mesh(mesh.devices.reshape(4, 4, 4, 2), ALL)
    return jax.shard_map(
        per_device,
        mesh=torus,
        in_specs=(
            P(None, ALL),
            P(KV, TP, None, None),
            P(),
            P(None, ALL),
            P(None, ALL),
            P(ALL, None),
            P(),
            P(KV, TP),
            P(KV, TP),
            P(KV, TP),
            P(KV, TP),
            P(TP),
            P(),
            P(TP, KV),
            P(),
            P(None, ALL),
            P(None, ALL),
            P(ALL, None),
        ),
        out_specs=(P(None, ALL), P(KV, TP, None, None)),
        check_vma=False,
    )
```

```python
import functools

import jax
import jax.numpy as jnp
from jax import lax
from jax.experimental import pallas as pl
from jax.experimental.pallas import tpu as pltpu
from jax.sharding import Mesh
from jax.sharding import PartitionSpec as P

D = 4096
ALL = ("z", "y", "x", "c")
KV = ("z", "y")
TP = ("x", "c")
epsilon = 1e-06
f32 = jnp.float32
bf16 = jnp.bfloat16


def copy_for_each(value, axes):
    copies = jnp.broadcast_to(value, (lax.axis_size(axes), *value.shape))
    return lax.all_to_all(copies, axes, split_axis=0, concat_axis=0, tiled=True)


def exchange(pieces, axes):
    return lax.all_to_all(pieces, axes, split_axis=0, concat_axis=0, tiled=True)


def other_core(value):
    return lax.ppermute(value, "c", [(0, 1), (1, 0)])


def dot_t(left, right):
    return lax.dot_general(left, right, (((1,), (0,)), ((), ())), preferred_element_type=f32)


def device(z, y, x, c):
    return ((z % 4 * 4 + y % 4) * 4 + x % 4) * 2 + c


PLACES = [(z, y, x, c) for z in range(4) for y in range(4) for x in range(4) for c in range(2)]
PLANES = [[device(z, m, x, 0) for z in range(4) for m in range(4)] for x in range(4)] + [
    [device(z, y, m, 1) for z in range(4) for m in range(4)] for y in range(4)
]


def shift(value, steps):
    pairs = [
        (device(z, y, x, c), device(z, y, x + steps, c) if c == 0 else device(z, y + steps, x, c))
        for z, y, x, c in PLACES
    ]
    return lax.ppermute(value, ALL, pairs)


def plane_exchange(pieces):
    return lax.all_to_all(
        pieces, ALL, split_axis=0, concat_axis=0, axis_index_groups=PLANES, tiled=True
    )


PAD = 96


def padded(rows):
    return -(-rows // 16) * 16


def sources(core):
    out = lax.broadcasted_iota(jnp.int32, (1, 512), 1)
    chunk, place, column = out // 128, out // 32 % 4, out % 32
    far_x = (lax.axis_index("x") + chunk) % 4
    far_y = (lax.axis_index("y") + chunk) % 4
    return column + jnp.where(
        core == 0, place * 256 + far_x * 64, far_y * 256 + place * 64 + 32
    )


def order_body(mine, theirs, gain, gate, up, down, near, far, gains, rows, picks):
    units = gate.shape[0]

    @pl.when(pl.program_id(0) == 0)
    def _():
        rows[...] = jnp.zeros_like(rows)
        place = lax.broadcasted_iota(jnp.int32, (1024, 512), 0)
        picks[0] = (place == mine[...]).astype(bf16)
        picks[1] = (place == theirs[...]).astype(bf16)

    for j, weight in enumerate((gate, up, down)):
        rows[PAD * j : PAD * j + units, :] = weight[...]
    for side, out in enumerate((near, far)):
        chosen = jnp.dot(rows[...], picks[side], preferred_element_type=f32).astype(bf16)
        for k in range(4):
            for j in range(3):
                out[k, j] = chosen[PAD * j : PAD * (j + 1), 128 * k : 128 * (k + 1)]
    row = jnp.dot(
        jnp.broadcast_to(gain[pl.ds(pl.program_id(0), 1), :], (128, 1024)),
        picks[0].astype(f32),
        preferred_element_type=f32,
        precision=lax.Precision.HIGHEST,
    )
    for k in range(4):
        gains[k] = row[:, 128 * k : 128 * (k + 1)].T


def order_weights(gain, gate, up, down):
    core = lax.axis_index("c")
    units = gate.shape[0]
    whole = pl.BlockSpec((1, 512), lambda z: (0, 0))
    piece = pl.BlockSpec((units, 1024), lambda z: (0, z))
    side = pl.BlockSpec((4, 3, PAD, 128), lambda z: (0, 0, 0, z))
    shape = jax.ShapeDtypeStruct((4, 3, PAD, 512), bf16)
    return pl.pallas_call(
        order_body,
        grid=(4,),
        in_specs=[
            whole,
            whole,
            pl.BlockSpec((4, 1024), lambda z: (0, 0)),
            piece,
            piece,
            piece,
        ],
        out_specs=[side, side, pl.BlockSpec((4, 128, 128), lambda z: (0, z, 0))],
        out_shape=[shape, shape, jax.ShapeDtypeStruct((4, 512, 128), f32)],
        scratch_shapes=[pltpu.VMEM((3 * PAD, 1024), bf16), pltpu.VMEM((2, 1024, 512), bf16)],
        cost_estimate=pl.CostEstimate(flops=5 * 10**9, bytes_accessed=6 * 10**6, transcendentals=0),
        compiler_params=pltpu.CompilerParams(vmem_limit_bytes=20 * 2**20),
        name="order",
    )(sources(core), sources(1 - core), gain.reshape(4, 1024), gate, up, down)


def product_body(*refs, parts, starts):
    chunks = len(starts)
    pieces, refs = refs[: len(parts)], refs[len(parts) :]
    nears, fars, gains = refs[:chunks], refs[chunks : 2 * chunks], refs[2 * chunks : 3 * chunks]
    if len(refs) > 3 * chunks + 2:
        before, out, normed = refs[3 * chunks :]
    else:
        before, (out, normed) = None, refs[3 * chunks :]
    squares = 0.0
    for piece, (chunk, first) in zip(pieces, parts, strict=True):
        count, rows = piece.shape
        value = piece[...].astype(f32)
        squares = squares + jnp.sum(value * value, axis=0, keepdims=True)
        gain = gains[chunk][0, first : first + count, :]
        gain = jnp.concatenate([gain] * (rows // 128), axis=1)
        normed[512 * chunk + first : 512 * chunk + first + count, :] = (value * gain).astype(bf16)
    for side, weights in enumerate((nears, fars)):
        weights = jnp.concatenate([w[0].reshape(2 * PAD, 512) for w in weights], axis=1)
        total = jnp.dot(weights, normed[...], preferred_element_type=f32)
        where = slice(2 * PAD * side, 2 * PAD * (side + 1))
        out[where, :] = total if before is None else before[where, :] + total
    squares = jnp.broadcast_to(squares, (8, squares.shape[1]))
    where = slice(4 * PAD, 4 * PAD + 8)
    out[where, :] = squares if before is None else before[where, :] + squares


def products(pieces, chunks, near, far, gains, before=None):
    rows = pieces[0][0].shape[1]
    parts = tuple((chunks.index(k), first) for _, k, first in pieces)
    operands = [p for p, _, _ in pieces]
    specs = [pl.BlockSpec(p.shape, lambda i: (0, 0)) for p in operands]
    for weights in (near, far):
        for k in chunks:
            operands.append(weights)
            specs.append(pl.BlockSpec((1, 2, PAD, 512), lambda i, k=k: (k, 0, 0, 0)))
    for k in chunks:
        operands.append(gains)
        specs.append(pl.BlockSpec((1, 512, 128), lambda i, k=k: (k, 0, 0)))
    height = 4 * PAD + 8
    if before is not None:
        operands.append(before)
        specs.append(pl.BlockSpec((height, rows), lambda i: (0, 0)))
    return pl.pallas_call(
        functools.partial(product_body, parts=parts, starts=chunks),
        grid=(1,),
        in_specs=specs,
        out_specs=pl.BlockSpec((height, rows), lambda i: (0, 0)),
        out_shape=jax.ShapeDtypeStruct((height, rows), f32),
        scratch_shapes=[pltpu.VMEM((512 * len(chunks), rows), bf16)],
        cost_estimate=pl.CostEstimate(
            flops=len(chunks) * 4 * 10**8, bytes_accessed=len(chunks) * 10**6, transcendentals=0
        ),
        compiler_params=pltpu.CompilerParams(vmem_limit_bytes=16 * 2**20),
        name="products",
    )(*operands)


def state_body(arrived, past, floor, gain, new, mixed, columns, value, gate, readout):
    step = pl.program_id(0)
    group, heads, width, _ = past.shape
    count = readout.shape[0]

    @pl.when(step == 0)
    def _():
        total = arrived[0].astype(f32)
        for i in range(1, arrived.shape[0]):
            total = total + arrived[i].astype(f32)
        inner = heads * width
        squares = total[:, 4 * inner : 4 * inner + 1] + total[:, 4 * inner + 64 : 4 * inner + 65]
        total = total[:, : 4 * inner] * lax.rsqrt(squares / D + epsilon)
        query, keep = total[:, :inner], total[:, inner : 2 * inner]
        value[...] = total[:, 2 * inner : 3 * inner]
        gate[...] = jax.nn.silu(total[:, 3 * inner :])
        query = jax.nn.silu(query)
        bound = floor[...]
        forget = bound + (1.0 - bound) * jax.nn.sigmoid(keep)
        written = (1.0 - bound) * jax.nn.sigmoid(-keep)
        for h in range(heads):
            lanes = slice(width * h, width * (h + 1))
            table = [forget[:, lanes], written[:, lanes], query[:, lanes], query[:, lanes]]
            columns[h] = jnp.concatenate(table, axis=0).T

    here = pl.ds(pl.multiple_of(group * step, group), group)
    for h in range(heads):
        lanes = slice(width * h, width * (h + 1))
        near = pltpu.roll(columns[h], lax.rem(4 * count - group * step, 4 * count), axis=1)
        values = value[here, lanes]
        sums = []
        for j in range(group):
            forget, written, query = (
                jnp.broadcast_to(near[:, count * i + j : count * i + j + 1], (width, width))
                for i in range(3)
            )
            state = forget * past[j, h] + written * values[j : j + 1, :]
            new[j, h] = state
            sums.append(jnp.sum(state * query, axis=0, keepdims=True))
        readout[here, lanes] = jnp.concatenate(sums, axis=0)

    @pl.when(step == pl.num_programs(0) - 1)
    def _():
        for h in range(heads):
            lanes = slice(width * h, width * (h + 1))
            r = readout[:, lanes]
            r = r * lax.rsqrt(jnp.mean(r * r, axis=1, keepdims=True) + epsilon) * gain[...]
            mixed[:, lanes] = (r * gate[:, lanes]).astype(bf16)


def state_update(arrived, past, floor, gain):
    count, heads, width, _ = past.shape
    group = 8
    block = pl.BlockSpec((group, heads, width, width), lambda i: (i, 0, 0, 0))
    rows = pltpu.VMEM((count, heads * width), f32)
    return pl.pallas_call(
        state_body,
        grid=(count // group,),
        in_specs=[
            pl.BlockSpec(arrived.shape, lambda i: (0, 0, 0)),
            block,
            pl.BlockSpec((1, heads * width), lambda i: (0, 0)),
            pl.BlockSpec((1, width), lambda i: (0, 0)),
        ],
        out_specs=[block, pl.BlockSpec((count, heads * width), lambda i: (0, 0))],
        out_shape=[
            jax.ShapeDtypeStruct(past.shape, f32),
            jax.ShapeDtypeStruct((count, heads * width), bf16),
        ],
        scratch_shapes=[pltpu.VMEM((heads, width, 4 * count), f32), rows, rows, rows],
        compiler_params=pltpu.CompilerParams(vmem_limit_bytes=14 * 2**20),
        name="state",
    )(arrived, past, floor.reshape(1, -1), gain.reshape(1, -1))


def project_body(block, gain, *refs):
    weights, out = refs[:-1], refs[-1]
    value = block[...].astype(f32)
    rows = value.shape[1]
    normed = (value * jnp.concatenate([gain[...]] * (rows // 128), axis=1)).astype(bf16)
    normed = normed.T
    count, own, _ = out.shape
    for i, w in enumerate(weights):
        part = jnp.dot(normed, w[...], preferred_element_type=f32).astype(bf16)
        out[:, :, 256 * i : 256 * (i + 1)] = part.reshape(count, own, 256)
    squares = jnp.sum(value * value, axis=0, keepdims=True)
    squares = jnp.broadcast_to(squares, (128, rows)).T
    high = squares.astype(bf16)
    low = squares - high.astype(f32)
    lane = lax.broadcasted_iota(jnp.int32, squares.shape, 1)
    both = jnp.where(lane < 64, high.astype(f32), low).astype(bf16)
    out[:, :, 1024:1152] = both.reshape(count, own, 128)


def project(block, gain, weights, own_rows):
    width, rows = block.shape
    return pl.pallas_call(
        project_body,
        out_shape=jax.ShapeDtypeStruct((rows // own_rows, own_rows, 4 * width + 128), bf16),
        compiler_params=pltpu.CompilerParams(vmem_limit_bytes=14 * 2**20),
        name="project",
    )(block, jnp.broadcast_to(gain[:, None], (width, 128)), *weights)


def half_step(own, near_w, far_w, gains, near):
    width, rows = own.shape
    half = near.shape[0] // 2
    top, low = slice(0, half), slice(half, 2 * half)
    left_top = shift(near[top], 1)
    right_low = shift(near[low], -1)
    left_low = shift(near[low], 1)
    right_top = shift(near[top], -1)
    left_top, right_low, far_w = lax.optimization_barrier((left_top, right_low, far_w))
    far_top = shift(left_top, 1)
    far_low = shift(right_low, -1)
    early = [
        (near, 0, 0),
        (left_top, 3, 0),
        (right_low, 1, half),
        (left_low, 3, half),
        (right_top, 1, 0),
    ]
    sent = products(early, [0, 3, 1], near_w, far_w, gains)
    sent = products([(far_top, 2, 0), (far_low, 2, half)], [2], near_w, far_w, gains, sent)
    got = other_core(sent)
    scale = lax.rsqrt((sent[4 * PAD] + got[4 * PAD]) / D + epsilon)[None, :]
    own_acc = sent[: 2 * PAD] + got[2 * PAD : 4 * PAD]
    far_acc = sent[2 * PAD : 4 * PAD] + got[: 2 * PAD]
    hidden = jnp.concatenate(
        [
            (jax.nn.silu(scale * a[:PAD]) * (scale * a[PAD:])).astype(bf16)
            for a in (own_acc, far_acc)
        ],
        axis=0,
    )
    deep = jnp.concatenate([near_w[:, 2], far_w[:, 2]], axis=1)

    def sums(k, part):
        return lax.dot_general(
            deep[k][:, part], hidden, (((0,), (0,)), ((), ())), preferred_element_type=f32
        )

    over_left = shift(sums(2, top).astype(bf16), 1)
    over_right = shift(sums(2, low).astype(bf16), -1)
    left_low = shift(sums(1, low).astype(bf16), 1)
    right_top = shift(sums(3, top).astype(bf16), -1)
    left_top = shift((sums(1, top) + over_left.astype(f32)).astype(bf16), 1)
    right_low = shift((sums(3, low) + over_right.astype(f32)).astype(bf16), -1)
    total = jnp.concatenate(
        [
            (sums(0, top) + left_top.astype(f32) + right_top.astype(f32)).astype(bf16),
            (sums(0, low) + left_low.astype(f32) + right_low.astype(f32)).astype(bf16),
        ],
        axis=0,
    )
    total = plane_exchange(total.reshape(16, width, rows)).astype(f32).sum(axis=0)
    return (own.astype(f32) + 0.5 * total).astype(bf16)


def plane_gather(own):
    return plane_exchange(jnp.broadcast_to(own, (16, *own.shape))).reshape(-1, own.shape[1])


def per_device(
    tokens,
    past_state,
    pre_gain,
    pre_gate,
    pre_up,
    pre_down,
    mix_gain,
    query_weight,
    forget_weight,
    value_weight,
    output_gate_weight,
    forget_floor,
    head_gain,
    proj_out,
    post_gain,
    post_gate,
    post_up,
    post_down,
):
    tokens = tokens.T
    near = plane_gather(tokens)
    near_w, far_w, gains = order_weights(pre_gain, pre_gate.T, pre_up.T, pre_down)
    near, near_w, far_w = lax.optimization_barrier((near, near_w, far_w))
    first = half_step(tokens, near_w, other_core(far_w), gains, near)

    width = mix_gain.shape[0] // lax.axis_size(KV)
    own_rows, local_heads, head_width, _ = past_state.shape
    gains = lax.dynamic_slice_in_dim(mix_gain, lax.axis_index(KV) * width, width, 0)
    block = copy_for_each(first, TP)
    block = block.reshape(-1, block.shape[2])
    rows = block.shape[1]
    weight_list = (query_weight, forget_weight, value_weight, output_gate_weight)
    sent = project(block, gains, weight_list, own_rows)
    sent, post_gate, post_up, post_down = lax.optimization_barrier(
        (sent, post_gate, post_up, post_down)
    )
    near_w, far_w, gains = order_weights(post_gain, post_gate.T, post_up.T, post_down)
    arrived = exchange(sent, KV)
    arrived, near_w, far_w = lax.optimization_barrier((arrived, near_w, far_w))
    far_w = other_core(far_w)
    new_state, mixed_in = state_update(arrived, past_state, forget_floor, head_gain)
    gathered = copy_for_each(mixed_in, KV).reshape(rows, local_heads * head_width)
    partials = lax.dot_general(
        proj_out, gathered, (((0,), (1,)), ((), ())), preferred_element_type=f32
    ).astype(bf16)
    mixed_sum = jnp.sum(exchange(partials.reshape(-1, *first.shape), TP).astype(f32), axis=0)
    second = (first.astype(f32) + mixed_sum).astype(bf16)
    result = half_step(second, near_w, far_w, gains, plane_gather(second))
    return (result.T, new_state)


def solution(mesh):
    torus = Mesh(mesh.devices.reshape(4, 4, 4, 2), ALL)
    return jax.shard_map(
        per_device,
        mesh=torus,
        in_specs=(
            P(None, ALL),
            P(KV, TP, None, None),
            P(),
            P(None, ALL),
            P(None, ALL),
            P(ALL, None),
            P(),
            P(KV, TP),
            P(KV, TP),
            P(KV, TP),
            P(KV, TP),
            P(TP),
            P(),
            P(TP, KV),
            P(),
            P(None, ALL),
            P(None, ALL),
            P(ALL, None),
        ),
        out_specs=(P(None, ALL), P(KV, TP, None, None)),
        check_vma=False,
    )
```

```python
import functools

import jax
import jax.numpy as jnp
from jax import lax
from jax.experimental import pallas as pl
from jax.experimental.pallas import tpu as pltpu
from jax.sharding import Mesh
from jax.sharding import PartitionSpec as P

D = 4096
ALL = ("z", "y", "x", "c")
KV = ("z", "y")
TP = ("x", "c")
epsilon = 1e-06
f32 = jnp.float32
bf16 = jnp.bfloat16


def copy_for_each(value, axes):
    copies = jnp.broadcast_to(value, (lax.axis_size(axes), *value.shape))
    return lax.all_to_all(copies, axes, split_axis=0, concat_axis=0, tiled=True)


def exchange(pieces, axes):
    return lax.all_to_all(pieces, axes, split_axis=0, concat_axis=0, tiled=True)


def other_core(value):
    return lax.ppermute(value, "c", [(0, 1), (1, 0)])


def dot_t(left, right):
    return lax.dot_general(left, right, (((1,), (0,)), ((), ())), preferred_element_type=f32)


def device(z, y, x, c):
    return ((z % 4 * 4 + y % 4) * 4 + x % 4) * 2 + c


PLACES = [(z, y, x, c) for z in range(4) for y in range(4) for x in range(4) for c in range(2)]
PLANES = [[device(z, m, x, 0) for z in range(4) for m in range(4)] for x in range(4)] + [
    [device(z, y, m, 1) for z in range(4) for m in range(4)] for y in range(4)
]


def shift(value, steps):
    pairs = [
        (device(z, y, x, c), device(z, y, x + steps, c) if c == 0 else device(z, y + steps, x, c))
        for z, y, x, c in PLACES
    ]
    return lax.ppermute(value, ALL, pairs)


def plane_exchange(pieces):
    return lax.all_to_all(
        pieces, ALL, split_axis=0, concat_axis=0, axis_index_groups=PLANES, tiled=True
    )


PAD = 96


def in_hbm(value):
    return pltpu.with_memory_space_constraint(value, pltpu.HBM)


def sources(core):
    out = lax.broadcasted_iota(jnp.int32, (1, 512), 1)
    chunk, place, column = out // 128, out // 32 % 4, out % 32
    far_x = (lax.axis_index("x") + chunk) % 4
    far_y = (lax.axis_index("y") + chunk) % 4
    return column + jnp.where(
        core == 0, place * 256 + far_x * 64, far_y * 256 + place * 64 + 32
    )


def order_body(mine, theirs, gain, gate, up, down, near, far, gains, rows, picks):
    units = gate.shape[0]

    @pl.when(pl.program_id(0) == 0)
    def _():
        rows[...] = jnp.zeros_like(rows)
        place = lax.broadcasted_iota(jnp.int32, (1024, 512), 0)
        picks[0] = (place == mine[...]).astype(bf16)
        picks[1] = (place == theirs[...]).astype(bf16)

    for j, weight in enumerate((gate, up, down)):
        rows[PAD * j : PAD * j + units, :] = weight[...]
    rest, row = gain[0], lax.broadcasted_iota(jnp.int32, (16, gain.shape[2]), 0)
    split = jnp.zeros(row.shape, f32)
    for i in range(3):
        part = rest.astype(bf16).astype(f32)
        rest = rest - part
        split = jnp.where(row == i, part, split)
    rows[3 * PAD :, :] = split.astype(bf16)
    mine = jnp.dot(rows[...], picks[0], preferred_element_type=f32)
    theirs = jnp.dot(rows[: 3 * PAD, :], picks[1], preferred_element_type=f32)
    for chosen, out in ((mine, near), (theirs, far)):
        chosen = chosen[: 3 * PAD].astype(bf16)
        for k in range(4):
            for j in range(3):
                out[k, j] = chosen[PAD * j : PAD * (j + 1), 128 * k : 128 * (k + 1)]
    line = jnp.sum(mine[3 * PAD : 3 * PAD + 8], axis=0, keepdims=True)
    line = jnp.broadcast_to(line, (128, line.shape[1]))
    for k in range(4):
        gains[k] = line[:, 128 * k : 128 * (k + 1)].T


def order_weights(gain, gate, up, down):
    core = lax.axis_index("c")
    units = gate.shape[0]
    whole = pl.BlockSpec((1, 512), lambda z: (0, 0))
    piece = pl.BlockSpec((units, 1024), lambda z: (0, z))
    side = pl.BlockSpec((4, 3, PAD, 128), lambda z: (0, 0, 0, z))
    shape = jax.ShapeDtypeStruct((4, 3, PAD, 512), bf16)
    return pl.pallas_call(
        order_body,
        grid=(4,),
        in_specs=[
            whole,
            whole,
            pl.BlockSpec((1, 1, 1024), lambda z: (z, 0, 0)),
            piece,
            piece,
            piece,
        ],
        out_specs=[side, side, pl.BlockSpec((4, 128, 128), lambda z: (0, z, 0))],
        out_shape=[shape, shape, jax.ShapeDtypeStruct((4, 512, 128), f32)],
        scratch_shapes=[pltpu.VMEM((3 * PAD + 16, 1024), bf16), pltpu.VMEM((2, 1024, 512), bf16)],
        cost_estimate=pl.CostEstimate(flops=5 * 10**9, bytes_accessed=6 * 10**6, transcendentals=0),
        compiler_params=pltpu.CompilerParams(vmem_limit_bytes=20 * 2**20),
        name="order",
    )(sources(core), sources(1 - core), gain.reshape(4, 1, 1024), *(in_hbm(w) for w in (gate, up, down)))


def product_body(*refs, parts, starts):
    chunks = len(starts)
    pieces, refs = refs[: len(parts)], refs[len(parts) :]
    nears, fars, gains = refs[:chunks], refs[chunks : 2 * chunks], refs[2 * chunks : 3 * chunks]
    if len(refs) > 3 * chunks + 2:
        before, out, normed = refs[3 * chunks :]
    else:
        before, (out, normed) = None, refs[3 * chunks :]
    squares = 0.0
    for piece, (chunk, first) in zip(pieces, parts, strict=True):
        count, rows = piece.shape
        value = piece[...].astype(f32)
        squares = squares + jnp.sum(value * value, axis=0, keepdims=True)
        gain = gains[chunk][0, first : first + count, :]
        gain = jnp.concatenate([gain] * (rows // 128), axis=1)
        normed[512 * chunk + first : 512 * chunk + first + count, :] = (value * gain).astype(bf16)
    for side, weights in enumerate((nears, fars)):
        weights = jnp.concatenate([w[0].reshape(2 * PAD, 512) for w in weights], axis=1)
        total = jnp.dot(weights, normed[...], preferred_element_type=f32)
        where = slice(2 * PAD * side, 2 * PAD * (side + 1))
        out[where, :] = total if before is None else before[where, :] + total
    squares = jnp.broadcast_to(squares, (8, squares.shape[1]))
    where = slice(4 * PAD, 4 * PAD + 8)
    out[where, :] = squares if before is None else before[where, :] + squares


def products(pieces, chunks, near, far, gains, before=None):
    rows = pieces[0][0].shape[1]
    parts = tuple((chunks.index(k), first) for _, k, first in pieces)
    operands = [p for p, _, _ in pieces]
    specs = [pl.BlockSpec(p.shape, lambda i: (0, 0)) for p in operands]
    for weights in (near, far):
        for k in chunks:
            operands.append(weights)
            specs.append(pl.BlockSpec((1, 2, PAD, 512), lambda i, k=k: (k, 0, 0, 0)))
    for k in chunks:
        operands.append(gains)
        specs.append(pl.BlockSpec((1, 512, 128), lambda i, k=k: (k, 0, 0)))
    height = 4 * PAD + 8
    if before is not None:
        operands.append(before)
        specs.append(pl.BlockSpec((height, rows), lambda i: (0, 0)))
    return pl.pallas_call(
        functools.partial(product_body, parts=parts, starts=chunks),
        grid=(1,),
        in_specs=specs,
        out_specs=pl.BlockSpec((height, rows), lambda i: (0, 0)),
        out_shape=jax.ShapeDtypeStruct((height, rows), f32),
        scratch_shapes=[pltpu.VMEM((512 * len(chunks), rows), bf16)],
        cost_estimate=pl.CostEstimate(
            flops=len(chunks) * 4 * 10**8, bytes_accessed=len(chunks) * 10**6, transcendentals=0
        ),
        compiler_params=pltpu.CompilerParams(vmem_limit_bytes=16 * 2**20),
        name="products",
    )(*operands)


def state_body(arrived, past, floor, gain, new, mixed, columns, query, value, gate, readout):
    step = pl.program_id(0)
    group, heads, width, _ = past.shape
    count = readout.shape[0]

    @pl.when(step == 0)
    def _():
        total = arrived[0].astype(f32)
        for i in range(1, arrived.shape[0]):
            total = total + arrived[i].astype(f32)
        inner = heads * width
        squares = total[:, 4 * inner : 4 * inner + 1] + total[:, 4 * inner + 64 : 4 * inner + 65]
        total = total[:, : 4 * inner] * lax.rsqrt(squares / D + epsilon)
        query[...] = jax.nn.silu(total[:, :inner])
        value[...] = total[:, 2 * inner : 3 * inner]
        gate[...] = jax.nn.silu(total[:, 3 * inner :])
        bound = floor[...]
        forget = bound + (1.0 - bound) * jax.nn.sigmoid(total[:, inner : 2 * inner])
        for h in range(heads):
            table = forget[:, width * h : width * (h + 1)]
            columns[h] = jnp.concatenate([table] * 4, axis=0).T

    here = pl.ds(pl.multiple_of(group * step, group), group)
    for h in range(heads):
        lanes = slice(width * h, width * (h + 1))
        near = pltpu.roll(columns[h], lax.rem(4 * count - group * step, 4 * count), axis=1)
        values, queries = value[here, lanes], query[here, lanes]
        high = queries.astype(bf16).astype(f32)
        queries = jnp.concatenate([high, queries - high], axis=0).astype(bf16)
        sums = []
        for j in range(group):
            forget = jnp.broadcast_to(near[:, j : j + 1], (width, width))
            added = values[j : j + 1, :]
            state = added + forget * (past[j, h] - added)
            new[j, h] = state
            both = jnp.dot(queries, state.astype(bf16), preferred_element_type=f32)
            sums.append(both[j : j + 1] + both[group + j : group + j + 1])
        readout[here, lanes] = jnp.concatenate(sums, axis=0)

    @pl.when(step == pl.num_programs(0) - 1)
    def _():
        for h in range(heads):
            lanes = slice(width * h, width * (h + 1))
            r = readout[:, lanes]
            r = r * lax.rsqrt(jnp.mean(r * r, axis=1, keepdims=True) + epsilon) * gain[...]
            mixed[:, lanes] = (r * gate[:, lanes]).astype(bf16)


def state_update(arrived, past, floor, gain):
    count, heads, width, _ = past.shape
    group = 8
    block = pl.BlockSpec((group, heads, width, width), lambda i: (i, 0, 0, 0))
    rows = pltpu.VMEM((count, heads * width), f32)
    return pl.pallas_call(
        state_body,
        grid=(count // group,),
        in_specs=[
            pl.BlockSpec(arrived.shape, lambda i: (0, 0, 0)),
            block,
            pl.BlockSpec((1, heads * width), lambda i: (0, 0)),
            pl.BlockSpec((1, width), lambda i: (0, 0)),
        ],
        out_specs=[block, pl.BlockSpec((count, heads * width), lambda i: (0, 0))],
        out_shape=[
            jax.ShapeDtypeStruct(past.shape, f32),
            jax.ShapeDtypeStruct((count, heads * width), bf16),
        ],
        scratch_shapes=[pltpu.VMEM((heads, width, 4 * count), f32), rows, rows, rows, rows],
        compiler_params=pltpu.CompilerParams(vmem_limit_bytes=14 * 2**20),
        name="state",
    )(arrived, in_hbm(past), floor.reshape(1, -1), gain.reshape(1, -1))


def project_body(block, gain, *refs):
    weights, out = refs[:-1], refs[-1]
    value = block[...].astype(f32)
    rows = value.shape[1]
    normed = (value * jnp.concatenate([gain[...]] * (rows // 128), axis=1)).astype(bf16)
    normed = normed.T
    count, own, _ = out.shape
    for i, w in enumerate(weights):
        part = jnp.dot(normed, w[...], preferred_element_type=f32).astype(bf16)
        out[:, :, 256 * i : 256 * (i + 1)] = part.reshape(count, own, 256)
    squares = jnp.sum(value * value, axis=0, keepdims=True)
    squares = jnp.broadcast_to(squares, (128, rows)).T
    high = squares.astype(bf16)
    low = squares - high.astype(f32)
    lane = lax.broadcasted_iota(jnp.int32, squares.shape, 1)
    both = jnp.where(lane < 64, high.astype(f32), low).astype(bf16)
    out[:, :, 1024:1152] = both.reshape(count, own, 128)


def project(block, gain, weights, own_rows):
    width, rows = block.shape
    return pl.pallas_call(
        project_body,
        out_shape=jax.ShapeDtypeStruct((rows // own_rows, own_rows, 4 * width + 128), bf16),
        compiler_params=pltpu.CompilerParams(vmem_limit_bytes=14 * 2**20),
        name="project",
    )(block, jnp.broadcast_to(gain[:, None], (width, 128)), *weights)


def half_step(own, near_w, far_w, gains, near):
    width, rows = own.shape
    half = near.shape[0] // 2
    top, low = slice(0, half), slice(half, 2 * half)
    left_top = shift(near[top], 1)
    right_low = shift(near[low], -1)
    left_low = shift(near[low], 1)
    right_top = shift(near[top], -1)
    left_top, right_low, far_w = lax.optimization_barrier((left_top, right_low, far_w))
    far_top = shift(left_top, 1)
    far_low = shift(right_low, -1)
    early = [
        (near, 0, 0),
        (left_top, 3, 0),
        (right_low, 1, half),
        (left_low, 3, half),
        (right_top, 1, 0),
    ]
    sent = products(early, [0, 3, 1], near_w, far_w, gains)
    sent = products([(far_top, 2, 0), (far_low, 2, half)], [2], near_w, far_w, gains, sent)
    got = other_core(sent)
    scale = lax.rsqrt((sent[4 * PAD] + got[4 * PAD]) / D + epsilon)[None, :]
    own_acc = sent[: 2 * PAD] + got[2 * PAD : 4 * PAD]
    far_acc = sent[2 * PAD : 4 * PAD] + got[: 2 * PAD]
    hidden = jnp.concatenate(
        [
            (jax.nn.silu(scale * a[:PAD]) * (scale * a[PAD:])).astype(bf16)
            for a in (own_acc, far_acc)
        ],
        axis=0,
    )
    deep = jnp.concatenate([near_w[:, 2], far_w[:, 2]], axis=1)

    sums = {
        k: lax.dot_general(
            deep[k], hidden, (((0,), (0,)), ((), ())), preferred_element_type=f32
        ).astype(bf16)
        for k in (2, 1, 3, 0)
    }
    arrived = [shift(sums[k], k) for k in (2, 1, 3)]
    total = sums[0].astype(f32)
    for piece in arrived:
        total = total + piece.astype(f32)
    total = total.astype(bf16)
    total = plane_exchange(total.reshape(16, width, rows)).astype(f32).sum(axis=0)
    return lax.optimization_barrier((own.astype(f32) + 0.5 * total).astype(bf16))


def plane_gather(own):
    return plane_exchange(jnp.broadcast_to(own, (16, *own.shape))).reshape(-1, own.shape[1])


def per_device(
    tokens,
    past_state,
    pre_gain,
    pre_gate,
    pre_up,
    pre_down,
    mix_gain,
    query_weight,
    forget_weight,
    value_weight,
    output_gate_weight,
    forget_floor,
    head_gain,
    proj_out,
    post_gain,
    post_gate,
    post_up,
    post_down,
):
    tokens = tokens.T
    near = plane_gather(tokens)
    near_w, far_w, gains = order_weights(pre_gain, pre_gate.T, pre_up.T, pre_down)
    near, near_w, far_w = lax.optimization_barrier((near, near_w, far_w))
    first = half_step(tokens, near_w, other_core(far_w), gains, near)

    width = mix_gain.shape[0] // lax.axis_size(KV)
    own_rows, local_heads, head_width, _ = past_state.shape
    gains = lax.dynamic_slice_in_dim(mix_gain, lax.axis_index(KV) * width, width, 0)
    block = copy_for_each(first, TP)
    block = block.reshape(-1, block.shape[2])
    rows = block.shape[1]
    weight_list = (query_weight, forget_weight, value_weight, output_gate_weight)
    sent = project(block, gains, weight_list, own_rows)
    sent, post_gate, post_up, post_down = lax.optimization_barrier(
        (sent, post_gate, post_up, post_down)
    )
    near_w, far_w, gains = order_weights(post_gain, post_gate.T, post_up.T, post_down)
    arrived = exchange(sent, KV)
    far_w = other_core(far_w)
    arrived, near_w = lax.optimization_barrier((arrived, near_w))
    new_state, mixed_in = state_update(arrived, past_state, forget_floor, head_gain)
    gathered = copy_for_each(mixed_in, KV).reshape(rows, local_heads * head_width)
    partials = lax.dot_general(
        proj_out, gathered, (((0,), (1,)), ((), ())), preferred_element_type=f32
    ).astype(bf16)
    mixed_sum = jnp.sum(exchange(partials.reshape(-1, *first.shape), TP).astype(f32), axis=0)
    second = lax.optimization_barrier((first.astype(f32) + mixed_sum).astype(bf16))
    result = half_step(second, near_w, far_w, gains, plane_gather(second))
    return (result.T, new_state)


def solution(mesh):
    torus = Mesh(mesh.devices.reshape(4, 4, 4, 2), ALL)
    return jax.shard_map(
        per_device,
        mesh=torus,
        in_specs=(
            P(None, ALL),
            P(KV, TP, None, None),
            P(),
            P(None, ALL),
            P(None, ALL),
            P(ALL, None),
            P(),
            P(KV, TP),
            P(KV, TP),
            P(KV, TP),
            P(KV, TP),
            P(TP),
            P(),
            P(TP, KV),
            P(),
            P(None, ALL),
            P(None, ALL),
            P(ALL, None),
        ),
        out_specs=(P(None, ALL), P(KV, TP, None, None)),
        check_vma=False,
    )
```

```python
import functools

import jax
import jax.numpy as jnp
from jax import lax
from jax.experimental import pallas as pl
from jax.experimental.pallas import tpu as pltpu
from jax.sharding import Mesh
from jax.sharding import PartitionSpec as P

D = 4096
ALL = ("z", "y", "x", "c")
KV = ("z", "y")
TP = ("x", "c")
epsilon = 1e-06
f32 = jnp.float32
bf16 = jnp.bfloat16


def copy_for_each(value, axes):
    copies = jnp.broadcast_to(value, (lax.axis_size(axes), *value.shape))
    return lax.all_to_all(copies, axes, split_axis=0, concat_axis=0, tiled=True)


def exchange(pieces, axes):
    return lax.all_to_all(pieces, axes, split_axis=0, concat_axis=0, tiled=True)


def other_core(value):
    return lax.ppermute(value, "c", [(0, 1), (1, 0)])


def dot_t(left, right):
    return lax.dot_general(left, right, (((1,), (0,)), ((), ())), preferred_element_type=f32)


def device(z, y, x, c):
    return ((z % 4 * 4 + y % 4) * 4 + x % 4) * 2 + c


PLACES = [(z, y, x, c) for z in range(4) for y in range(4) for x in range(4) for c in range(2)]
PLANES = [[device(z, m, x, 0) for z in range(4) for m in range(4)] for x in range(4)] + [
    [device(z, y, m, 1) for z in range(4) for m in range(4)] for y in range(4)
]


def shift(value, steps):
    pairs = [
        (device(z, y, x, c), device(z, y, x + steps, c) if c == 0 else device(z, y + steps, x, c))
        for z, y, x, c in PLACES
    ]
    return lax.ppermute(value, ALL, pairs)


def shift_x(value, steps):
    pairs = [(device(z, y, x, c), device(z, y, x + steps, c)) for z, y, x, c in PLACES]
    return lax.ppermute(value, ALL, pairs)


def plane_exchange(pieces):
    return lax.all_to_all(
        pieces, ALL, split_axis=0, concat_axis=0, axis_index_groups=PLANES, tiled=True
    )


PAD = 96


def in_hbm(value):
    return pltpu.with_memory_space_constraint(value, pltpu.HBM)


def sources(core):
    out = lax.broadcasted_iota(jnp.int32, (1, 512), 1)
    chunk, place, column = out // 128, out // 32 % 4, out % 32
    far_x = (lax.axis_index("x") + chunk) % 4
    far_y = (lax.axis_index("y") + chunk) % 4
    return column + jnp.where(
        core == 0, place * 256 + far_x * 64, far_y * 256 + place * 64 + 32
    )


def order_body(mine, theirs, gain, gate, up, down, near, far, gains, rows, picks):
    units = gate.shape[0]

    @pl.when(pl.program_id(0) == 0)
    def _():
        rows[...] = jnp.zeros_like(rows)
        place = lax.broadcasted_iota(jnp.int32, (1024, 512), 0)
        picks[0] = (place == mine[...]).astype(bf16)
        picks[1] = (place == theirs[...]).astype(bf16)

    for j, weight in enumerate((gate, up, down)):
        rows[PAD * j : PAD * j + units, :] = weight[...]
    rest, row = gain[0], lax.broadcasted_iota(jnp.int32, (16, gain.shape[2]), 0)
    split = jnp.zeros(row.shape, f32)
    for i in range(3):
        part = rest.astype(bf16).astype(f32)
        rest = rest - part
        split = jnp.where(row == i, part, split)
    rows[3 * PAD :, :] = split.astype(bf16)
    mine = jnp.dot(rows[...], picks[0], preferred_element_type=f32)
    theirs = jnp.dot(rows[: 3 * PAD, :], picks[1], preferred_element_type=f32)
    for chosen, out in ((mine, near), (theirs, far)):
        chosen = chosen[: 3 * PAD].astype(bf16)
        for k in range(4):
            for j in range(3):
                out[k, j] = chosen[PAD * j : PAD * (j + 1), 128 * k : 128 * (k + 1)]
    line = jnp.sum(mine[3 * PAD : 3 * PAD + 8], axis=0, keepdims=True)
    line = jnp.broadcast_to(line, (128, line.shape[1]))
    for k in range(4):
        gains[k] = line[:, 128 * k : 128 * (k + 1)].T


def order_weights(gain, gate, up, down):
    core = lax.axis_index("c")
    units = gate.shape[0]
    whole = pl.BlockSpec((1, 512), lambda z: (0, 0))
    piece = pl.BlockSpec((units, 1024), lambda z: (0, z))
    side = pl.BlockSpec((4, 3, PAD, 128), lambda z: (0, 0, 0, z))
    shape = jax.ShapeDtypeStruct((4, 3, PAD, 512), bf16)
    return pl.pallas_call(
        order_body,
        grid=(4,),
        in_specs=[
            whole,
            whole,
            pl.BlockSpec((1, 1, 1024), lambda z: (z, 0, 0)),
            piece,
            piece,
            piece,
        ],
        out_specs=[side, side, pl.BlockSpec((4, 128, 128), lambda z: (0, z, 0))],
        out_shape=[shape, shape, jax.ShapeDtypeStruct((4, 512, 128), f32)],
        scratch_shapes=[pltpu.VMEM((3 * PAD + 16, 1024), bf16), pltpu.VMEM((2, 1024, 512), bf16)],
        cost_estimate=pl.CostEstimate(flops=5 * 10**9, bytes_accessed=6 * 10**6, transcendentals=0),
        compiler_params=pltpu.CompilerParams(vmem_limit_bytes=20 * 2**20),
        name="order",
    )(sources(core), sources(1 - core), gain.reshape(4, 1, 1024), *(in_hbm(w) for w in (gate, up, down)))


def product_body(*refs, parts, starts):
    chunks = len(starts)
    pieces, refs = refs[: len(parts)], refs[len(parts) :]
    nears, fars, gains = refs[:chunks], refs[chunks : 2 * chunks], refs[2 * chunks : 3 * chunks]
    if len(refs) > 3 * chunks + 2:
        before, out, normed = refs[3 * chunks :]
    else:
        before, (out, normed) = None, refs[3 * chunks :]
    squares = 0.0
    for piece, (chunk, first) in zip(pieces, parts, strict=True):
        count, rows = piece.shape
        value = piece[...].astype(f32)
        squares = squares + jnp.sum(value * value, axis=0, keepdims=True)
        gain = gains[chunk][0, first : first + count, :]
        gain = jnp.concatenate([gain] * (rows // 128), axis=1)
        normed[512 * chunk + first : 512 * chunk + first + count, :] = (value * gain).astype(bf16)
    for side, weights in enumerate((nears, fars)):
        weights = jnp.concatenate([w[0].reshape(2 * PAD, 512) for w in weights], axis=1)
        total = jnp.dot(weights, normed[...], preferred_element_type=f32)
        where = slice(2 * PAD * side, 2 * PAD * (side + 1))
        out[where, :] = total if before is None else before[where, :] + total
    squares = jnp.broadcast_to(squares, (8, squares.shape[1]))
    where = slice(4 * PAD, 4 * PAD + 8)
    out[where, :] = squares if before is None else before[where, :] + squares


def products(pieces, chunks, near, far, gains, before=None):
    rows = pieces[0][0].shape[1]
    parts = tuple((chunks.index(k), first) for _, k, first in pieces)
    operands = [p for p, _, _ in pieces]
    specs = [pl.BlockSpec(p.shape, lambda i: (0, 0)) for p in operands]
    for weights in (near, far):
        for k in chunks:
            operands.append(weights)
            specs.append(pl.BlockSpec((1, 2, PAD, 512), lambda i, k=k: (k, 0, 0, 0)))
    for k in chunks:
        operands.append(gains)
        specs.append(pl.BlockSpec((1, 512, 128), lambda i, k=k: (k, 0, 0)))
    height = 4 * PAD + 8
    if before is not None:
        operands.append(before)
        specs.append(pl.BlockSpec((height, rows), lambda i: (0, 0)))
    return pl.pallas_call(
        functools.partial(product_body, parts=parts, starts=chunks),
        grid=(1,),
        in_specs=specs,
        out_specs=pl.BlockSpec((height, rows), lambda i: (0, 0)),
        out_shape=jax.ShapeDtypeStruct((height, rows), f32),
        scratch_shapes=[pltpu.VMEM((512 * len(chunks), rows), bf16)],
        cost_estimate=pl.CostEstimate(
            flops=len(chunks) * 4 * 10**8, bytes_accessed=len(chunks) * 10**6, transcendentals=0
        ),
        compiler_params=pltpu.CompilerParams(vmem_limit_bytes=16 * 2**20),
        name="products",
    )(*operands)


def readout_body(arrived, past, floor, gain, mixed, forget, value, query, gate, readout):
    step = pl.program_id(0)
    group, heads, width, _ = past.shape

    @pl.when(step == 0)
    def _():
        total = arrived[0].astype(f32)
        for i in range(1, arrived.shape[0]):
            total = total + arrived[i].astype(f32)
        inner = heads * width
        squares = total[:, 4 * inner : 4 * inner + 1] + total[:, 4 * inner + 64 : 4 * inner + 65]
        total = total[:, : 4 * inner] * lax.rsqrt(squares / D + epsilon)
        query[...] = jax.nn.silu(total[:, :inner])
        value[...] = total[:, 2 * inner : 3 * inner]
        gate[...] = jax.nn.silu(total[:, 3 * inner :])
        bound = floor[...]
        forget[...] = bound + (1.0 - bound) * jax.nn.sigmoid(total[:, inner : 2 * inner])

    here = pl.ds(pl.multiple_of(group * step, group), group)
    for h in range(heads):
        lanes = slice(width * h, width * (h + 1))
        keep, ask = forget[here, lanes], query[here, lanes]
        both = keep * ask
        high = both.astype(bf16).astype(f32)
        both = jnp.concatenate([high, both - high], axis=0).astype(bf16)
        sums = []
        for j in range(group):
            state = past[j, h]
            top = state.astype(bf16)
            low = (state - top.astype(f32)).astype(bf16)
            dots = jnp.dot(both, top, preferred_element_type=f32) + jnp.dot(
                both, low, preferred_element_type=f32
            )
            sums.append(dots[j : j + 1] + dots[group + j : group + j + 1])
        share = jnp.sum((1.0 - keep) * ask, axis=1, keepdims=True)
        readout[here, lanes] = jnp.concatenate(sums, axis=0) + share * value[here, lanes]

    @pl.when(step == pl.num_programs(0) - 1)
    def _():
        for h in range(heads):
            lanes = slice(width * h, width * (h + 1))
            r = readout[:, lanes]
            r = r * lax.rsqrt(jnp.mean(r * r, axis=1, keepdims=True) + epsilon) * gain[...]
            mixed[:, lanes] = (r * gate[:, lanes]).astype(bf16)


def read_out(arrived, past, floor, gain):
    count, heads, width, _ = past.shape
    inner, group = heads * width, 8
    rows = pltpu.VMEM((count, inner), f32)
    table = jax.ShapeDtypeStruct((count, inner), f32)
    whole = pl.BlockSpec((count, inner), lambda i: (0, 0))
    return pl.pallas_call(
        readout_body,
        grid=(count // group,),
        in_specs=[
            pl.BlockSpec(arrived.shape, lambda i: (0, 0, 0)),
            pl.BlockSpec((group, heads, width, width), lambda i: (i, 0, 0, 0)),
            pl.BlockSpec((1, inner), lambda i: (0, 0)),
            pl.BlockSpec((1, width), lambda i: (0, 0)),
        ],
        out_specs=[whole, whole, whole],
        out_shape=[jax.ShapeDtypeStruct((count, inner), bf16), table, table],
        scratch_shapes=[rows, rows, rows],
        compiler_params=pltpu.CompilerParams(vmem_limit_bytes=12 * 2**20),
        name="readout",
    )(arrived, in_hbm(past), floor.reshape(1, -1), gain.reshape(1, -1))


def state_body(forget, value, past, new, columns):
    step = pl.program_id(0)
    group, heads, width, _ = past.shape
    count = forget.shape[0]

    @pl.when(step == 0)
    def _():
        for h in range(heads):
            table = forget[:, width * h : width * (h + 1)]
            columns[h] = jnp.concatenate([table] * 4, axis=0).T

    here = pl.ds(pl.multiple_of(group * step, group), group)
    for h in range(heads):
        near = pltpu.roll(columns[h], lax.rem(4 * count - group * step, 4 * count), axis=1)
        values = value[here, width * h : width * (h + 1)]
        for j in range(group):
            keep = jnp.broadcast_to(near[:, j : j + 1], (width, width))
            added = values[j : j + 1, :]
            new[j, h] = added + keep * (past[j, h] - added)


def update_state(forget, value, past):
    count, heads, width, _ = past.shape
    group = 8
    block = pl.BlockSpec((group, heads, width, width), lambda i: (i, 0, 0, 0))
    whole = pl.BlockSpec(forget.shape, lambda i: (0, 0))
    return pl.pallas_call(
        state_body,
        grid=(count // group,),
        in_specs=[whole, whole, block],
        out_specs=block,
        out_shape=jax.ShapeDtypeStruct(past.shape, f32),
        scratch_shapes=[pltpu.VMEM((heads, width, 4 * count), f32)],
        compiler_params=pltpu.CompilerParams(vmem_limit_bytes=12 * 2**20),
        cost_estimate=pl.CostEstimate(
            flops=4 * 10**9, bytes_accessed=8 * 10**6, transcendentals=0
        ),
        name="state",
    )(forget, value, in_hbm(past))


def project_body(place, gain, *refs):
    pieces, weights, (out, block) = refs[:4], refs[4:-2], refs[-2:]
    width, rows = pieces[0].shape[0] // 2, pieces[0].shape[1]
    for k, piece in enumerate(pieces):
        first = lax.rem(place[0] + k, 4) * 2 * width
        for side in range(2):
            row = pl.multiple_of(first + lax.rem(place[1] + side, 2) * width, width)
            block[pl.ds(row, width), :] = piece[width * side : width * (side + 1), :]
    value = block[...].astype(f32)
    normed = (value * jnp.concatenate([gain[...]] * (rows // 128), axis=1)).astype(bf16)
    normed = normed.T
    count, own, _ = out.shape
    for i, w in enumerate(weights):
        part = jnp.dot(normed, w[...], preferred_element_type=f32).astype(bf16)
        out[:, :, 256 * i : 256 * (i + 1)] = part.reshape(count, own, 256)
    squares = jnp.sum(value * value, axis=0, keepdims=True)
    squares = jnp.broadcast_to(squares, (128, rows)).T
    high = squares.astype(bf16)
    low = squares - high.astype(f32)
    lane = lax.broadcasted_iota(jnp.int32, squares.shape, 1)
    both = jnp.where(lane < 64, high.astype(f32), low).astype(bf16)
    out[:, :, 1024:1152] = both.reshape(count, own, 128)


def in_smem():
    return pl.BlockSpec(memory_space=pltpu.SMEM)


def place_on_tp():
    return jnp.stack([lax.axis_index("x"), lax.axis_index("c")]).astype(jnp.int32)


def project(pieces, gain, weights, own_rows):
    rows, width = pieces[0].shape[1], gain.shape[0]
    operands = [jnp.broadcast_to(gain[:, None], (width, 128)), *pieces, *weights]
    return pl.pallas_call(
        project_body,
        in_specs=[in_smem()] + [pl.BlockSpec(v.shape, lambda: (0, 0)) for v in operands],
        out_shape=jax.ShapeDtypeStruct((rows // own_rows, own_rows, 4 * width + 128), bf16),
        scratch_shapes=[pltpu.VMEM((width, rows), bf16)],
        compiler_params=pltpu.CompilerParams(vmem_limit_bytes=14 * 2**20),
        name="project",
    )(place_on_tp(), *operands)


def output_body(place, gathered, weight, mine, theirs, block):
    width = mine.shape[1]
    block[...] = lax.dot_general(
        weight[...].T, gathered[...], (((1,), (1,)), ((), ())), preferred_element_type=f32
    )
    for k in range(4):
        first = lax.rem(place[0] + k, 4) * 2 * width
        for side, out in enumerate((mine, theirs)):
            row = pl.multiple_of(first + lax.rem(place[1] + side, 2) * width, width)
            out[k] = block[pl.ds(row, width), :].astype(bf16)


def project_out(gathered, weight):
    rows, width = gathered.shape[0], weight.shape[1]
    shape = jax.ShapeDtypeStruct((4, width // 8, rows), bf16)
    return pl.pallas_call(
        output_body,
        in_specs=[in_smem()] + [pl.BlockSpec(v.shape, lambda: (0, 0)) for v in (gathered, weight)],
        out_shape=[shape, shape],
        scratch_shapes=[pltpu.VMEM((width, rows), f32)],
        compiler_params=pltpu.CompilerParams(vmem_limit_bytes=10 * 2**20),
        name="output",
    )(place_on_tp(), gathered, weight)


def half_step(own, near_w, far_w, gains, near):
    width, rows = own.shape
    half = near.shape[0] // 2
    top, low = slice(0, half), slice(half, 2 * half)
    left_top = shift(near[top], 1)
    right_low = shift(near[low], -1)
    left_low = shift(near[low], 1)
    right_top = shift(near[top], -1)
    left_top, right_low, far_w = lax.optimization_barrier((left_top, right_low, far_w))
    far_top = shift(left_top, 1)
    far_low = shift(right_low, -1)
    early = [
        (near, 0, 0),
        (left_top, 3, 0),
        (right_low, 1, half),
        (left_low, 3, half),
        (right_top, 1, 0),
    ]
    sent = products(early, [0, 3, 1], near_w, far_w, gains)
    sent = products([(far_top, 2, 0), (far_low, 2, half)], [2], near_w, far_w, gains, sent)
    got = other_core(sent)
    scale = lax.rsqrt((sent[4 * PAD] + got[4 * PAD]) / D + epsilon)[None, :]
    own_acc = sent[: 2 * PAD] + got[2 * PAD : 4 * PAD]
    far_acc = sent[2 * PAD : 4 * PAD] + got[: 2 * PAD]
    hidden = jnp.concatenate(
        [
            (jax.nn.silu(scale * a[:PAD]) * (scale * a[PAD:])).astype(bf16)
            for a in (own_acc, far_acc)
        ],
        axis=0,
    )
    deep = jnp.concatenate([near_w[:, 2], far_w[:, 2]], axis=1)

    sums = {
        k: lax.dot_general(
            deep[k], hidden, (((0,), (0,)), ((), ())), preferred_element_type=f32
        ).astype(bf16)
        for k in (2, 1, 3, 0)
    }
    arrived = [shift(sums[k], k) for k in (2, 1, 3)]
    total = sums[0].astype(f32)
    for piece in arrived:
        total = total + piece.astype(f32)
    total = total.astype(bf16)
    total = plane_exchange(total.reshape(16, width, rows)).astype(f32).sum(axis=0)
    return lax.optimization_barrier((own.astype(f32) + 0.5 * total).astype(bf16))


def plane_gather(own):
    return plane_exchange(jnp.broadcast_to(own, (16, *own.shape))).reshape(-1, own.shape[1])


def per_device(
    tokens,
    past_state,
    pre_gain,
    pre_gate,
    pre_up,
    pre_down,
    mix_gain,
    query_weight,
    forget_weight,
    value_weight,
    output_gate_weight,
    forget_floor,
    head_gain,
    proj_out,
    post_gain,
    post_gate,
    post_up,
    post_down,
):
    tokens = tokens.T
    near = plane_gather(tokens)
    near_w, far_w, gains = order_weights(pre_gain, pre_gate.T, pre_up.T, pre_down)
    near, near_w, far_w = lax.optimization_barrier((near, near_w, far_w))
    first = half_step(tokens, near_w, other_core(far_w), gains, near)

    width = mix_gain.shape[0] // lax.axis_size(KV)
    own_rows, local_heads, head_width, _ = past_state.shape
    gains = lax.dynamic_slice_in_dim(mix_gain, lax.axis_index(KV) * width, width, 0)
    pair = jnp.concatenate([first, other_core(first)], axis=0)
    pieces = [pair] + [shift_x(pair, -k) for k in (1, 2, 3)]
    weight_list = (query_weight, forget_weight, value_weight, output_gate_weight)
    sent = project(pieces, gains, weight_list, own_rows)
    sent, post_gate, post_up, post_down = lax.optimization_barrier(
        (sent, post_gate, post_up, post_down)
    )
    near_w, far_w, gains = order_weights(post_gain, post_gate.T, post_up.T, post_down)
    arrived = exchange(sent, KV)
    far_w = other_core(far_w)
    arrived, near_w = lax.optimization_barrier((arrived, near_w))
    mixed_in, forget, value = read_out(arrived, past_state, forget_floor, head_gain)
    new_state = update_state(forget, value, past_state)
    gathered = copy_for_each(mixed_in, KV).reshape(-1, mixed_in.shape[1])
    gathered, new_state = lax.optimization_barrier((gathered, new_state))
    mine, theirs = project_out(gathered, proj_out)
    mixed = (mine.astype(f32) + other_core(theirs).astype(f32)).astype(bf16)
    mixed_sum = mixed[0].astype(f32)
    for piece in [shift_x(mixed[k], k) for k in (2, 1, 3)]:
        mixed_sum = mixed_sum + piece.astype(f32)
    second = lax.optimization_barrier((first.astype(f32) + mixed_sum).astype(bf16))
    result = half_step(second, near_w, far_w, gains, plane_gather(second))
    return (result.T, new_state)


def solution(mesh):
    torus = Mesh(mesh.devices.reshape(4, 4, 4, 2), ALL)
    return jax.shard_map(
        per_device,
        mesh=torus,
        in_specs=(
            P(None, ALL),
            P(KV, TP, None, None),
            P(),
            P(None, ALL),
            P(None, ALL),
            P(ALL, None),
            P(),
            P(KV, TP),
            P(KV, TP),
            P(KV, TP),
            P(KV, TP),
            P(TP),
            P(),
            P(TP, KV),
            P(),
            P(None, ALL),
            P(None, ALL),
            P(ALL, None),
        ),
        out_specs=(P(None, ALL), P(KV, TP, None, None)),
        check_vma=False,
    )
```

```python
import functools

import jax
import jax.numpy as jnp
from jax import lax
from jax.experimental import pallas as pl
from jax.experimental.pallas import tpu as pltpu
from jax.sharding import Mesh
from jax.sharding import PartitionSpec as P


D = 4096
ALL = ("z", "y", "x", "c")
KV = ("z", "y")
TP = ("x", "c")
epsilon = 1e-06
f32 = jnp.float32
bf16 = jnp.bfloat16


def copy_for_each(value, axes):
    copies = jnp.broadcast_to(value, (lax.axis_size(axes), *value.shape))
    return lax.all_to_all(copies, axes, split_axis=0, concat_axis=0, tiled=True)


def exchange(pieces, axes):
    return lax.all_to_all(pieces, axes, split_axis=0, concat_axis=0, tiled=True)


def other_core(value):
    return lax.ppermute(value, "c", [(0, 1), (1, 0)])


def device(z, y, x, c):
    return ((z % 4 * 4 + y % 4) * 4 + x % 4) * 2 + c


PLACES = [(z, y, x, c) for z in range(4) for y in range(4) for x in range(4) for c in range(2)]
PLANES = [[device(z, m, x, 0) for z in range(4) for m in range(4)] for x in range(4)] + [
    [device(z, y, m, 1) for z in range(4) for m in range(4)] for y in range(4)
]


def shift(value, steps):
    pairs = [
        (device(z, y, x, c), device(z, y, x + steps, c) if c == 0 else device(z, y + steps, x, c))
        for z, y, x, c in PLACES
    ]
    return lax.ppermute(value, ALL, pairs)


def shift_x(value, steps):
    pairs = [(device(z, y, x, c), device(z, y, x + steps, c)) for z, y, x, c in PLACES]
    return lax.ppermute(value, ALL, pairs)


def plane_exchange(pieces):
    return lax.all_to_all(
        pieces, ALL, split_axis=0, concat_axis=0, axis_index_groups=PLANES, tiled=True
    )


PAD = 96


def in_hbm(value):
    return pltpu.with_memory_space_constraint(value, pltpu.HBM)


def sources(core):
    out = lax.broadcasted_iota(jnp.int32, (1, 512), 1)
    chunk, place, column = out // 128, out // 32 % 4, out % 32
    far_x = (lax.axis_index("x") + chunk) % 4
    far_y = (lax.axis_index("y") + chunk) % 4
    return column + jnp.where(
        core == 0, place * 256 + far_x * 64, far_y * 256 + place * 64 + 32
    )


def order_body(mine, theirs, gain, gate, up, down, near, far, gains, rows, picks):
    units = gate.shape[0]

    @pl.when(pl.program_id(0) == 0)
    def _():
        rows[...] = jnp.zeros_like(rows)
        place = lax.broadcasted_iota(jnp.int32, (1024, 512), 0)
        picks[0] = (place == mine[...]).astype(bf16)
        picks[1] = (place == theirs[...]).astype(bf16)

    for j, weight in enumerate((gate, up, down)):
        rows[PAD * j : PAD * j + units, :] = weight[...]
    rest, row = gain[0], lax.broadcasted_iota(jnp.int32, (16, gain.shape[2]), 0)
    split = jnp.zeros(row.shape, f32)
    for i in range(3):
        part = rest.astype(bf16).astype(f32)
        rest = rest - part
        split = jnp.where(row == i, part, split)
    rows[3 * PAD :, :] = split.astype(bf16)
    mine = jnp.dot(rows[...], picks[0], preferred_element_type=f32)
    theirs = jnp.dot(rows[: 3 * PAD, :], picks[1], preferred_element_type=f32)
    for chosen, out in ((mine, near), (theirs, far)):
        chosen = chosen[: 3 * PAD].astype(bf16)
        for k in range(4):
            for j in range(3):
                out[k, j] = chosen[PAD * j : PAD * (j + 1), 128 * k : 128 * (k + 1)]
    line = jnp.sum(mine[3 * PAD : 3 * PAD + 8], axis=0, keepdims=True)
    line = jnp.broadcast_to(line, (128, line.shape[1]))
    for k in range(4):
        gains[k] = line[:, 128 * k : 128 * (k + 1)].T


def order_weights(gain, gate, up, down):
    core = lax.axis_index("c")
    units = gate.shape[0]
    whole = pl.BlockSpec((1, 512), lambda z: (0, 0))
    piece = pl.BlockSpec((units, 1024), lambda z: (0, z))
    side = pl.BlockSpec((4, 3, PAD, 128), lambda z: (0, 0, 0, z))
    shape = jax.ShapeDtypeStruct((4, 3, PAD, 512), bf16)
    return pl.pallas_call(
        order_body,
        grid=(4,),
        in_specs=[
            whole,
            whole,
            pl.BlockSpec((1, 1, 1024), lambda z: (z, 0, 0)),
            piece,
            piece,
            piece,
        ],
        out_specs=[side, side, pl.BlockSpec((4, 128, 128), lambda z: (0, z, 0))],
        out_shape=[shape, shape, jax.ShapeDtypeStruct((4, 512, 128), f32)],
        scratch_shapes=[pltpu.VMEM((3 * PAD + 16, 1024), bf16), pltpu.VMEM((2, 1024, 512), bf16)],
        cost_estimate=pl.CostEstimate(flops=5 * 10**9, bytes_accessed=6 * 10**6, transcendentals=0),
        compiler_params=pltpu.CompilerParams(vmem_limit_bytes=20 * 2**20),
        name="order",
    )(sources(core), sources(1 - core), gain.reshape(4, 1, 1024), *(in_hbm(w) for w in (gate, up, down)))


def product_body(*refs, parts, starts, more):
    chunks = len(starts)
    pieces, refs = refs[: len(parts)], refs[len(parts) :]
    nears, fars, gains = refs[:chunks], refs[chunks : 2 * chunks], refs[2 * chunks : 3 * chunks]
    before, out, away, normed = refs[3 * chunks :] if more else (None, refs[-2], None, refs[-1])
    squares = 0.0
    for piece, (chunk, first) in zip(pieces, parts, strict=True):
        count, rows = piece.shape
        value = piece[...].astype(f32)
        squares = squares + jnp.sum(value * value, axis=0, keepdims=True)
        gain = gains[chunk][0, first : first + count, :]
        gain = jnp.concatenate([gain] * (rows // 128), axis=1)
        normed[512 * chunk + first : 512 * chunk + first + count, :] = (value * gain).astype(bf16)
    for side, weights in enumerate((nears, fars)):
        weights = jnp.concatenate([w[0].reshape(2 * PAD, 512) for w in weights], axis=1)
        total = jnp.dot(weights, normed[...], preferred_element_type=f32)
        where = slice(2 * PAD * side, 2 * PAD * (side + 1))
        if more:
            total = before[where, :] + total
            away[where, :] = total.astype(bf16)
        out[where, :] = total
    squares = jnp.broadcast_to(squares, (8, squares.shape[1]))
    where = slice(4 * PAD, 4 * PAD + 8)
    if more:
        squares = before[where, :] + squares
        high = squares.astype(bf16).astype(f32)
        away[4 * PAD :, :] = jnp.concatenate([high, squares - high], axis=0).astype(bf16)
    out[where, :] = squares


def products(pieces, chunks, near, far, gains, before=None):
    rows = pieces[0][0].shape[1]
    parts = tuple((chunks.index(k), first) for _, k, first in pieces)
    operands = [p for p, _, _ in pieces]
    specs = [pl.BlockSpec(p.shape, lambda i: (0, 0)) for p in operands]
    for weights in (near, far):
        for k in chunks:
            operands.append(weights)
            specs.append(pl.BlockSpec((1, 2, PAD, 512), lambda i, k=k: (k, 0, 0, 0)))
    for k in chunks:
        operands.append(gains)
        specs.append(pl.BlockSpec((1, 512, 128), lambda i, k=k: (k, 0, 0)))
    outs = [jax.ShapeDtypeStruct((4 * PAD + 8, rows), f32)]
    if before is not None:
        operands.append(before)
        specs.append(pl.BlockSpec(before.shape, lambda i: (0, 0)))
        outs.append(jax.ShapeDtypeStruct((4 * PAD + 16, rows), bf16))
    return pl.pallas_call(
        functools.partial(product_body, parts=parts, starts=chunks, more=before is not None),
        grid=(1,),
        in_specs=specs,
        out_specs=[pl.BlockSpec(o.shape, lambda i: (0, 0)) for o in outs],
        out_shape=outs,
        scratch_shapes=[pltpu.VMEM((512 * len(chunks), rows), bf16)],
        cost_estimate=pl.CostEstimate(
            flops=len(chunks) * 4 * 10**8, bytes_accessed=len(chunks) * 10**6, transcendentals=0
        ),
        compiler_params=pltpu.CompilerParams(vmem_limit_bytes=16 * 2**20),
        name="products",
    )(*operands)


def readout_body(arrived, past, floor, gain, mixed, forget, value, query, gate, readout):
    step = pl.program_id(0)
    group, heads, width, _ = past.shape

    @pl.when(step == 0)
    def _():
        total = arrived[0].astype(f32)
        for i in range(1, arrived.shape[0]):
            total = total + arrived[i].astype(f32)
        inner = heads * width
        squares = total[:, 4 * inner : 4 * inner + 1] + total[:, 4 * inner + 64 : 4 * inner + 65]
        total = total[:, : 4 * inner] * lax.rsqrt(squares / D + epsilon)
        query[...] = jax.nn.silu(total[:, :inner])
        value[...] = total[:, 2 * inner : 3 * inner]
        gate[...] = jax.nn.silu(total[:, 3 * inner :])
        bound = floor[...]
        forget[...] = bound + (1.0 - bound) * jax.nn.sigmoid(total[:, inner : 2 * inner])

    here = pl.ds(pl.multiple_of(group * step, group), group)
    for h in range(heads):
        lanes = slice(width * h, width * (h + 1))
        keep, ask = forget[here, lanes], query[here, lanes]
        both = keep * ask
        high = both.astype(bf16).astype(f32)
        both = jnp.concatenate([high, both - high], axis=0).astype(bf16)
        sums = []
        for j in range(group):
            state = past[j, h]
            top = state.astype(bf16)
            low = (state - top.astype(f32)).astype(bf16)
            dots = jnp.dot(both, top, preferred_element_type=f32) + jnp.dot(
                both, low, preferred_element_type=f32
            )
            sums.append(dots[j : j + 1] + dots[group + j : group + j + 1])
        share = jnp.sum((1.0 - keep) * ask, axis=1, keepdims=True)
        readout[here, lanes] = jnp.concatenate(sums, axis=0) + share * value[here, lanes]

    @pl.when(step == pl.num_programs(0) - 1)
    def _():
        for h in range(heads):
            lanes = slice(width * h, width * (h + 1))
            r = readout[:, lanes]
            r = r * lax.rsqrt(jnp.mean(r * r, axis=1, keepdims=True) + epsilon) * gain[...]
            mixed[:, lanes] = (r * gate[:, lanes]).astype(bf16)


def read_out(arrived, past, floor, gain):
    count, heads, width, _ = past.shape
    inner, group = heads * width, 8
    rows = pltpu.VMEM((count, inner), f32)
    table = jax.ShapeDtypeStruct((count, inner), f32)
    whole = pl.BlockSpec((count, inner), lambda i: (0, 0))
    return pl.pallas_call(
        readout_body,
        grid=(count // group,),
        in_specs=[
            pl.BlockSpec(arrived.shape, lambda i: (0, 0, 0)),
            pl.BlockSpec((group, heads, width, width), lambda i: (i, 0, 0, 0)),
            pl.BlockSpec((1, inner), lambda i: (0, 0)),
            pl.BlockSpec((1, width), lambda i: (0, 0)),
        ],
        out_specs=[whole, whole, whole],
        out_shape=[jax.ShapeDtypeStruct((count, inner), bf16), table, table],
        scratch_shapes=[rows, rows, rows],
        compiler_params=pltpu.CompilerParams(vmem_limit_bytes=12 * 2**20),
        name="readout",
    )(arrived, in_hbm(past), floor.reshape(1, -1), gain.reshape(1, -1))


def state_body(forget, value, past, new, columns):
    step = pl.program_id(0)
    group, heads, width, _ = past.shape
    count = forget.shape[0]

    @pl.when(step == 0)
    def _():
        for h in range(heads):
            table = forget[:, width * h : width * (h + 1)]
            columns[h] = jnp.concatenate([table] * 4, axis=0).T

    here = pl.ds(pl.multiple_of(group * step, group), group)
    for h in range(heads):
        near = pltpu.roll(columns[h], lax.rem(4 * count - group * step, 4 * count), axis=1)
        values = value[here, width * h : width * (h + 1)]
        for j in range(group):
            keep = jnp.broadcast_to(near[:, j : j + 1], (width, width))
            added = values[j : j + 1, :]
            new[j, h] = added + keep * (past[j, h] - added)


def update_state(forget, value, past):
    count, heads, width, _ = past.shape
    group = 8
    block = pl.BlockSpec((group, heads, width, width), lambda i: (i, 0, 0, 0))
    whole = pl.BlockSpec(forget.shape, lambda i: (0, 0))
    return pl.pallas_call(
        state_body,
        grid=(count // group,),
        in_specs=[whole, whole, block],
        out_specs=block,
        out_shape=jax.ShapeDtypeStruct(past.shape, f32),
        scratch_shapes=[pltpu.VMEM((heads, width, 4 * count), f32)],
        compiler_params=pltpu.CompilerParams(vmem_limit_bytes=12 * 2**20),
        cost_estimate=pl.CostEstimate(
            flops=4 * 10**9, bytes_accessed=8 * 10**6, transcendentals=0
        ),
        name="state",
    )(forget, value, in_hbm(past))


def project_body(place, gain, *refs):
    pieces, weights, (out, block) = refs[:4], refs[4:-2], refs[-2:]
    width, rows = pieces[0].shape[0] // 2, pieces[0].shape[1]
    for k, piece in enumerate(pieces):
        first = lax.rem(place[0] + k, 4) * 2 * width
        for side in range(2):
            row = pl.multiple_of(first + lax.rem(place[1] + side, 2) * width, width)
            block[pl.ds(row, width), :] = piece[width * side : width * (side + 1), :]
    value = block[...].astype(f32)
    normed = (value * jnp.concatenate([gain[...]] * (rows // 128), axis=1)).astype(bf16)
    normed = normed.T
    count, own, _ = out.shape
    for i, w in enumerate(weights):
        part = jnp.dot(normed, w[...], preferred_element_type=f32).astype(bf16)
        out[:, :, 256 * i : 256 * (i + 1)] = part.reshape(count, own, 256)
    squares = jnp.sum(value * value, axis=0, keepdims=True)
    high = squares.astype(bf16).astype(f32)
    line = lax.broadcasted_iota(jnp.int32, (128, rows), 0)
    both = jnp.where(line < 64, high, squares - high).astype(bf16).T
    out[:, :, 1024:1152] = both.reshape(count, own, 128)


def in_smem():
    return pl.BlockSpec(memory_space=pltpu.SMEM)


def place_on_tp():
    return jnp.stack([lax.axis_index("x"), lax.axis_index("c")]).astype(jnp.int32)


def project(pieces, gain, weights, own_rows):
    rows, width = pieces[0].shape[1], gain.shape[0]
    operands = [jnp.broadcast_to(gain[:, None], (width, 128)), *pieces, *weights]
    return pl.pallas_call(
        project_body,
        in_specs=[in_smem()] + [pl.BlockSpec(v.shape, lambda: (0, 0)) for v in operands],
        out_shape=jax.ShapeDtypeStruct((rows // own_rows, own_rows, 4 * width + 128), bf16),
        scratch_shapes=[pltpu.VMEM((width, rows), bf16)],
        compiler_params=pltpu.CompilerParams(vmem_limit_bytes=14 * 2**20),
        name="project",
    )(place_on_tp(), *operands)


def output_body(place, gathered, weight, mine, theirs, block):
    width = mine.shape[1]
    block[...] = lax.dot_general(
        weight[...].T, gathered[...], (((1,), (1,)), ((), ())), preferred_element_type=f32
    )
    for k in range(4):
        first = lax.rem(place[0] + k, 4) * 2 * width
        for side, out in enumerate((mine, theirs)):
            row = pl.multiple_of(first + lax.rem(place[1] + side, 2) * width, width)
            out[k] = block[pl.ds(row, width), :].astype(bf16)


def project_out(gathered, weight):
    rows, width = gathered.shape[0], weight.shape[1]
    shape = jax.ShapeDtypeStruct((4, width // 8, rows), bf16)
    return pl.pallas_call(
        output_body,
        in_specs=[in_smem()] + [pl.BlockSpec(v.shape, lambda: (0, 0)) for v in (gathered, weight)],
        out_shape=[shape, shape],
        scratch_shapes=[pltpu.VMEM((width, rows), f32)],
        compiler_params=pltpu.CompilerParams(vmem_limit_bytes=10 * 2**20),
        name="output",
    )(place_on_tp(), gathered, weight)


def half_step(own, near_w, far_w, gains, near):
    width, rows = own.shape
    half = near.shape[0] // 2
    top, low = slice(0, half), slice(half, 2 * half)
    left_top = shift(near[top], 1)
    right_low = shift(near[low], -1)
    left_low = shift(near[low], 1)
    right_top = shift(near[top], -1)
    left_top, right_low, far_w = lax.optimization_barrier((left_top, right_low, far_w))
    far_top = shift(left_top, 1)
    far_low = shift(right_low, -1)
    early = [
        (near, 0, 0),
        (left_top, 3, 0),
        (right_low, 1, half),
        (left_low, 3, half),
        (right_top, 1, 0),
    ]
    (acc,) = products(early, [0, 3, 1], near_w, far_w, gains)
    late = [(far_top, 2, 0), (far_low, 2, half)]
    acc, away = products(late, [2], near_w, far_w, gains, acc)
    got = other_core(away).astype(f32)
    squares = acc[4 * PAD] + got[4 * PAD] + got[4 * PAD + 8]
    scale = lax.rsqrt(squares / D + epsilon)[None, :]
    own_acc = acc[: 2 * PAD] + got[2 * PAD : 4 * PAD]
    far_acc = acc[2 * PAD : 4 * PAD] + got[: 2 * PAD]
    hidden = jnp.concatenate(
        [
            (jax.nn.silu(scale * a[:PAD]) * (scale * a[PAD:])).astype(bf16)
            for a in (own_acc, far_acc)
        ],
        axis=0,
    )
    deep = jnp.concatenate([near_w[:, 2], far_w[:, 2]], axis=1)

    sums, arrived = {}, []
    for k in (2, 1, 3, 0):
        sums[k] = lax.dot_general(
            deep[k], hidden, (((0,), (0,)), ((), ())), preferred_element_type=f32
        ).astype(bf16)
        if k:
            arrived.append(shift(sums[k], k))
    total = sums[0].astype(f32)
    for piece in arrived:
        total = total + piece.astype(f32)
    total = total.astype(bf16)
    total = plane_exchange(total.reshape(16, width, rows)).astype(f32).sum(axis=0)
    return lax.optimization_barrier((own.astype(f32) + 0.5 * total).astype(bf16))


def plane_gather(own):
    return plane_exchange(jnp.broadcast_to(own, (16, *own.shape))).reshape(-1, own.shape[1])


def per_device(
    tokens,
    past_state,
    pre_gain,
    pre_gate,
    pre_up,
    pre_down,
    mix_gain,
    query_weight,
    forget_weight,
    value_weight,
    output_gate_weight,
    forget_floor,
    head_gain,
    proj_out,
    post_gain,
    post_gate,
    post_up,
    post_down,
):
    tokens = tokens.T
    near = plane_gather(tokens)
    near_w, far_w, gains = order_weights(pre_gain, pre_gate.T, pre_up.T, pre_down)
    near, near_w, far_w = lax.optimization_barrier((near, near_w, far_w))
    first = half_step(tokens, near_w, other_core(far_w), gains, near)

    width = mix_gain.shape[0] // lax.axis_size(KV)
    own_rows, _, _, _ = past_state.shape
    gains = lax.dynamic_slice_in_dim(mix_gain, lax.axis_index(KV) * width, width, 0)
    pair = jnp.concatenate([first, other_core(first)], axis=0)
    pieces = [pair] + [shift_x(pair, -k) for k in (1, 2, 3)]
    weight_list = (query_weight, forget_weight, value_weight, output_gate_weight)
    sent = project(pieces, gains, weight_list, own_rows)
    sent, post_gate, post_up, post_down = lax.optimization_barrier(
        (sent, post_gate, post_up, post_down)
    )
    near_w, far_w, gains = order_weights(post_gain, post_gate.T, post_up.T, post_down)
    arrived = exchange(sent, KV)
    arrived, near_w = lax.optimization_barrier((arrived, near_w))
    mixed_in, forget, value = read_out(arrived, past_state, forget_floor, head_gain)
    new_state = update_state(forget, value, past_state)
    gathered = copy_for_each(mixed_in, KV).reshape(-1, mixed_in.shape[1])
    gathered, new_state = lax.optimization_barrier((gathered, new_state))
    mine, theirs = project_out(gathered, proj_out)
    mixed = (mine.astype(f32) + other_core(theirs).astype(f32)).astype(bf16)
    mixed_sum = mixed[0].astype(f32)
    for piece in [shift_x(mixed[k], k) for k in (2, 1, 3)]:
        mixed_sum = mixed_sum + piece.astype(f32)
    second = lax.optimization_barrier((first.astype(f32) + mixed_sum).astype(bf16))
    near = plane_gather(second)
    near, far_w = lax.optimization_barrier((near, far_w))
    far_w = other_core(far_w)
    result = half_step(second, near_w, far_w, gains, near)
    return (result.T, new_state)


def solution(mesh):
    torus = Mesh(mesh.devices.reshape(4, 4, 4, 2), ALL)
    return jax.shard_map(
        per_device,
        mesh=torus,
        in_specs=(
            P(None, ALL),
            P(KV, TP, None, None),
            P(),
            P(None, ALL),
            P(None, ALL),
            P(ALL, None),
            P(),
            P(KV, TP),
            P(KV, TP),
            P(KV, TP),
            P(KV, TP),
            P(TP),
            P(),
            P(TP, KV),
            P(),
            P(None, ALL),
            P(None, ALL),
            P(ALL, None),
        ),
        out_specs=(P(None, ALL), P(KV, TP, None, None)),
        check_vma=False,
    )
```

```python
import functools

import jax
import jax.numpy as jnp
from jax import lax
from jax.experimental import pallas as pl
from jax.experimental.pallas import tpu as pltpu
from jax.sharding import Mesh
from jax.sharding import PartitionSpec as P


D = 4096
ALL = ("z", "y", "x", "c")
KV = ("z", "y")
TP = ("x", "c")
epsilon = 1e-06
f32 = jnp.float32
bf16 = jnp.bfloat16


def copy_for_each(value, axes):
    copies = jnp.broadcast_to(value, (lax.axis_size(axes), *value.shape))
    return lax.all_to_all(copies, axes, split_axis=0, concat_axis=0, tiled=True)


def exchange(pieces, axes):
    return lax.all_to_all(pieces, axes, split_axis=0, concat_axis=0, tiled=True)


def other_core(value):
    return lax.ppermute(value, "c", [(0, 1), (1, 0)])


def device(z, y, x, c):
    return ((z % 4 * 4 + y % 4) * 4 + x % 4) * 2 + c


PLACES = [(z, y, x, c) for z in range(4) for y in range(4) for x in range(4) for c in range(2)]
PLANES = [[device(z, m, x, 0) for z in range(4) for m in range(4)] for x in range(4)] + [
    [device(z, y, m, 1) for z in range(4) for m in range(4)] for y in range(4)
]


def shift(value, steps):
    pairs = [
        (device(z, y, x, c), device(z, y, x + steps, c) if c == 0 else device(z, y + steps, x, c))
        for z, y, x, c in PLACES
    ]
    return lax.ppermute(value, ALL, pairs)


def shift_x(value, steps):
    pairs = [(device(z, y, x, c), device(z, y, x + steps, c)) for z, y, x, c in PLACES]
    return lax.ppermute(value, ALL, pairs)


def plane_exchange(pieces):
    return lax.all_to_all(
        pieces, ALL, split_axis=0, concat_axis=0, axis_index_groups=PLANES, tiled=True
    )


PAD = 96


def in_hbm(value):
    return pltpu.with_memory_space_constraint(value, pltpu.HBM)


def sources(core):
    out = lax.broadcasted_iota(jnp.int32, (1, 512), 1)
    chunk, place, column = out // 128, out // 32 % 4, out % 32
    far_x = (lax.axis_index("x") + chunk) % 4
    far_y = (lax.axis_index("y") + chunk) % 4
    return column + jnp.where(
        core == 0, place * 256 + far_x * 64, far_y * 256 + place * 64 + 32
    )


def order_body(mine, theirs, gain, gate, up, down, near, far, gains, rows, picks):
    units = gate.shape[0]

    @pl.when(pl.program_id(0) == 0)
    def _():
        rows[...] = jnp.zeros_like(rows)
        place = lax.broadcasted_iota(jnp.int32, (1024, 512), 0)
        picks[0] = (place == mine[...]).astype(bf16)
        picks[1] = (place == theirs[...]).astype(bf16)

    for j, weight in enumerate((gate, up, down)):
        rows[PAD * j : PAD * j + units, :] = weight[...]
    rest, row = gain[0], lax.broadcasted_iota(jnp.int32, (16, gain.shape[2]), 0)
    split = jnp.zeros(row.shape, f32)
    for i in range(3):
        part = rest.astype(bf16).astype(f32)
        rest = rest - part
        split = jnp.where(row == i, part, split)
    rows[3 * PAD :, :] = split.astype(bf16)
    mine = jnp.dot(rows[...], picks[0], preferred_element_type=f32)
    theirs = jnp.dot(rows[: 3 * PAD, :], picks[1], preferred_element_type=f32)
    for chosen, out in ((mine, near), (theirs, far)):
        chosen = chosen[: 3 * PAD].astype(bf16)
        for k in range(4):
            for j in range(3):
                out[k, j] = chosen[PAD * j : PAD * (j + 1), 128 * k : 128 * (k + 1)]
    line = jnp.sum(mine[3 * PAD : 3 * PAD + 8], axis=0, keepdims=True)
    line = jnp.broadcast_to(line, (128, line.shape[1]))
    for k in range(4):
        gains[k] = line[:, 128 * k : 128 * (k + 1)].T


def order_weights(gain, gate, up, down):
    core = lax.axis_index("c")
    units = gate.shape[0]
    whole = pl.BlockSpec((1, 512), lambda z: (0, 0))
    piece = pl.BlockSpec((units, 1024), lambda z: (0, z))
    side = pl.BlockSpec((4, 3, PAD, 128), lambda z: (0, 0, 0, z))
    shape = jax.ShapeDtypeStruct((4, 3, PAD, 512), bf16)
    return pl.pallas_call(
        order_body,
        grid=(4,),
        in_specs=[
            whole,
            whole,
            pl.BlockSpec((1, 1, 1024), lambda z: (z, 0, 0)),
            piece,
            piece,
            piece,
        ],
        out_specs=[side, side, pl.BlockSpec((4, 128, 128), lambda z: (0, z, 0))],
        out_shape=[shape, shape, jax.ShapeDtypeStruct((4, 512, 128), f32)],
        scratch_shapes=[pltpu.VMEM((3 * PAD + 16, 1024), bf16), pltpu.VMEM((2, 1024, 512), bf16)],
        cost_estimate=pl.CostEstimate(flops=5 * 10**9, bytes_accessed=6 * 10**6, transcendentals=0),
        compiler_params=pltpu.CompilerParams(vmem_limit_bytes=20 * 2**20),
        name="order",
    )(sources(core), sources(1 - core), gain.reshape(4, 1, 1024), *(in_hbm(w) for w in (gate, up, down)))


def product_body(*refs, parts, starts, more):
    chunks = len(starts)
    pieces, refs = refs[: len(parts)], refs[len(parts) :]
    nears, fars, gains = refs[:chunks], refs[chunks : 2 * chunks], refs[2 * chunks : 3 * chunks]
    before, out, away, normed = refs[3 * chunks :] if more else (None, refs[-2], None, refs[-1])
    squares = 0.0
    for piece, (chunk, first) in zip(pieces, parts, strict=True):
        count, rows = piece.shape
        value = piece[...].astype(f32)
        squares = squares + jnp.sum(value * value, axis=0, keepdims=True)
        gain = gains[chunk][0, first : first + count, :]
        gain = jnp.concatenate([gain] * (rows // 128), axis=1)
        normed[512 * chunk + first : 512 * chunk + first + count, :] = (value * gain).astype(bf16)
    for side, weights in enumerate((nears, fars)):
        weights = jnp.concatenate([w[0].reshape(2 * PAD, 512) for w in weights], axis=1)
        total = jnp.dot(weights, normed[...], preferred_element_type=f32)
        where = slice(2 * PAD * side, 2 * PAD * (side + 1))
        if more:
            total = before[where, :] + total
            away[where, :] = total.astype(bf16)
        out[where, :] = total
    squares = jnp.broadcast_to(squares, (8, squares.shape[1]))
    where = slice(4 * PAD, 4 * PAD + 8)
    if more:
        squares = before[where, :] + squares
        high = squares.astype(bf16).astype(f32)
        away[4 * PAD :, :] = jnp.concatenate([high, squares - high], axis=0).astype(bf16)
    out[where, :] = squares


def products(pieces, chunks, near, far, gains, before=None):
    rows = pieces[0][0].shape[1]
    parts = tuple((chunks.index(k), first) for _, k, first in pieces)
    operands = [p for p, _, _ in pieces]
    specs = [pl.BlockSpec(p.shape, lambda i: (0, 0)) for p in operands]
    for weights in (near, far):
        for k in chunks:
            operands.append(weights)
            specs.append(pl.BlockSpec((1, 2, PAD, 512), lambda i, k=k: (k, 0, 0, 0)))
    for k in chunks:
        operands.append(gains)
        specs.append(pl.BlockSpec((1, 512, 128), lambda i, k=k: (k, 0, 0)))
    outs = [jax.ShapeDtypeStruct((4 * PAD + 8, rows), f32)]
    if before is not None:
        operands.append(before)
        specs.append(pl.BlockSpec(before.shape, lambda i: (0, 0)))
        outs.append(jax.ShapeDtypeStruct((4 * PAD + 16, rows), bf16))
    return pl.pallas_call(
        functools.partial(product_body, parts=parts, starts=chunks, more=before is not None),
        grid=(1,),
        in_specs=specs,
        out_specs=[pl.BlockSpec(o.shape, lambda i: (0, 0)) for o in outs],
        out_shape=outs,
        scratch_shapes=[pltpu.VMEM((512 * len(chunks), rows), bf16)],
        cost_estimate=pl.CostEstimate(
            flops=len(chunks) * 4 * 10**8, bytes_accessed=len(chunks) * 10**6, transcendentals=0
        ),
        compiler_params=pltpu.CompilerParams(vmem_limit_bytes=16 * 2**20),
        name="products",
    )(*operands)


def chunk_copies(source, target, sems, outward=False):
    copies = []
    for i in range(target.shape[0] // 8):
        rows = pl.ds(8 * i, 8)
        ends = (target.at[rows], source.at[rows]) if outward else (source.at[rows], target.at[rows])
        copies.append(pltpu.make_async_copy(*ends, sems.at[i]))
    return copies


def readout_body(arrived, past, floor, gain, mixed, forget, value, query, gate, states, sems):
    copies = chunk_copies(past, states, sems)
    for copy in copies:
        copy.start()
    heads, width = past.shape[1:3]
    inner = heads * width
    total = arrived[0].astype(f32)
    for i in range(1, arrived.shape[0]):
        total = total + arrived[i].astype(f32)
    squares = total[:, 4 * inner : 4 * inner + 1] + total[:, 4 * inner + 64 : 4 * inner + 65]
    total = total[:, : 4 * inner] * lax.rsqrt(squares / D + epsilon)
    query[...] = jax.nn.silu(total[:, :inner])
    value[...] = total[:, 2 * inner : 3 * inner]
    gate[...] = jax.nn.silu(total[:, 3 * inner :])
    bound = floor[...]
    forget[...] = bound + (1.0 - bound) * jax.nn.sigmoid(total[:, inner : 2 * inner])
    for i, copy in enumerate(copies):
        copy.wait()
        here = slice(8 * i, 8 * (i + 1))
        for h in range(heads):
            lanes = slice(width * h, width * (h + 1))
            keep, ask = forget[here, lanes], query[here, lanes]
            both = keep * ask
            high = both.astype(bf16).astype(f32)
            both = jnp.concatenate([high, both - high], axis=0).astype(bf16)
            sums = []
            for j in range(8):
                state = states[8 * i + j, h]
                top = state.astype(bf16)
                low = (state - top.astype(f32)).astype(bf16)
                dots = jnp.dot(both, top, preferred_element_type=f32) + jnp.dot(
                    both, low, preferred_element_type=f32
                )
                sums.append(dots[j : j + 1] + dots[8 + j : 8 + j + 1])
            share = jnp.sum((1.0 - keep) * ask, axis=1, keepdims=True)
            r = jnp.concatenate(sums, axis=0) + share * value[here, lanes]
            r = r * lax.rsqrt(jnp.mean(r * r, axis=1, keepdims=True) + epsilon) * gain[...]
            query[here, lanes] = r * gate[here, lanes]
    mixed[...] = query[...].astype(bf16)


def read_out(arrived, past, floor, gain):
    count, heads, width, _ = past.shape
    inner = heads * width
    rows = pltpu.VMEM((count, inner), f32)
    table = jax.ShapeDtypeStruct((count, inner), f32)
    return pl.pallas_call(
        readout_body,
        in_specs=[
            pl.BlockSpec(arrived.shape, lambda: (0, 0, 0)),
            pl.BlockSpec(memory_space=pl.ANY),
            pl.BlockSpec((1, inner), lambda: (0, 0)),
            pl.BlockSpec((1, width), lambda: (0, 0)),
        ],
        out_shape=[jax.ShapeDtypeStruct((count, inner), bf16), table, table],
        scratch_shapes=[
            rows,
            rows,
            pltpu.VMEM(past.shape, f32),
            pltpu.SemaphoreType.DMA((count // 8,)),
        ],
        compiler_params=pltpu.CompilerParams(vmem_limit_bytes=14 * 2**20),
        name="readout",
    )(arrived, in_hbm(past), floor.reshape(1, -1), gain.reshape(1, -1))


def state_body(forget, value, past, new, columns, states, arrivals, departures):
    copies = chunk_copies(past, states, arrivals)
    for copy in copies:
        copy.start()
    count, heads, width, _ = past.shape
    for h in range(heads):
        table = forget[:, width * h : width * (h + 1)]
        columns[h] = jnp.concatenate([table] * (width // count), axis=0).T
    leaving = chunk_copies(new, states, departures, outward=True)
    for i, copy in enumerate(copies):
        copy.wait()
        for h in range(heads):
            near = columns[h]
            for j in range(8 * i, 8 * (i + 1)):
                keep = jnp.broadcast_to(near[:, j : j + 1], (width, width))
                added = value[j : j + 1, width * h : width * (h + 1)]
                states[j, h] = added + keep * (states[j, h] - added)
        leaving[i].start()
    for copy in leaving:
        copy.wait()


def update_state(forget, value, past):
    count, heads, width, _ = past.shape
    whole = pl.BlockSpec(forget.shape, lambda: (0, 0))
    sems = pltpu.SemaphoreType.DMA((count // 8,))
    return pl.pallas_call(
        state_body,
        in_specs=[whole, whole, pl.BlockSpec(memory_space=pl.ANY)],
        out_specs=pl.BlockSpec(memory_space=pl.ANY),
        out_shape=jax.ShapeDtypeStruct(past.shape, f32),
        scratch_shapes=[
            pltpu.VMEM((heads, width, width), f32),
            pltpu.VMEM(past.shape, f32),
            sems,
            sems,
        ],
        compiler_params=pltpu.CompilerParams(vmem_limit_bytes=12 * 2**20),
        cost_estimate=pl.CostEstimate(
            flops=4 * 10**9, bytes_accessed=8 * 10**6, transcendentals=0
        ),
        name="state",
    )(forget, value, in_hbm(past))


def project_body(gain, *refs):
    place = lax.axis_index("x"), lax.axis_index("c")
    pieces, weights, (out, block) = refs[:4], refs[4:-2], refs[-2:]
    width, rows = pieces[0].shape[0] // 2, pieces[0].shape[1]
    for k, piece in enumerate(pieces):
        first = lax.rem(place[0] + k, 4) * 2 * width
        for side in range(2):
            row = pl.multiple_of(first + lax.rem(place[1] + side, 2) * width, width)
            block[pl.ds(row, width), :] = piece[width * side : width * (side + 1), :]
    value = block[...].astype(f32)
    normed = (value * jnp.concatenate([gain[...]] * (rows // 128), axis=1)).astype(bf16)
    normed = normed.T
    count, own, _ = out.shape
    for i, w in enumerate(weights):
        part = jnp.dot(normed, w[...], preferred_element_type=f32).astype(bf16)
        out[:, :, 256 * i : 256 * (i + 1)] = part.reshape(count, own, 256)
    squares = jnp.sum(value * value, axis=0, keepdims=True)
    high = squares.astype(bf16).astype(f32)
    line = lax.broadcasted_iota(jnp.int32, (128, rows), 0)
    both = jnp.where(line < 64, high, squares - high).astype(bf16).T
    out[:, :, 1024:1152] = both.reshape(count, own, 128)


def project(pieces, gain, weights, own_rows):
    rows, width = pieces[0].shape[1], gain.shape[0]
    operands = [jnp.broadcast_to(gain[:, None], (width, 128)), *pieces, *weights]
    return pl.pallas_call(
        project_body,
        in_specs=[pl.BlockSpec(v.shape, lambda: (0, 0)) for v in operands],
        out_shape=jax.ShapeDtypeStruct((rows // own_rows, own_rows, 4 * width + 128), bf16),
        scratch_shapes=[pltpu.VMEM((width, rows), bf16)],
        compiler_params=pltpu.CompilerParams(vmem_limit_bytes=14 * 2**20),
        name="project",
    )(*operands)


def output_body(gathered, weight, mine, theirs, block):
    place = lax.axis_index("x"), lax.axis_index("c")
    width = mine.shape[1]
    block[...] = lax.dot_general(
        weight[...].T, gathered[...], (((1,), (1,)), ((), ())), preferred_element_type=f32
    )
    for k in range(4):
        first = lax.rem(place[0] + k, 4) * 2 * width
        for side, out in enumerate((mine, theirs)):
            row = pl.multiple_of(first + lax.rem(place[1] + side, 2) * width, width)
            out[k] = block[pl.ds(row, width), :].astype(bf16)


def project_out(gathered, weight):
    rows, width = gathered.shape[0], weight.shape[1]
    shape = jax.ShapeDtypeStruct((4, width // 8, rows), bf16)
    return pl.pallas_call(
        output_body,
        in_specs=[pl.BlockSpec(v.shape, lambda: (0, 0)) for v in (gathered, weight)],
        out_shape=[shape, shape],
        scratch_shapes=[pltpu.VMEM((width, rows), f32)],
        compiler_params=pltpu.CompilerParams(vmem_limit_bytes=10 * 2**20),
        name="output",
    )(gathered, weight)


def half_step(own, near_w, far_w, gains, near):
    width, rows = own.shape
    half = near.shape[0] // 2
    top, low = slice(0, half), slice(half, 2 * half)
    left_top = shift(near[top], 1)
    right_low = shift(near[low], -1)
    left_low = shift(near[low], 1)
    right_top = shift(near[top], -1)
    left_top, right_low, far_w = lax.optimization_barrier((left_top, right_low, far_w))
    far_top = shift(left_top, 1)
    far_low = shift(right_low, -1)
    early = [
        (near, 0, 0),
        (left_top, 3, 0),
        (right_low, 1, half),
        (left_low, 3, half),
        (right_top, 1, 0),
    ]
    (acc,) = products(early, [0, 3, 1], near_w, far_w, gains)
    late = [(far_top, 2, 0), (far_low, 2, half)]
    acc, away = products(late, [2], near_w, far_w, gains, acc)
    got = other_core(away).astype(f32)
    squares = acc[4 * PAD] + got[4 * PAD] + got[4 * PAD + 8]
    scale = lax.rsqrt(squares / D + epsilon)[None, :]
    own_acc = acc[: 2 * PAD] + got[2 * PAD : 4 * PAD]
    far_acc = acc[2 * PAD : 4 * PAD] + got[: 2 * PAD]
    hidden = jnp.concatenate(
        [
            (jax.nn.silu(scale * a[:PAD]) * (scale * a[PAD:])).astype(bf16)
            for a in (own_acc, far_acc)
        ],
        axis=0,
    )
    deep = jnp.concatenate([near_w[:, 2], far_w[:, 2]], axis=1)

    sums, arrived = {}, []
    for k in (2, 1, 3, 0):
        sums[k] = lax.dot_general(
            deep[k], hidden, (((0,), (0,)), ((), ())), preferred_element_type=f32
        ).astype(bf16)
        if k:
            arrived.append(shift(sums[k], k))
    total = sums[0].astype(f32)
    for piece in arrived:
        total = total + piece.astype(f32)
    total = total.astype(bf16)
    total = plane_exchange(total.reshape(16, width, rows)).astype(f32).sum(axis=0)
    return lax.optimization_barrier((own.astype(f32) + 0.5 * total).astype(bf16))


def plane_gather(own):
    return plane_exchange(jnp.broadcast_to(own, (16, *own.shape))).reshape(-1, own.shape[1])


def per_device(
    tokens,
    past_state,
    pre_gain,
    pre_gate,
    pre_up,
    pre_down,
    mix_gain,
    query_weight,
    forget_weight,
    value_weight,
    output_gate_weight,
    forget_floor,
    head_gain,
    proj_out,
    post_gain,
    post_gate,
    post_up,
    post_down,
):
    tokens = tokens.T
    near = plane_gather(tokens)
    near_w, far_w, gains = order_weights(pre_gain, pre_gate.T, pre_up.T, pre_down)
    near, near_w, far_w = lax.optimization_barrier((near, near_w, far_w))
    first = half_step(tokens, near_w, other_core(far_w), gains, near)

    width = mix_gain.shape[0] // lax.axis_size(KV)
    own_rows, _, _, _ = past_state.shape
    gains = lax.dynamic_slice_in_dim(mix_gain, lax.axis_index(KV) * width, width, 0)
    pair = jnp.concatenate([first, other_core(first)], axis=0)
    pieces = [pair] + [shift_x(pair, -k) for k in (1, 2, 3)]
    weight_list = (query_weight, forget_weight, value_weight, output_gate_weight)
    sent = project(pieces, gains, weight_list, own_rows)
    sent, post_gate, post_up, post_down = lax.optimization_barrier(
        (sent, post_gate, post_up, post_down)
    )
    near_w, far_w, gains = order_weights(post_gain, post_gate.T, post_up.T, post_down)
    arrived = exchange(sent, KV)
    arrived, near_w = lax.optimization_barrier((arrived, near_w))
    mixed_in, forget, value = read_out(arrived, past_state, forget_floor, head_gain)
    new_state = update_state(forget, value, past_state)
    gathered = copy_for_each(mixed_in, KV).reshape(-1, mixed_in.shape[1])
    gathered, new_state = lax.optimization_barrier((gathered, new_state))
    mine, theirs = project_out(gathered, proj_out)
    mixed = (mine.astype(f32) + other_core(theirs).astype(f32)).astype(bf16)
    mixed_sum = mixed[0].astype(f32)
    for piece in [shift_x(mixed[k], k) for k in (2, 1, 3)]:
        mixed_sum = mixed_sum + piece.astype(f32)
    second = lax.optimization_barrier((first.astype(f32) + mixed_sum).astype(bf16))
    near = plane_gather(second)
    near, far_w = lax.optimization_barrier((near, far_w))
    far_w = other_core(far_w)
    result = half_step(second, near_w, far_w, gains, near)
    return (result.T, new_state)


def solution(mesh):
    torus = Mesh(mesh.devices.reshape(4, 4, 4, 2), ALL)
    return jax.shard_map(
        per_device,
        mesh=torus,
        in_specs=(
            P(None, ALL),
            P(KV, TP, None, None),
            P(),
            P(None, ALL),
            P(None, ALL),
            P(ALL, None),
            P(),
            P(KV, TP),
            P(KV, TP),
            P(KV, TP),
            P(KV, TP),
            P(TP),
            P(),
            P(TP, KV),
            P(),
            P(None, ALL),
            P(None, ALL),
            P(ALL, None),
        ),
        out_specs=(P(None, ALL), P(KV, TP, None, None)),
        check_vma=False,
    )
```

```python
import functools

import jax
import jax.numpy as jnp
from jax import lax
from jax.experimental import pallas as pl
from jax.experimental.pallas import tpu as pltpu
from jax.sharding import Mesh
from jax.sharding import PartitionSpec as P

D = 4096
ALL = ("z", "y", "x", "c")
KV = ("z", "y")
TP = ("x", "c")
epsilon = 1e-06
f32 = jnp.float32
bf16 = jnp.bfloat16


def copy_for_each(value, axes):
    copies = jnp.broadcast_to(value, (lax.axis_size(axes), *value.shape))
    return lax.all_to_all(copies, axes, split_axis=0, concat_axis=0, tiled=True)


def exchange(pieces, axes):
    return lax.all_to_all(pieces, axes, split_axis=0, concat_axis=0, tiled=True)


def other_core(value):
    return lax.ppermute(value, "c", [(0, 1), (1, 0)])


def device(z, y, x, c):
    return ((z % 4 * 4 + y % 4) * 4 + x % 4) * 2 + c


PLACES = [(z, y, x, c) for z in range(4) for y in range(4) for x in range(4) for c in range(2)]
PLANES = [[device(z, m, x, 0) for z in range(4) for m in range(4)] for x in range(4)] + [
    [device(z, y, m, 1) for z in range(4) for m in range(4)] for y in range(4)
]


def shift(value, steps):
    pairs = [
        (device(z, y, x, c), device(z, y, x + steps, c) if c == 0 else device(z, y + steps, x, c))
        for z, y, x, c in PLACES
    ]
    return lax.ppermute(value, ALL, pairs)


def shift_x(value, steps):
    pairs = [(device(z, y, x, c), device(z, y, x + steps, c)) for z, y, x, c in PLACES]
    return lax.ppermute(value, ALL, pairs)


def plane_exchange(pieces):
    return lax.all_to_all(
        pieces, ALL, split_axis=0, concat_axis=0, axis_index_groups=PLANES, tiled=True
    )


PAD = 96


def in_hbm(value):
    return pltpu.with_memory_space_constraint(value, pltpu.HBM)


def sources(core):
    out = lax.broadcasted_iota(jnp.int32, (1, 512), 1)
    chunk, place, column = out // 128, out // 32 % 4, out % 32
    far_x = (lax.axis_index("x") + chunk) % 4
    far_y = (lax.axis_index("y") + chunk) % 4
    return column + jnp.where(
        core == 0, place * 256 + far_x * 64, far_y * 256 + place * 64 + 32
    )


def order_body(mine, theirs, gain, gate, up, down, near, far, gains, rows, picks):
    units = gate.shape[0]

    @pl.when(pl.program_id(0) == 0)
    def _():
        rows[...] = jnp.zeros_like(rows)
        place = lax.broadcasted_iota(jnp.int32, (1024, 512), 0)
        picks[0] = (place == mine[...]).astype(bf16)
        picks[1] = (place == theirs[...]).astype(bf16)

    for j, weight in enumerate((gate, up, down)):
        rows[PAD * j : PAD * j + units, :] = weight[...]
    rest, row = gain[0], lax.broadcasted_iota(jnp.int32, (16, gain.shape[2]), 0)
    split = jnp.zeros(row.shape, f32)
    for i in range(3):
        part = rest.astype(bf16).astype(f32)
        rest = rest - part
        split = jnp.where(row == i, part, split)
    rows[3 * PAD :, :] = split.astype(bf16)
    mine = jnp.dot(rows[...], picks[0], preferred_element_type=f32)
    theirs = jnp.dot(rows[: 3 * PAD, :], picks[1], preferred_element_type=f32)
    for chosen, out in ((mine, near), (theirs, far)):
        chosen = chosen[: 3 * PAD].astype(bf16)
        for k in range(4):
            for j in range(3):
                out[k, j] = chosen[PAD * j : PAD * (j + 1), 128 * k : 128 * (k + 1)]
    line = jnp.sum(mine[3 * PAD : 3 * PAD + 8], axis=0, keepdims=True)
    line = jnp.broadcast_to(line, (128, line.shape[1]))
    for k in range(4):
        gains[k] = line[:, 128 * k : 128 * (k + 1)].T


def order_weights(gain, gate, up, down):
    core = lax.axis_index("c")
    units = gate.shape[0]
    whole = pl.BlockSpec((1, 512), lambda z: (0, 0))
    piece = pl.BlockSpec((units, 1024), lambda z: (0, z))
    side = pl.BlockSpec((4, 3, PAD, 128), lambda z: (0, 0, 0, z))
    shape = jax.ShapeDtypeStruct((4, 3, PAD, 512), bf16)
    return pl.pallas_call(
        order_body,
        grid=(4,),
        in_specs=[
            whole,
            whole,
            pl.BlockSpec((1, 1, 1024), lambda z: (z, 0, 0)),
            piece,
            piece,
            piece,
        ],
        out_specs=[side, side, pl.BlockSpec((4, 128, 128), lambda z: (0, z, 0))],
        out_shape=[shape, pltpu.HBM(shape.shape, bf16), jax.ShapeDtypeStruct((4, 512, 128), f32)],
        scratch_shapes=[pltpu.VMEM((3 * PAD + 16, 1024), bf16), pltpu.VMEM((2, 1024, 512), bf16)],
        cost_estimate=pl.CostEstimate(flops=5 * 10**9, bytes_accessed=6 * 10**6, transcendentals=0),
        compiler_params=pltpu.CompilerParams(vmem_limit_bytes=20 * 2**20),
        name="order",
    )(sources(core), sources(1 - core), gain.reshape(4, 1, 1024), *(in_hbm(w) for w in (gate, up, down)))


def product_body(*refs, parts, starts, more):
    chunks = len(starts)
    pieces, refs = refs[: len(parts)], refs[len(parts) :]
    nears, fars, gains = refs[:chunks], refs[chunks : 2 * chunks], refs[2 * chunks : 3 * chunks]
    before, out, away, normed = refs[3 * chunks :] if more else (None, refs[-2], None, refs[-1])
    squares = 0.0
    for piece, (chunk, first) in zip(pieces, parts, strict=True):
        count, rows = piece.shape
        value = piece[...].astype(f32)
        squares = squares + jnp.sum(value * value, axis=0, keepdims=True)
        gain = gains[chunk][0, first : first + count, :]
        gain = jnp.concatenate([gain] * (rows // 128), axis=1)
        normed[512 * chunk + first : 512 * chunk + first + count, :] = (value * gain).astype(bf16)
    for side, weights in enumerate((nears, fars)):
        weights = jnp.concatenate([w[0].reshape(2 * PAD, 512) for w in weights], axis=1)
        total = jnp.dot(weights, normed[...], preferred_element_type=f32)
        where = slice(2 * PAD * side, 2 * PAD * (side + 1))
        if more:
            total = before[where, :] + total
            away[where, :] = total.astype(bf16)
        out[where, :] = total
    squares = jnp.broadcast_to(squares, (8, squares.shape[1]))
    where = slice(4 * PAD, 4 * PAD + 8)
    if more:
        squares = before[where, :] + squares
        high = squares.astype(bf16).astype(f32)
        away[4 * PAD :, :] = jnp.concatenate([high, squares - high], axis=0).astype(bf16)
    out[where, :] = squares


def products(pieces, chunks, near, far, gains, before=None):
    rows = pieces[0][0].shape[1]
    parts = tuple((chunks.index(k), first) for _, k, first in pieces)
    operands = [p for p, _, _ in pieces]
    specs = [pl.BlockSpec(p.shape, lambda i: (0, 0)) for p in operands]
    for weights in (near, far):
        for k in chunks:
            operands.append(weights)
            specs.append(pl.BlockSpec((1, 2, PAD, 512), lambda i, k=k: (k, 0, 0, 0)))
    for k in chunks:
        operands.append(gains)
        specs.append(pl.BlockSpec((1, 512, 128), lambda i, k=k: (k, 0, 0)))
    outs = [jax.ShapeDtypeStruct((4 * PAD + 8, rows), f32)]
    if before is not None:
        operands.append(before)
        specs.append(pl.BlockSpec(before.shape, lambda i: (0, 0)))
        outs.append(jax.ShapeDtypeStruct((4 * PAD + 16, rows), bf16))
    return pl.pallas_call(
        functools.partial(product_body, parts=parts, starts=chunks, more=before is not None),
        grid=(1,),
        in_specs=specs,
        out_specs=[pl.BlockSpec(o.shape, lambda i: (0, 0)) for o in outs],
        out_shape=outs,
        scratch_shapes=[pltpu.VMEM((512 * len(chunks), rows), bf16)],
        cost_estimate=pl.CostEstimate(
            flops=len(chunks) * 4 * 10**8, bytes_accessed=len(chunks) * 10**6, transcendentals=0
        ),
        compiler_params=pltpu.CompilerParams(vmem_limit_bytes=16 * 2**20),
        name="products",
    )(*operands)


def chunk_copies(source, target, sems, outward=False):
    copies = []
    for i in range(target.shape[0] // 8):
        rows = pl.ds(8 * i, 8)
        ends = (target.at[rows], source.at[rows]) if outward else (source.at[rows], target.at[rows])
        copies.append(pltpu.make_async_copy(*ends, sems.at[i]))
    return copies


def readout_body(arrived, past, floor, gain, mixed, forget, value, query, gate, states, sems):
    copies = chunk_copies(past, states, sems)
    for copy in copies:
        copy.start()
    heads, width = past.shape[1:3]
    inner = heads * width
    total = arrived[0].astype(f32)
    for i in range(1, arrived.shape[0]):
        total = total + arrived[i].astype(f32)
    squares = total[:, 4 * inner : 4 * inner + 1] + total[:, 4 * inner + 64 : 4 * inner + 65]
    total = total[:, : 4 * inner] * lax.rsqrt(squares / D + epsilon)
    query[...] = jax.nn.silu(total[:, :inner])
    value[...] = total[:, 2 * inner : 3 * inner]
    gate[...] = jax.nn.silu(total[:, 3 * inner :])
    bound = floor[...]
    forget[...] = bound + (1.0 - bound) * jax.nn.sigmoid(total[:, inner : 2 * inner])
    for i, copy in enumerate(copies):
        copy.wait()
        here = slice(8 * i, 8 * (i + 1))
        for h in range(heads):
            lanes = slice(width * h, width * (h + 1))
            keep, ask = forget[here, lanes], query[here, lanes]
            both = keep * ask
            high = both.astype(bf16).astype(f32)
            both = jnp.concatenate([high, both - high], axis=0).astype(bf16)
            sums = []
            for j in range(8):
                state = states[8 * i + j, h]
                top = state.astype(bf16)
                low = (state - top.astype(f32)).astype(bf16)
                dots = jnp.dot(both, top, preferred_element_type=f32) + jnp.dot(
                    both, low, preferred_element_type=f32
                )
                sums.append(dots[j : j + 1] + dots[8 + j : 8 + j + 1])
            share = jnp.sum((1.0 - keep) * ask, axis=1, keepdims=True)
            r = jnp.concatenate(sums, axis=0) + share * value[here, lanes]
            r = r * lax.rsqrt(jnp.mean(r * r, axis=1, keepdims=True) + epsilon) * gain[...]
            query[here, lanes] = r * gate[here, lanes]
    mixed[...] = query[...].astype(bf16)


def read_out(arrived, past, floor, gain):
    count, heads, width, _ = past.shape
    inner = heads * width
    rows = pltpu.VMEM((count, inner), f32)
    table = jax.ShapeDtypeStruct((count, inner), f32)
    return pl.pallas_call(
        readout_body,
        in_specs=[
            pl.BlockSpec(arrived.shape, lambda: (0, 0, 0)),
            pl.BlockSpec(memory_space=pl.ANY),
            pl.BlockSpec((1, inner), lambda: (0, 0)),
            pl.BlockSpec((1, width), lambda: (0, 0)),
        ],
        out_shape=[jax.ShapeDtypeStruct((count, inner), bf16), table, table],
        scratch_shapes=[
            rows,
            rows,
            pltpu.VMEM(past.shape, f32),
            pltpu.SemaphoreType.DMA((count // 8,)),
        ],
        compiler_params=pltpu.CompilerParams(vmem_limit_bytes=14 * 2**20),
        name="readout",
    )(arrived, in_hbm(past), floor.reshape(1, -1), gain.reshape(1, -1))


def state_body(forget, value, past, new, columns, states, arrivals, departures):
    copies = chunk_copies(past, states, arrivals)
    for copy in copies:
        copy.start()
    count, heads, width, _ = past.shape
    for h in range(heads):
        table = forget[:, width * h : width * (h + 1)]
        columns[h] = jnp.concatenate([table] * (width // count), axis=0).T
    leaving = chunk_copies(new, states, departures, outward=True)
    for i, copy in enumerate(copies):
        copy.wait()
        for h in range(heads):
            near = columns[h]
            for j in range(8 * i, 8 * (i + 1)):
                keep = jnp.broadcast_to(near[:, j : j + 1], (width, width))
                added = value[j : j + 1, width * h : width * (h + 1)]
                states[j, h] = added + keep * (states[j, h] - added)
        leaving[i].start()
    for copy in leaving:
        copy.wait()


def update_state(forget, value, past):
    count, heads, width, _ = past.shape
    whole = pl.BlockSpec(forget.shape, lambda: (0, 0))
    sems = pltpu.SemaphoreType.DMA((count // 8,))
    return pl.pallas_call(
        state_body,
        in_specs=[whole, whole, pl.BlockSpec(memory_space=pl.ANY)],
        out_specs=pl.BlockSpec(memory_space=pl.ANY),
        out_shape=jax.ShapeDtypeStruct(past.shape, f32),
        scratch_shapes=[
            pltpu.VMEM((heads, width, width), f32),
            pltpu.VMEM(past.shape, f32),
            sems,
            sems,
        ],
        compiler_params=pltpu.CompilerParams(vmem_limit_bytes=12 * 2**20),
        cost_estimate=pl.CostEstimate(
            flops=4 * 10**9, bytes_accessed=8 * 10**6, transcendentals=0
        ),
        name="state",
    )(forget, value, in_hbm(past))


def project_body(gain, *refs):
    place = lax.axis_index("x"), lax.axis_index("c")
    pieces, weights, (out, block) = refs[:4], refs[4:-2], refs[-2:]
    width, rows = pieces[0].shape[0] // 2, pieces[0].shape[1]
    for k, piece in enumerate(pieces):
        first = lax.rem(place[0] + k, 4) * 2 * width
        for side in range(2):
            row = pl.multiple_of(first + lax.rem(place[1] + side, 2) * width, width)
            block[pl.ds(row, width), :] = piece[width * side : width * (side + 1), :]
    value = block[...].astype(f32)
    normed = (value * jnp.concatenate([gain[...]] * (rows // 128), axis=1)).astype(bf16)
    normed = normed.T
    count, own, _ = out.shape
    for i, w in enumerate(weights):
        part = jnp.dot(normed, w[...], preferred_element_type=f32).astype(bf16)
        out[:, :, 256 * i : 256 * (i + 1)] = part.reshape(count, own, 256)
    squares = jnp.sum(value * value, axis=0, keepdims=True)
    high = squares.astype(bf16).astype(f32)
    line = lax.broadcasted_iota(jnp.int32, (128, rows), 0)
    both = jnp.where(line < 64, high, squares - high).astype(bf16).T
    out[:, :, 1024:1152] = both.reshape(count, own, 128)


def project(pieces, gain, weights, own_rows):
    rows, width = pieces[0].shape[1], gain.shape[0]
    operands = [jnp.broadcast_to(gain[:, None], (width, 128)), *pieces, *weights]
    return pl.pallas_call(
        project_body,
        in_specs=[pl.BlockSpec(v.shape, lambda: (0, 0)) for v in operands],
        out_shape=jax.ShapeDtypeStruct((rows // own_rows, own_rows, 4 * width + 128), bf16),
        scratch_shapes=[pltpu.VMEM((width, rows), bf16)],
        compiler_params=pltpu.CompilerParams(vmem_limit_bytes=14 * 2**20),
        name="project",
    )(*operands)


def output_body(gathered, weight, mine, theirs, block):
    place = lax.axis_index("x"), lax.axis_index("c")
    width = mine.shape[1]
    block[...] = lax.dot_general(
        weight[...].T, gathered[...], (((1,), (1,)), ((), ())), preferred_element_type=f32
    )
    for k in range(4):
        first = lax.rem(place[0] + k, 4) * 2 * width
        for side, out in enumerate((mine, theirs)):
            row = pl.multiple_of(first + lax.rem(place[1] + side, 2) * width, width)
            out[k] = block[pl.ds(row, width), :].astype(bf16)


def project_out(gathered, weight):
    rows, width = gathered.shape[0], weight.shape[1]
    shape = jax.ShapeDtypeStruct((4, width // 8, rows), bf16)
    return pl.pallas_call(
        output_body,
        in_specs=[pl.BlockSpec(v.shape, lambda: (0, 0)) for v in (gathered, weight)],
        out_shape=[shape, shape],
        scratch_shapes=[pltpu.VMEM((width, rows), f32)],
        compiler_params=pltpu.CompilerParams(vmem_limit_bytes=10 * 2**20),
        name="output",
    )(gathered, weight)


def half_step(own, near_w, far_w, gains, near):
    width, rows = own.shape
    half = near.shape[0] // 2
    top, low = slice(0, half), slice(half, 2 * half)
    left_top = shift(near[top], 1)
    right_low = shift(near[low], -1)
    left_low = shift(near[low], 1)
    right_top = shift(near[top], -1)
    left_top, right_low, far_w = lax.optimization_barrier((left_top, right_low, far_w))
    far_top = shift(left_top, 1)
    far_low = shift(right_low, -1)
    early = [
        (near, 0, 0),
        (left_top, 3, 0),
        (right_low, 1, half),
        (left_low, 3, half),
        (right_top, 1, 0),
    ]
    (acc,) = products(early, [0, 3, 1], near_w, far_w, gains)
    late = [(far_top, 2, 0), (far_low, 2, half)]
    acc, away = products(late, [2], near_w, far_w, gains, acc)
    got = other_core(away).astype(f32)
    squares = acc[4 * PAD] + got[4 * PAD] + got[4 * PAD + 8]
    scale = lax.rsqrt(squares / D + epsilon)[None, :]
    own_acc = acc[: 2 * PAD] + got[2 * PAD : 4 * PAD]
    far_acc = acc[2 * PAD : 4 * PAD] + got[: 2 * PAD]
    hidden = jnp.concatenate(
        [
            (jax.nn.silu(scale * a[:PAD]) * (scale * a[PAD:])).astype(bf16)
            for a in (own_acc, far_acc)
        ],
        axis=0,
    )
    deep = jnp.concatenate([near_w[:, 2], far_w[:, 2]], axis=1)

    def sums(weights):
        return lax.dot_general(
            weights, hidden, (((0,), (0,)), ((), ())), preferred_element_type=f32
        )

    to_right = jnp.concatenate([deep[2][:, top], deep[1][:, low]], axis=1)
    to_left = jnp.concatenate([deep[2][:, low], deep[3][:, top]], axis=1)
    from_left = shift(sums(to_right).astype(bf16), 1)
    from_right = shift(sums(to_left).astype(bf16), -1)
    next_top, next_low = sums(deep[1][:, top]), sums(deep[3][:, low])
    own_sums = sums(deep[0])
    next_top = shift((next_top + from_left[top].astype(f32)).astype(bf16), 1)
    next_low = shift((next_low + from_right[top].astype(f32)).astype(bf16), -1)
    total = jnp.concatenate(
        [
            own_sums[top] + from_right[low].astype(f32) + next_top.astype(f32),
            own_sums[low] + from_left[low].astype(f32) + next_low.astype(f32),
        ],
        axis=0,
    ).astype(bf16)
    total = plane_exchange(total.reshape(16, width, rows)).astype(f32).sum(axis=0)
    return lax.optimization_barrier((own.astype(f32) + 0.5 * total).astype(bf16))


def plane_gather(own):
    return plane_exchange(jnp.broadcast_to(own, (16, *own.shape))).reshape(-1, own.shape[1])


def per_device(
    tokens,
    past_state,
    pre_gain,
    pre_gate,
    pre_up,
    pre_down,
    mix_gain,
    query_weight,
    forget_weight,
    value_weight,
    output_gate_weight,
    forget_floor,
    head_gain,
    proj_out,
    post_gain,
    post_gate,
    post_up,
    post_down,
):
    tokens = tokens.T
    near = plane_gather(tokens)
    near_w, far_w, gains = order_weights(pre_gain, pre_gate.T, pre_up.T, pre_down)
    near, near_w, far_w = lax.optimization_barrier((near, near_w, far_w))
    first = half_step(tokens, near_w, other_core(far_w), gains, near)

    width = mix_gain.shape[0] // lax.axis_size(KV)
    own_rows, _, _, _ = past_state.shape
    gains = lax.dynamic_slice_in_dim(mix_gain, lax.axis_index(KV) * width, width, 0)
    pair = jnp.concatenate([first, other_core(first)], axis=0)
    pieces = [pair] + [shift_x(pair, -k) for k in (1, 2, 3)]
    weight_list = (query_weight, forget_weight, value_weight, output_gate_weight)
    sent = project(pieces, gains, weight_list, own_rows)
    sent, post_gate, post_up, post_down = lax.optimization_barrier(
        (sent, post_gate, post_up, post_down)
    )
    near_w, far_w, gains = order_weights(post_gain, post_gate.T, post_up.T, post_down)
    arrived = exchange(sent, KV)
    arrived, near_w = lax.optimization_barrier((arrived, near_w))
    mixed_in, forget, value = read_out(arrived, past_state, forget_floor, head_gain)
    new_state = update_state(forget, value, past_state)
    gathered = copy_for_each(mixed_in, KV).reshape(-1, mixed_in.shape[1])
    gathered, new_state = lax.optimization_barrier((gathered, new_state))
    mine, theirs = project_out(gathered, proj_out)
    mixed = (mine.astype(f32) + other_core(theirs).astype(f32)).astype(bf16)
    mixed_sum = mixed[0].astype(f32)
    for piece in [shift_x(mixed[k], k) for k in (2, 1, 3)]:
        mixed_sum = mixed_sum + piece.astype(f32)
    second = lax.optimization_barrier((first.astype(f32) + mixed_sum).astype(bf16))
    near = plane_gather(second)
    near, far_w = lax.optimization_barrier((near, far_w))
    far_w = other_core(far_w)
    result = half_step(second, near_w, far_w, gains, near)
    return (result.T, new_state)


def solution(mesh):
    torus = Mesh(mesh.devices.reshape(4, 4, 4, 2), ALL)
    return jax.shard_map(
        per_device,
        mesh=torus,
        in_specs=(
            P(None, ALL),
            P(KV, TP, None, None),
            P(),
            P(None, ALL),
            P(None, ALL),
            P(ALL, None),
            P(),
            P(KV, TP),
            P(KV, TP),
            P(KV, TP),
            P(KV, TP),
            P(TP),
            P(),
            P(TP, KV),
            P(),
            P(None, ALL),
            P(None, ALL),
            P(ALL, None),
        ),
        out_specs=(P(None, ALL), P(KV, TP, None, None)),
        check_vma=False,
    )
```

```python
import functools

import jax
import jax.numpy as jnp
from jax import lax
from jax.experimental import pallas as pl
from jax.experimental.pallas import tpu as pltpu
from jax.sharding import Mesh
from jax.sharding import PartitionSpec as P


D = 4096
ALL = ("z", "y", "x", "c")
KV = ("z", "y")
TP = ("x", "c")
epsilon = 1e-06
f32 = jnp.float32
bf16 = jnp.bfloat16


def copy_for_each(value, axes):
    copies = jnp.broadcast_to(value, (lax.axis_size(axes), *value.shape))
    return lax.all_to_all(copies, axes, split_axis=0, concat_axis=0, tiled=True)


def other_core(value):
    return lax.ppermute(value, "c", [(0, 1), (1, 0)])


def device(z, y, x, c):
    return ((z % 4 * 4 + y % 4) * 4 + x % 4) * 2 + c


PLACES = [(z, y, x, c) for z in range(4) for y in range(4) for x in range(4) for c in range(2)]
PLANES = [[device(z, m, x, 0) for z in range(4) for m in range(4)] for x in range(4)] + [
    [device(z, y, m, 1) for z in range(4) for m in range(4)] for y in range(4)
]


def shift(value, steps):
    pairs = [
        (device(z, y, x, c), device(z, y, x + steps, c) if c == 0 else device(z, y + steps, x, c))
        for z, y, x, c in PLACES
    ]
    return lax.ppermute(value, ALL, pairs)


def shift_kv(value, steps, stage):
    pairs = [
        (
            device(z, y, x, c),
            device(z + steps, y, x, c) if c == stage else device(z, y + steps, x, c),
        )
        for z, y, x, c in PLACES
    ]
    return lax.ppermute(value, ALL, pairs)


def shift_x(value, steps):
    pairs = [(device(z, y, x, c), device(z, y, x + steps, c)) for z, y, x, c in PLACES]
    return lax.ppermute(value, ALL, pairs)


def plane_exchange(pieces):
    return lax.all_to_all(
        pieces, ALL, split_axis=0, concat_axis=0, axis_index_groups=PLANES, tiled=True
    )


PAD = 96


def in_hbm(value):
    return pltpu.with_memory_space_constraint(value, pltpu.HBM)


def sources(core):
    out = lax.broadcasted_iota(jnp.int32, (1, 512), 1)
    chunk, place, column = out // 128, out // 32 % 4, out % 32
    far_x = (lax.axis_index("x") + chunk) % 4
    far_y = (lax.axis_index("y") + chunk) % 4
    return column + jnp.where(
        core == 0, place * 256 + far_x * 64, far_y * 256 + place * 64 + 32
    )


def order_body(mine, theirs, gain, gate, up, down, near, far, gains, rows, picks):
    units = gate.shape[0]

    @pl.when(pl.program_id(0) == 0)
    def _():
        rows[...] = jnp.zeros_like(rows)
        place = lax.broadcasted_iota(jnp.int32, (1024, 512), 0)
        picks[0] = (place == mine[...]).astype(bf16)
        picks[1] = (place == theirs[...]).astype(bf16)

    for j, weight in enumerate((gate, up, down)):
        rows[PAD * j : PAD * j + units, :] = weight[...]
    rest, row = gain[0], lax.broadcasted_iota(jnp.int32, (16, gain.shape[2]), 0)
    split = jnp.zeros(row.shape, f32)
    for i in range(3):
        part = rest.astype(bf16).astype(f32)
        rest = rest - part
        split = jnp.where(row == i, part, split)
    rows[3 * PAD :, :] = split.astype(bf16)
    mine = jnp.dot(rows[...], picks[0], preferred_element_type=f32)
    theirs = jnp.dot(rows[: 3 * PAD, :], picks[1], preferred_element_type=f32)
    for chosen, out in ((mine, near), (theirs, far)):
        chosen = chosen[: 3 * PAD].astype(bf16)
        for k in range(4):
            for j in range(3):
                out[k, j] = chosen[PAD * j : PAD * (j + 1), 128 * k : 128 * (k + 1)]
    line = jnp.sum(mine[3 * PAD : 3 * PAD + 8], axis=0, keepdims=True)
    line = jnp.broadcast_to(line, (128, line.shape[1]))
    for k in range(4):
        gains[k] = line[:, 128 * k : 128 * (k + 1)].T


def order_weights(gain, gate, up, down):
    core = lax.axis_index("c")
    units = gate.shape[0]
    whole = pl.BlockSpec((1, 512), lambda z: (0, 0))
    piece = pl.BlockSpec((units, 1024), lambda z: (0, z))
    side = pl.BlockSpec((4, 3, PAD, 128), lambda z: (0, 0, 0, z))
    shape = jax.ShapeDtypeStruct((4, 3, PAD, 512), bf16)
    return pl.pallas_call(
        order_body,
        grid=(4,),
        in_specs=[
            whole,
            whole,
            pl.BlockSpec((1, 1, 1024), lambda z: (z, 0, 0)),
            piece,
            piece,
            piece,
        ],
        out_specs=[side, side, pl.BlockSpec((4, 128, 128), lambda z: (0, z, 0))],
        out_shape=[shape, shape, jax.ShapeDtypeStruct((4, 512, 128), f32)],
        scratch_shapes=[pltpu.VMEM((3 * PAD + 16, 1024), bf16), pltpu.VMEM((2, 1024, 512), bf16)],
        cost_estimate=pl.CostEstimate(flops=5 * 10**9, bytes_accessed=6 * 10**6, transcendentals=0),
        compiler_params=pltpu.CompilerParams(vmem_limit_bytes=20 * 2**20),
        name="order",
    )(sources(core), sources(1 - core), gain.reshape(4, 1, 1024), *(in_hbm(w) for w in (gate, up, down)))


def product_body(*refs, parts, starts, more):
    chunks = len(starts)
    pieces, refs = refs[: len(parts)], refs[len(parts) :]
    nears, fars, gains = refs[:chunks], refs[chunks : 2 * chunks], refs[2 * chunks : 3 * chunks]
    before, out, away, normed = refs[3 * chunks :] if more else (None, refs[-2], None, refs[-1])
    squares = 0.0
    for piece, (chunk, first) in zip(pieces, parts, strict=True):
        count, rows = piece.shape
        value = piece[...].astype(f32)
        squares = squares + jnp.sum(value * value, axis=0, keepdims=True)
        gain = gains[chunk][0, first : first + count, :]
        gain = jnp.concatenate([gain] * (rows // 128), axis=1)
        normed[512 * chunk + first : 512 * chunk + first + count, :] = (value * gain).astype(bf16)
    for side, weights in enumerate((nears, fars)):
        weights = jnp.concatenate([w[0].reshape(2 * PAD, 512) for w in weights], axis=1)
        total = jnp.dot(weights, normed[...], preferred_element_type=f32)
        where = slice(2 * PAD * side, 2 * PAD * (side + 1))
        if more:
            total = before[where, :] + total
            away[where, :] = total.astype(bf16)
        out[where, :] = total
    squares = jnp.broadcast_to(squares, (8, squares.shape[1]))
    where = slice(4 * PAD, 4 * PAD + 8)
    if more:
        squares = before[where, :] + squares
        high = squares.astype(bf16).astype(f32)
        away[4 * PAD :, :] = jnp.concatenate([high, squares - high], axis=0).astype(bf16)
    out[where, :] = squares


def products(pieces, chunks, near, far, gains, before=None):
    rows = pieces[0][0].shape[1]
    parts = tuple((chunks.index(k), first) for _, k, first in pieces)
    operands = [p for p, _, _ in pieces]
    specs = [pl.BlockSpec(p.shape, lambda i: (0, 0)) for p in operands]
    for weights in (near, far):
        for k in chunks:
            operands.append(weights)
            specs.append(pl.BlockSpec((1, 2, PAD, 512), lambda i, k=k: (k, 0, 0, 0)))
    for k in chunks:
        operands.append(gains)
        specs.append(pl.BlockSpec((1, 512, 128), lambda i, k=k: (k, 0, 0)))
    outs = [jax.ShapeDtypeStruct((4 * PAD + 8, rows), f32)]
    if before is not None:
        operands.append(before)
        specs.append(pl.BlockSpec(before.shape, lambda i: (0, 0)))
        outs.append(jax.ShapeDtypeStruct((4 * PAD + 16, rows), bf16))
    return pl.pallas_call(
        functools.partial(product_body, parts=parts, starts=chunks, more=before is not None),
        grid=(1,),
        in_specs=specs,
        out_specs=[pl.BlockSpec(o.shape, lambda i: (0, 0)) for o in outs],
        out_shape=outs,
        scratch_shapes=[pltpu.VMEM((512 * len(chunks), rows), bf16)],
        cost_estimate=pl.CostEstimate(
            flops=len(chunks) * 4 * 10**8, bytes_accessed=len(chunks) * 10**6, transcendentals=0
        ),
        compiler_params=pltpu.CompilerParams(vmem_limit_bytes=16 * 2**20),
        name="products",
    )(*operands)


def chunk_copies(source, target, sems, outward=False):
    copies = []
    for i in range(target.shape[0] // 8):
        rows = pl.ds(8 * i, 8)
        ends = (target.at[rows], source.at[rows]) if outward else (source.at[rows], target.at[rows])
        copies.append(pltpu.make_async_copy(*ends, sems.at[i]))
    return copies


def readout_body(*refs):
    arrived, refs = refs[:4], refs[4:]
    past, floor, gain, mixed, forget, value, query, gate, states, sems = refs
    copies = chunk_copies(past, states, sems)
    for copy in copies:
        copy.start()
    heads, width = past.shape[1:3]
    inner = heads * width
    total = arrived[0][...].astype(f32)
    for piece in arrived[1:]:
        total = total + piece[...].astype(f32)
    squares = total[:, 4 * inner : 4 * inner + 1] + total[:, 4 * inner + 64 : 4 * inner + 65]
    total = total[:, : 4 * inner] * lax.rsqrt(squares / D + epsilon)
    query[...] = jax.nn.silu(total[:, :inner])
    value[...] = total[:, 2 * inner : 3 * inner]
    gate[...] = jax.nn.silu(total[:, 3 * inner :])
    bound = floor[...]
    forget[...] = bound + (1.0 - bound) * jax.nn.sigmoid(total[:, inner : 2 * inner])
    for i, copy in enumerate(copies):
        copy.wait()
        here = slice(8 * i, 8 * (i + 1))
        for h in range(heads):
            lanes = slice(width * h, width * (h + 1))
            keep, ask = forget[here, lanes], query[here, lanes]
            both = keep * ask
            high = both.astype(bf16).astype(f32)
            both = jnp.concatenate([high, both - high], axis=0).astype(bf16)
            sums = []
            for j in range(8):
                state = states[8 * i + j, h]
                top = state.astype(bf16)
                low = (state - top.astype(f32)).astype(bf16)
                dots = jnp.dot(both, top, preferred_element_type=f32) + jnp.dot(
                    both, low, preferred_element_type=f32
                )
                sums.append(dots[j : j + 1] + dots[8 + j : 8 + j + 1])
            share = jnp.sum((1.0 - keep) * ask, axis=1, keepdims=True)
            r = jnp.concatenate(sums, axis=0) + share * value[here, lanes]
            r = r * lax.rsqrt(jnp.mean(r * r, axis=1, keepdims=True) + epsilon) * gain[...]
            query[here, lanes] = r * gate[here, lanes]
    mixed[...] = query[...].astype(bf16)


def read_out(arrived, past, floor, gain):
    count, heads, width, _ = past.shape
    inner = heads * width
    rows = pltpu.VMEM((count, inner), f32)
    table = jax.ShapeDtypeStruct((count, inner), f32)
    return pl.pallas_call(
        readout_body,
        in_specs=[
            *[pl.BlockSpec(piece.shape, lambda: (0, 0)) for piece in arrived],
            pl.BlockSpec(memory_space=pl.ANY),
            pl.BlockSpec((1, inner), lambda: (0, 0)),
            pl.BlockSpec((1, width), lambda: (0, 0)),
        ],
        out_shape=[jax.ShapeDtypeStruct((count, inner), bf16), table, table],
        scratch_shapes=[
            rows,
            rows,
            pltpu.VMEM(past.shape, f32),
            pltpu.SemaphoreType.DMA((count // 8,)),
        ],
        compiler_params=pltpu.CompilerParams(vmem_limit_bytes=14 * 2**20),
        name="readout",
    )(*arrived, in_hbm(past), floor.reshape(1, -1), gain.reshape(1, -1))


def state_body(forget, value, past, new, columns, states, arrivals, departures):
    copies = chunk_copies(past, states, arrivals)
    for copy in copies:
        copy.start()
    count, heads, width, _ = past.shape
    for h in range(heads):
        table = forget[:, width * h : width * (h + 1)]
        columns[h] = jnp.concatenate([table] * (width // count), axis=0).T
    leaving = chunk_copies(new, states, departures, outward=True)
    for i, copy in enumerate(copies):
        copy.wait()
        for h in range(heads):
            near = columns[h]
            for j in range(8 * i, 8 * (i + 1)):
                keep = jnp.broadcast_to(near[:, j : j + 1], (width, width))
                added = value[j : j + 1, width * h : width * (h + 1)]
                states[j, h] = added + keep * (states[j, h] - added)
        leaving[i].start()
    for copy in leaving:
        copy.wait()


def update_state(forget, value, past):
    count, heads, width, _ = past.shape
    whole = pl.BlockSpec(forget.shape, lambda: (0, 0))
    sems = pltpu.SemaphoreType.DMA((count // 8,))
    return pl.pallas_call(
        state_body,
        in_specs=[whole, whole, pl.BlockSpec(memory_space=pl.ANY)],
        out_specs=pl.BlockSpec(memory_space=pl.ANY),
        out_shape=jax.ShapeDtypeStruct(past.shape, f32),
        scratch_shapes=[
            pltpu.VMEM((heads, width, width), f32),
            pltpu.VMEM(past.shape, f32),
            sems,
            sems,
        ],
        compiler_params=pltpu.CompilerParams(vmem_limit_bytes=12 * 2**20),
        cost_estimate=pl.CostEstimate(
            flops=4 * 10**9, bytes_accessed=8 * 10**6, transcendentals=0
        ),
        name="state",
    )(forget, value, in_hbm(past))


def project_body(gain, *refs):
    pieces, weights, outs = refs[:4], refs[4:8], refs[8:12]
    block, rows_scratch, sums_scratch = refs[12:]
    x, core = lax.axis_index("x"), lax.axis_index("c")
    width, rows = pieces[0].shape[0] // 2, pieces[0].shape[1]
    for k, piece in enumerate(pieces):
        first = lax.rem(x + k, 4) * 2 * width
        for side in range(2):
            row = pl.multiple_of(first + lax.rem(core + side, 2) * width, width)
            block[pl.ds(row, width), :] = piece[width * side : width * (side + 1), :]
    value = block[...].astype(f32)
    normed = (value * jnp.concatenate([gain[...]] * (rows // 128), axis=1)).astype(bf16)
    rows_scratch[...] = normed.T
    squares = jnp.sum(value * value, axis=0, keepdims=True)
    high = squares.astype(bf16).astype(f32)
    line = lax.broadcasted_iota(jnp.int32, (128, rows), 0)
    sums_scratch[...] = jnp.where(line < 64, high, squares - high).astype(bf16).T
    own = outs[0].shape[1]
    z, y = lax.axis_index("z"), lax.axis_index("y")
    starts = []
    for k in range(4):
        for m in range(4):
            ahead = jnp.where(core == 0, k, m), jnp.where(core == 0, m, k)
            owner = lax.rem(z + ahead[0], 4) * 4 + lax.rem(y + ahead[1], 4)
            starts.append(pl.multiple_of(owner * own, own))
    normed = jnp.concatenate([rows_scratch[pl.ds(row, own), :] for row in starts], axis=0)
    for i, w in enumerate(weights):
        part = jnp.dot(normed, w[...], preferred_element_type=f32).astype(bf16)
        for k, out in enumerate(outs):
            here = part[4 * own * k : 4 * own * (k + 1)]
            out[:, :, 256 * i : 256 * (i + 1)] = here.reshape(4, own, 256)
    for k, out in enumerate(outs):
        for m in range(4):
            out[m, :, 1024:1152] = sums_scratch[pl.ds(starts[4 * k + m], own), :]


def project(pieces, gain, weights, own_rows):
    rows, width = pieces[0].shape[1], gain.shape[0]
    operands = [jnp.broadcast_to(gain[:, None], (width, 128)), *pieces, *weights]
    return pl.pallas_call(
        project_body,
        in_specs=[pl.BlockSpec(v.shape, lambda: (0, 0)) for v in operands],
        out_shape=[jax.ShapeDtypeStruct((4, own_rows, 4 * width + 128), bf16)] * 4,
        scratch_shapes=[
            pltpu.VMEM((width, rows), bf16),
            pltpu.VMEM((rows, width), bf16),
            pltpu.VMEM((rows, 128), bf16),
        ],
        compiler_params=pltpu.CompilerParams(vmem_limit_bytes=14 * 2**20),
        name="project",
    )(*operands)


def output_body(gathered, weight, mine, theirs, block):
    place = lax.axis_index("x"), lax.axis_index("c")
    width = mine.shape[1]
    block[...] = lax.dot_general(
        weight[...].T, gathered[...], (((1,), (1,)), ((), ())), preferred_element_type=f32
    )
    for k in range(4):
        first = lax.rem(place[0] + k, 4) * 2 * width
        for side, out in enumerate((mine, theirs)):
            row = pl.multiple_of(first + lax.rem(place[1] + side, 2) * width, width)
            out[k] = block[pl.ds(row, width), :].astype(bf16)


def project_out(gathered, weight):
    rows, width = gathered.shape[0], weight.shape[1]
    shape = jax.ShapeDtypeStruct((4, width // 8, rows), bf16)
    return pl.pallas_call(
        output_body,
        in_specs=[pl.BlockSpec(v.shape, lambda: (0, 0)) for v in (gathered, weight)],
        out_shape=[shape, shape],
        scratch_shapes=[pltpu.VMEM((width, rows), f32)],
        compiler_params=pltpu.CompilerParams(vmem_limit_bytes=10 * 2**20),
        name="output",
    )(gathered, weight)


def half_step(own, near_w, far_w, gains, near):
    width, rows = own.shape
    half = near.shape[0] // 2
    top, low = slice(0, half), slice(half, 2 * half)
    left_top = shift(near[top], 1)
    right_low = shift(near[low], -1)
    left_low = shift(near[low], 1)
    right_top = shift(near[top], -1)
    left_top, right_low, far_w = lax.optimization_barrier((left_top, right_low, far_w))
    far_top = shift(left_top, 1)
    far_low = shift(right_low, -1)
    early = [
        (near, 0, 0),
        (left_top, 3, 0),
        (right_low, 1, half),
        (left_low, 3, half),
        (right_top, 1, 0),
    ]
    (acc,) = products(early, [0, 3, 1], near_w, far_w, gains)
    late = [(far_top, 2, 0), (far_low, 2, half)]
    acc, away = products(late, [2], near_w, far_w, gains, acc)
    got = other_core(away).astype(f32)
    squares = acc[4 * PAD] + got[4 * PAD] + got[4 * PAD + 8]
    scale = lax.rsqrt(squares / D + epsilon)[None, :]
    own_acc = acc[: 2 * PAD] + got[2 * PAD : 4 * PAD]
    far_acc = acc[2 * PAD : 4 * PAD] + got[: 2 * PAD]
    hidden = jnp.concatenate(
        [
            (jax.nn.silu(scale * a[:PAD]) * (scale * a[PAD:])).astype(bf16)
            for a in (own_acc, far_acc)
        ],
        axis=0,
    )
    deep = jnp.concatenate([near_w[:, 2], far_w[:, 2]], axis=1)

    sums, arrived = {}, []
    for k in (2, 1, 3, 0):
        sums[k] = lax.dot_general(
            deep[k], hidden, (((0,), (0,)), ((), ())), preferred_element_type=f32
        ).astype(bf16)
        if k:
            arrived.append(shift(sums[k], k))
    total = sums[0].astype(f32)
    for piece in arrived:
        total = total + piece.astype(f32)
    total = total.astype(bf16)
    total = plane_exchange(total.reshape(16, width, rows)).astype(f32).sum(axis=0)
    return lax.optimization_barrier((own.astype(f32) + 0.5 * total).astype(bf16))


def plane_gather(own):
    return plane_exchange(jnp.broadcast_to(own, (16, *own.shape))).reshape(-1, own.shape[1])


def per_device(
    tokens,
    past_state,
    pre_gain,
    pre_gate,
    pre_up,
    pre_down,
    mix_gain,
    query_weight,
    forget_weight,
    value_weight,
    output_gate_weight,
    forget_floor,
    head_gain,
    proj_out,
    post_gain,
    post_gate,
    post_up,
    post_down,
):
    tokens = tokens.T
    near = plane_gather(tokens)
    near_w, far_w, gains = order_weights(pre_gain, pre_gate.T, pre_up.T, pre_down)
    near, near_w, far_w = lax.optimization_barrier((near, near_w, far_w))
    first = half_step(tokens, near_w, other_core(far_w), gains, near)

    width = mix_gain.shape[0] // lax.axis_size(KV)
    own_rows, _, _, _ = past_state.shape
    gains = lax.dynamic_slice_in_dim(mix_gain, lax.axis_index(KV) * width, width, 0)
    pair = jnp.concatenate([first, other_core(first)], axis=0)
    pieces = [pair] + [shift_x(pair, -k) for k in (1, 2, 3)]
    weight_list = (query_weight, forget_weight, value_weight, output_gate_weight)
    sent = project(pieces, gains, weight_list, own_rows)
    blocks = list(sent)
    blocks[0], post_gate, post_up, post_down = lax.optimization_barrier(
        (blocks[0], post_gate, post_up, post_down)
    )
    near_w, far_w, gains = order_weights(post_gain, post_gate.T, post_up.T, post_down)
    summed = blocks[0].astype(f32)
    passed = [shift_kv(blocks[k], k, 0) for k in (2, 1, 3)]
    passed, near_w = lax.optimization_barrier((passed, near_w))
    for piece in passed:
        summed = summed + piece.astype(f32)
    summed = summed.astype(bf16)
    arrived = [summed[0]] + [shift_kv(summed[m], m, 1) for m in (2, 1, 3)]
    mixed_in, forget, value = read_out(arrived, past_state, forget_floor, head_gain)
    new_state = update_state(forget, value, past_state)
    gathered = copy_for_each(mixed_in, KV).reshape(-1, mixed_in.shape[1])
    gathered, new_state = lax.optimization_barrier((gathered, new_state))
    mine, theirs = project_out(gathered, proj_out)
    mixed = (mine.astype(f32) + other_core(theirs).astype(f32)).astype(bf16)
    mixed_sum = mixed[0].astype(f32)
    for piece in [shift_x(mixed[k], k) for k in (2, 1, 3)]:
        mixed_sum = mixed_sum + piece.astype(f32)
    second = lax.optimization_barrier((first.astype(f32) + mixed_sum).astype(bf16))
    near = plane_gather(second)
    near, far_w = lax.optimization_barrier((near, far_w))
    far_w = other_core(far_w)
    result = half_step(second, near_w, far_w, gains, near)
    return (result.T, new_state)


def solution(mesh):
    torus = Mesh(mesh.devices.reshape(4, 4, 4, 2), ALL)
    return jax.shard_map(
        per_device,
        mesh=torus,
        in_specs=(
            P(None, ALL),
            P(KV, TP, None, None),
            P(),
            P(None, ALL),
            P(None, ALL),
            P(ALL, None),
            P(),
            P(KV, TP),
            P(KV, TP),
            P(KV, TP),
            P(KV, TP),
            P(TP),
            P(),
            P(TP, KV),
            P(),
            P(None, ALL),
            P(None, ALL),
            P(ALL, None),
        ),
        out_specs=(P(None, ALL), P(KV, TP, None, None)),
        check_vma=False,
    )
```

```python
import functools

import jax
import jax.numpy as jnp
from jax import lax
from jax.experimental import pallas as pl
from jax.experimental.pallas import tpu as pltpu
from jax.sharding import Mesh
from jax.sharding import PartitionSpec as P


D = 4096
ALL = ("z", "y", "x", "c")
KV = ("z", "y")
TP = ("x", "c")
epsilon = 1e-06
f32 = jnp.float32
bf16 = jnp.bfloat16


def other_core(value):
    return lax.ppermute(value, "c", [(0, 1), (1, 0)])


def device(z, y, x, c):
    return ((z % 4 * 4 + y % 4) * 4 + x % 4) * 2 + c


PLACES = [(z, y, x, c) for z in range(4) for y in range(4) for x in range(4) for c in range(2)]
PLANES = [[device(z, m, x, 0) for z in range(4) for m in range(4)] for x in range(4)] + [
    [device(z, y, m, 1) for z in range(4) for m in range(4)] for y in range(4)
]


def shift(value, steps):
    pairs = [
        (device(z, y, x, c), device(z, y, x + steps, c) if c == 0 else device(z, y + steps, x, c))
        for z, y, x, c in PLACES
    ]
    return lax.ppermute(value, ALL, pairs)


def shift_kv(value, steps, stage):
    pairs = [
        (
            device(z, y, x, c),
            device(z + steps, y, x, c) if c == stage else device(z, y + steps, x, c),
        )
        for z, y, x, c in PLACES
    ]
    return lax.ppermute(value, ALL, pairs)


def shift_x(value, steps):
    pairs = [(device(z, y, x, c), device(z, y, x + steps, c)) for z, y, x, c in PLACES]
    return lax.ppermute(value, ALL, pairs)


def plane_exchange(pieces):
    return lax.all_to_all(
        pieces, ALL, split_axis=0, concat_axis=0, axis_index_groups=PLANES, tiled=True
    )


PAD = 96


def in_hbm(value):
    return pltpu.with_memory_space_constraint(value, pltpu.HBM)


def sources(core):
    out = lax.broadcasted_iota(jnp.int32, (1, 512), 1)
    chunk, place, column = out // 128, out // 32 % 4, out % 32
    far_x = (lax.axis_index("x") + chunk) % 4
    far_y = (lax.axis_index("y") + chunk) % 4
    return column + jnp.where(
        core == 0, place * 256 + far_x * 64, far_y * 256 + place * 64 + 32
    )


def order_body(mine, theirs, gain, gate, up, down, near, far, gains, rows, picks):
    units = gate.shape[0]

    @pl.when(pl.program_id(0) == 0)
    def _():
        rows[...] = jnp.zeros_like(rows)
        place = lax.broadcasted_iota(jnp.int32, (1024, 512), 0)
        picks[0] = (place == mine[...]).astype(bf16)
        picks[1] = (place == theirs[...]).astype(bf16)

    for j, weight in enumerate((gate, up, down)):
        rows[PAD * j : PAD * j + units, :] = weight[...]
    rest, row = gain[0], lax.broadcasted_iota(jnp.int32, (16, gain.shape[2]), 0)
    split = jnp.zeros(row.shape, f32)
    for i in range(3):
        part = rest.astype(bf16).astype(f32)
        rest = rest - part
        split = jnp.where(row == i, part, split)
    rows[3 * PAD :, :] = split.astype(bf16)
    mine = jnp.dot(rows[...], picks[0], preferred_element_type=f32)
    theirs = jnp.dot(rows[: 3 * PAD, :], picks[1], preferred_element_type=f32)
    for chosen, out in ((mine, near), (theirs, far)):
        chosen = chosen[: 3 * PAD].astype(bf16)
        for k in range(4):
            for j in range(3):
                out[k, j] = chosen[PAD * j : PAD * (j + 1), 128 * k : 128 * (k + 1)]
    line = jnp.sum(mine[3 * PAD : 3 * PAD + 8], axis=0, keepdims=True)
    line = jnp.broadcast_to(line, (128, line.shape[1]))
    for k in range(4):
        gains[k] = line[:, 128 * k : 128 * (k + 1)].T


def order_weights(gain, gate, up, down):
    core = lax.axis_index("c")
    units = gate.shape[0]
    whole = pl.BlockSpec((1, 512), lambda z: (0, 0))
    piece = pl.BlockSpec((units, 1024), lambda z: (0, z))
    side = pl.BlockSpec((4, 3, PAD, 128), lambda z: (0, 0, 0, z))
    shape = jax.ShapeDtypeStruct((4, 3, PAD, 512), bf16)
    return pl.pallas_call(
        order_body,
        grid=(4,),
        in_specs=[
            whole,
            whole,
            pl.BlockSpec((1, 1, 1024), lambda z: (z, 0, 0)),
            piece,
            piece,
            piece,
        ],
        out_specs=[side, side, pl.BlockSpec((4, 128, 128), lambda z: (0, z, 0))],
        out_shape=[shape, shape, jax.ShapeDtypeStruct((4, 512, 128), f32)],
        scratch_shapes=[pltpu.VMEM((3 * PAD + 16, 1024), bf16), pltpu.VMEM((2, 1024, 512), bf16)],
        cost_estimate=pl.CostEstimate(flops=5 * 10**9, bytes_accessed=6 * 10**6, transcendentals=0),
        compiler_params=pltpu.CompilerParams(vmem_limit_bytes=20 * 2**20),
        name="order",
    )(sources(core), sources(1 - core), gain.reshape(4, 1, 1024), *(in_hbm(w) for w in (gate, up, down)))


def product_body(*refs, parts, starts, more):
    chunks = len(starts)
    pieces, refs = refs[: len(parts)], refs[len(parts) :]
    nears, fars, gains = refs[:chunks], refs[chunks : 2 * chunks], refs[2 * chunks : 3 * chunks]
    before, out, away, normed = refs[3 * chunks :] if more else (None, refs[-2], None, refs[-1])
    squares = 0.0
    for piece, (chunk, first) in zip(pieces, parts, strict=True):
        count, rows = piece.shape
        value = piece[...].astype(f32)
        squares = squares + jnp.sum(value * value, axis=0, keepdims=True)
        gain = gains[chunk][0, first : first + count, :]
        gain = jnp.concatenate([gain] * (rows // 128), axis=1)
        normed[512 * chunk + first : 512 * chunk + first + count, :] = (value * gain).astype(bf16)
    for side, weights in enumerate((nears, fars)):
        weights = jnp.concatenate([w[0].reshape(2 * PAD, 512) for w in weights], axis=1)
        total = jnp.dot(weights, normed[...], preferred_element_type=f32)
        where = slice(2 * PAD * side, 2 * PAD * (side + 1))
        if more:
            total = before[where, :] + total
            away[where, :] = total.astype(bf16)
        out[where, :] = total
    squares = jnp.broadcast_to(squares, (8, squares.shape[1]))
    where = slice(4 * PAD, 4 * PAD + 8)
    if more:
        squares = before[where, :] + squares
        high = squares.astype(bf16).astype(f32)
        away[4 * PAD :, :] = jnp.concatenate([high, squares - high], axis=0).astype(bf16)
    out[where, :] = squares


def products(pieces, chunks, near, far, gains, before=None):
    rows = pieces[0][0].shape[1]
    parts = tuple((chunks.index(k), first) for _, k, first in pieces)
    operands = [p for p, _, _ in pieces]
    specs = [pl.BlockSpec(p.shape, lambda i: (0, 0)) for p in operands]
    for weights in (near, far):
        for k in chunks:
            operands.append(weights)
            specs.append(pl.BlockSpec((1, 2, PAD, 512), lambda i, k=k: (k, 0, 0, 0)))
    for k in chunks:
        operands.append(gains)
        specs.append(pl.BlockSpec((1, 512, 128), lambda i, k=k: (k, 0, 0)))
    outs = [jax.ShapeDtypeStruct((4 * PAD + 8, rows), f32)]
    if before is not None:
        operands.append(before)
        specs.append(pl.BlockSpec(before.shape, lambda i: (0, 0)))
        outs.append(jax.ShapeDtypeStruct((4 * PAD + 16, rows), bf16))
    return pl.pallas_call(
        functools.partial(product_body, parts=parts, starts=chunks, more=before is not None),
        grid=(1,),
        in_specs=specs,
        out_specs=[pl.BlockSpec(o.shape, lambda i: (0, 0)) for o in outs],
        out_shape=outs,
        scratch_shapes=[pltpu.VMEM((512 * len(chunks), rows), bf16)],
        cost_estimate=pl.CostEstimate(
            flops=len(chunks) * 4 * 10**8, bytes_accessed=len(chunks) * 10**6, transcendentals=0
        ),
        compiler_params=pltpu.CompilerParams(vmem_limit_bytes=16 * 2**20),
        name="products",
    )(*operands)


def chunk_copies(source, target, sems, outward=False):
    copies = []
    for i in range(target.shape[0] // 8):
        rows = pl.ds(8 * i, 8)
        ends = (target.at[rows], source.at[rows]) if outward else (source.at[rows], target.at[rows])
        copies.append(pltpu.make_async_copy(*ends, sems.at[i]))
    return copies


def readout_body(*refs):
    arrived, refs = refs[:4], refs[4:]
    past, floor, gain, mixed, forget, value, query, gate, states, sems = refs
    copies = chunk_copies(past, states, sems)
    for copy in copies:
        copy.start()
    heads, width = past.shape[1:3]
    inner = heads * width
    total = arrived[0][...].astype(f32)
    for piece in arrived[1:]:
        total = total + piece[...].astype(f32)
    squares = total[:, 4 * inner : 4 * inner + 1] + total[:, 4 * inner + 64 : 4 * inner + 65]
    total = total[:, : 4 * inner] * lax.rsqrt(squares / D + epsilon)
    query[...] = jax.nn.silu(total[:, :inner])
    value[...] = total[:, 2 * inner : 3 * inner]
    gate[...] = jax.nn.silu(total[:, 3 * inner :])
    bound = floor[...]
    forget[...] = bound + (1.0 - bound) * jax.nn.sigmoid(total[:, inner : 2 * inner])
    for i, copy in enumerate(copies):
        copy.wait()
        here = slice(8 * i, 8 * (i + 1))
        for h in range(heads):
            lanes = slice(width * h, width * (h + 1))
            keep, ask = forget[here, lanes], query[here, lanes]
            both = keep * ask
            high = both.astype(bf16).astype(f32)
            both = jnp.concatenate([high, both - high], axis=0).astype(bf16)
            sums = []
            for j in range(8):
                state = states[8 * i + j, h]
                top = state.astype(bf16)
                low = (state - top.astype(f32)).astype(bf16)
                dots = jnp.dot(both, top, preferred_element_type=f32) + jnp.dot(
                    both, low, preferred_element_type=f32
                )
                sums.append(dots[j : j + 1] + dots[8 + j : 8 + j + 1])
            share = jnp.sum((1.0 - keep) * ask, axis=1, keepdims=True)
            r = jnp.concatenate(sums, axis=0) + share * value[here, lanes]
            r = r * lax.rsqrt(jnp.mean(r * r, axis=1, keepdims=True) + epsilon) * gain[...]
            query[here, lanes] = r * gate[here, lanes]
    mixed[...] = query[...].astype(bf16)


def read_out(arrived, past, floor, gain):
    count, heads, width, _ = past.shape
    inner = heads * width
    rows = pltpu.VMEM((count, inner), f32)
    table = pltpu.HBM((count, inner), f32)
    return pl.pallas_call(
        readout_body,
        in_specs=[
            *[pl.BlockSpec(piece.shape, lambda: (0, 0)) for piece in arrived],
            pl.BlockSpec(memory_space=pl.ANY),
            pl.BlockSpec((1, inner), lambda: (0, 0)),
            pl.BlockSpec((1, width), lambda: (0, 0)),
        ],
        out_shape=[jax.ShapeDtypeStruct((count, inner), bf16), table, table],
        scratch_shapes=[
            rows,
            rows,
            pltpu.VMEM(past.shape, f32),
            pltpu.SemaphoreType.DMA((count // 8,)),
        ],
        compiler_params=pltpu.CompilerParams(vmem_limit_bytes=14 * 2**20),
        name="readout",
    )(*arrived, in_hbm(past), floor.reshape(1, -1), gain.reshape(1, -1))


def state_body(forget, value, past, new, columns, states, arrivals, departures):
    copies = chunk_copies(past, states, arrivals)
    for copy in copies:
        copy.start()
    count, heads, width, _ = past.shape
    for h in range(heads):
        table = forget[:, width * h : width * (h + 1)]
        columns[h] = jnp.concatenate([table] * (width // count), axis=0).T
    leaving = chunk_copies(new, states, departures, outward=True)
    for i, copy in enumerate(copies):
        copy.wait()
        for h in range(heads):
            near = columns[h]
            for j in range(8 * i, 8 * (i + 1)):
                keep = jnp.broadcast_to(near[:, j : j + 1], (width, width))
                added = value[j : j + 1, width * h : width * (h + 1)]
                states[j, h] = added + keep * (states[j, h] - added)
        leaving[i].start()
    for copy in leaving:
        copy.wait()


def update_state(forget, value, past):
    count, heads, width, _ = past.shape
    whole = pl.BlockSpec(forget.shape, lambda: (0, 0))
    sems = pltpu.SemaphoreType.DMA((count // 8,))
    return pl.pallas_call(
        state_body,
        in_specs=[whole, whole, pl.BlockSpec(memory_space=pl.ANY)],
        out_specs=pl.BlockSpec(memory_space=pl.ANY),
        out_shape=jax.ShapeDtypeStruct(past.shape, f32),
        scratch_shapes=[
            pltpu.VMEM((heads, width, width), f32),
            pltpu.VMEM(past.shape, f32),
            sems,
            sems,
        ],
        compiler_params=pltpu.CompilerParams(vmem_limit_bytes=12 * 2**20),
        cost_estimate=pl.CostEstimate(
            flops=4 * 10**9, bytes_accessed=8 * 10**6, transcendentals=0
        ),
        name="state",
    )(in_hbm(forget), in_hbm(value), in_hbm(past))


def project_body(gain, *refs):
    pieces, weights, outs = refs[:4], refs[4:8], refs[8:12]
    block, rows_scratch, sums_scratch = refs[12:]
    x, core = lax.axis_index("x"), lax.axis_index("c")
    width, rows = pieces[0].shape[0] // 2, pieces[0].shape[1]
    for k, piece in enumerate(pieces):
        first = lax.rem(x + k, 4) * 2 * width
        for side in range(2):
            row = pl.multiple_of(first + lax.rem(core + side, 2) * width, width)
            block[pl.ds(row, width), :] = piece[width * side : width * (side + 1), :]
    value = block[...].astype(f32)
    normed = (value * jnp.concatenate([gain[...]] * (rows // 128), axis=1)).astype(bf16)
    rows_scratch[...] = normed.T
    squares = jnp.sum(value * value, axis=0, keepdims=True)
    high = squares.astype(bf16).astype(f32)
    line = lax.broadcasted_iota(jnp.int32, (128, rows), 0)
    sums_scratch[...] = jnp.where(line < 64, high, squares - high).astype(bf16).T
    own = outs[0].shape[1]
    z, y = lax.axis_index("z"), lax.axis_index("y")
    starts = []
    for k in range(4):
        for m in range(4):
            ahead = jnp.where(core == 0, k, m), jnp.where(core == 0, m, k)
            owner = lax.rem(z + ahead[0], 4) * 4 + lax.rem(y + ahead[1], 4)
            starts.append(pl.multiple_of(owner * own, own))
    normed = jnp.concatenate([rows_scratch[pl.ds(row, own), :] for row in starts], axis=0)
    for i, w in enumerate(weights):
        part = jnp.dot(normed, w[...], preferred_element_type=f32).astype(bf16)
        for k, out in enumerate(outs):
            here = part[4 * own * k : 4 * own * (k + 1)]
            out[:, :, 256 * i : 256 * (i + 1)] = here.reshape(4, own, 256)
    for k, out in enumerate(outs):
        for m in range(4):
            out[m, :, 1024:1152] = sums_scratch[pl.ds(starts[4 * k + m], own), :]


def project(pieces, gain, weights, own_rows):
    rows, width = pieces[0].shape[1], gain.shape[0]
    operands = [jnp.broadcast_to(gain[:, None], (width, 128)), *pieces, *weights]
    return pl.pallas_call(
        project_body,
        in_specs=[pl.BlockSpec(v.shape, lambda: (0, 0)) for v in operands],
        out_shape=[jax.ShapeDtypeStruct((4, own_rows, 4 * width + 128), bf16)] * 4,
        scratch_shapes=[
            pltpu.VMEM((width, rows), bf16),
            pltpu.VMEM((rows, width), bf16),
            pltpu.VMEM((rows, 128), bf16),
        ],
        compiler_params=pltpu.CompilerParams(vmem_limit_bytes=14 * 2**20),
        name="project",
    )(*operands)


def output_body(*refs):
    pieces, (weight, mine, theirs, rows, block) = refs[:4], refs[4:]
    x, core = lax.axis_index("x"), lax.axis_index("c")
    z, y = lax.axis_index("z"), lax.axis_index("y")
    own = pieces[0].shape[1]
    for m, piece in enumerate(pieces):
        for k in range(4):
            ahead = jnp.where(core == 0, k, m), jnp.where(core == 0, m, k)
            owner = lax.rem(z + ahead[0], 4) * 4 + lax.rem(y + ahead[1], 4)
            rows[pl.ds(pl.multiple_of(owner * own, own), own), :] = piece[k]
    width = mine.shape[1]
    block[...] = lax.dot_general(
        weight[...].T, rows[...], (((1,), (1,)), ((), ())), preferred_element_type=f32
    )
    for k in range(4):
        first = lax.rem(x + k, 4) * 2 * width
        for side, out in enumerate((mine, theirs)):
            row = pl.multiple_of(first + lax.rem(core + side, 2) * width, width)
            out[k] = block[pl.ds(row, width), :].astype(bf16)


def project_out(pieces, weight):
    rows, width = 4 * pieces[0].shape[0] * pieces[0].shape[1], weight.shape[1]
    shape = jax.ShapeDtypeStruct((4, width // 8, rows), bf16)
    return pl.pallas_call(
        output_body,
        in_specs=[pl.BlockSpec(piece.shape, lambda: (0, 0, 0)) for piece in pieces]
        + [pl.BlockSpec(weight.shape, lambda: (0, 0))],
        out_shape=[shape, shape],
        scratch_shapes=[
            pltpu.VMEM((rows, weight.shape[0]), bf16),
            pltpu.VMEM((width, rows), f32),
        ],
        compiler_params=pltpu.CompilerParams(vmem_limit_bytes=10 * 2**20),
        name="output",
    )(*pieces, weight)


def half_step(own, near_w, far_w, gains, near):
    width, rows = own.shape
    half = near.shape[0] // 2
    top, low = slice(0, half), slice(half, 2 * half)
    left_top = shift(near[top], 1)
    right_low = shift(near[low], -1)
    left_low = shift(near[low], 1)
    right_top = shift(near[top], -1)
    left_top, right_low, far_w = lax.optimization_barrier((left_top, right_low, far_w))
    far_top = shift(left_top, 1)
    far_low = shift(right_low, -1)
    early = [
        (near, 0, 0),
        (left_top, 3, 0),
        (right_low, 1, half),
        (left_low, 3, half),
        (right_top, 1, 0),
    ]
    (acc,) = products(early, [0, 3, 1], near_w, far_w, gains)
    late = [(far_top, 2, 0), (far_low, 2, half)]
    acc, away = products(late, [2], near_w, far_w, gains, acc)
    got = other_core(away).astype(f32)
    squares = acc[4 * PAD] + got[4 * PAD] + got[4 * PAD + 8]
    scale = lax.rsqrt(squares / D + epsilon)[None, :]
    own_acc = acc[: 2 * PAD] + got[2 * PAD : 4 * PAD]
    far_acc = acc[2 * PAD : 4 * PAD] + got[: 2 * PAD]
    hidden = jnp.concatenate(
        [
            (jax.nn.silu(scale * a[:PAD]) * (scale * a[PAD:])).astype(bf16)
            for a in (own_acc, far_acc)
        ],
        axis=0,
    )
    deep = jnp.concatenate([near_w[:, 2], far_w[:, 2]], axis=1)

    sums, arrived = {}, []
    for k in (2, 1, 3, 0):
        sums[k] = lax.dot_general(
            deep[k], hidden, (((0,), (0,)), ((), ())), preferred_element_type=f32
        ).astype(bf16)
        if k:
            arrived.append(shift(sums[k], k))
    total = sums[0].astype(f32)
    for piece in arrived:
        total = total + piece.astype(f32)
    total = total.astype(bf16)
    total = plane_exchange(total.reshape(16, width, rows)).astype(f32).sum(axis=0)
    return lax.optimization_barrier((own.astype(f32) + 0.5 * total).astype(bf16))


def plane_gather(own):
    return plane_exchange(jnp.broadcast_to(own, (16, *own.shape))).reshape(-1, own.shape[1])


def per_device(
    tokens,
    past_state,
    pre_gain,
    pre_gate,
    pre_up,
    pre_down,
    mix_gain,
    query_weight,
    forget_weight,
    value_weight,
    output_gate_weight,
    forget_floor,
    head_gain,
    proj_out,
    post_gain,
    post_gate,
    post_up,
    post_down,
):
    tokens = tokens.T
    near = plane_gather(tokens)
    near_w, far_w, gains = order_weights(pre_gain, pre_gate.T, pre_up.T, pre_down)
    near, near_w, far_w = lax.optimization_barrier((near, near_w, far_w))
    first = half_step(tokens, near_w, other_core(far_w), gains, near)

    width = mix_gain.shape[0] // lax.axis_size(KV)
    own_rows, _, _, _ = past_state.shape
    gains = lax.dynamic_slice_in_dim(mix_gain, lax.axis_index(KV) * width, width, 0)
    pair = jnp.concatenate([first, other_core(first)], axis=0)
    pieces = [pair] + [shift_x(pair, -k) for k in (1, 2, 3)]
    weight_list = (query_weight, forget_weight, value_weight, output_gate_weight)
    sent = project(pieces, gains, weight_list, own_rows)
    blocks = list(sent)
    blocks[0], post_gate, post_up, post_down = lax.optimization_barrier(
        (blocks[0], post_gate, post_up, post_down)
    )
    near_w, far_w, gains = order_weights(post_gain, post_gate.T, post_up.T, post_down)
    summed = blocks[0].astype(f32)
    passed = [shift_kv(blocks[k], k, 0) for k in (2, 1, 3)]
    passed, near_w = lax.optimization_barrier((passed, near_w))
    for piece in passed:
        summed = summed + piece.astype(f32)
    summed = summed.astype(bf16)
    arrived = [summed[0]] + [shift_kv(summed[m], m, 1) for m in (2, 1, 3)]
    mixed_in, forget, value = read_out(arrived, past_state, forget_floor, head_gain)
    own_axis = {k: shift_kv(mixed_in, -k, 0) for k in (2, 1, 3)}
    line = jnp.stack([mixed_in, own_axis[1], own_axis[2], own_axis[3]])
    other_axis = {m: shift_kv(line, -m, 1) for m in (2, 1, 3)}
    mine, theirs = project_out([line, other_axis[1], other_axis[2], other_axis[3]], proj_out)
    mixed = (mine.astype(f32) + other_core(theirs).astype(f32)).astype(bf16)
    mixed_sum = mixed[0].astype(f32)
    for piece in [shift_x(mixed[k], k) for k in (2, 1, 3)]:
        mixed_sum = mixed_sum + piece.astype(f32)
    second = lax.optimization_barrier((first.astype(f32) + mixed_sum).astype(bf16))
    near = plane_gather(second)
    near, far_w = lax.optimization_barrier((near, far_w))
    far_w = other_core(far_w)
    new_state = update_state(forget, value, past_state)
    result = half_step(second, near_w, far_w, gains, near)
    return (result.T, new_state)


def solution(mesh):
    torus = Mesh(mesh.devices.reshape(4, 4, 4, 2), ALL)
    return jax.shard_map(
        per_device,
        mesh=torus,
        in_specs=(
            P(None, ALL),
            P(KV, TP, None, None),
            P(),
            P(None, ALL),
            P(None, ALL),
            P(ALL, None),
            P(),
            P(KV, TP),
            P(KV, TP),
            P(KV, TP),
            P(KV, TP),
            P(TP),
            P(),
            P(TP, KV),
            P(),
            P(None, ALL),
            P(None, ALL),
            P(ALL, None),
        ),
        out_specs=(P(None, ALL), P(KV, TP, None, None)),
        check_vma=False,
    )
```

```python
import functools

import jax
import jax.numpy as jnp
from jax import lax
from jax.experimental import pallas as pl
from jax.experimental.pallas import tpu as pltpu
from jax.sharding import Mesh
from jax.sharding import PartitionSpec as P


D = 4096
ALL = ("z", "y", "x", "c")
KV = ("z", "y")
TP = ("x", "c")
epsilon = 1e-06
f32 = jnp.float32
bf16 = jnp.bfloat16


def copy_for_each(value, axes):
    copies = jnp.broadcast_to(value, (lax.axis_size(axes), *value.shape))
    return lax.all_to_all(copies, axes, split_axis=0, concat_axis=0, tiled=True)


def other_core(value):
    return lax.ppermute(value, "c", [(0, 1), (1, 0)])


def device(z, y, x, c):
    return ((z % 4 * 4 + y % 4) * 4 + x % 4) * 2 + c


PLACES = [(z, y, x, c) for z in range(4) for y in range(4) for x in range(4) for c in range(2)]
PLANES = [[device(z, m, x, 0) for z in range(4) for m in range(4)] for x in range(4)] + [
    [device(z, y, m, 1) for z in range(4) for m in range(4)] for y in range(4)
]


def shift(value, steps):
    pairs = [
        (device(z, y, x, c), device(z, y, x + steps, c) if c == 0 else device(z, y + steps, x, c))
        for z, y, x, c in PLACES
    ]
    return lax.ppermute(value, ALL, pairs)


def shift_kv(value, steps, stage):
    pairs = [
        (
            device(z, y, x, c),
            device(z + steps, y, x, c) if c == stage else device(z, y + steps, x, c),
        )
        for z, y, x, c in PLACES
    ]
    return lax.ppermute(value, ALL, pairs)


def shift_x(value, steps):
    pairs = [(device(z, y, x, c), device(z, y, x + steps, c)) for z, y, x, c in PLACES]
    return lax.ppermute(value, ALL, pairs)


def plane_exchange(pieces):
    return lax.all_to_all(
        pieces, ALL, split_axis=0, concat_axis=0, axis_index_groups=PLANES, tiled=True
    )


PAD = 96


def in_hbm(value):
    return pltpu.with_memory_space_constraint(value, pltpu.HBM)


def sources(core):
    out = lax.broadcasted_iota(jnp.int32, (1, 512), 1)
    chunk, place, column = out // 128, out // 32 % 4, out % 32
    far_x = (lax.axis_index("x") + chunk) % 4
    far_y = (lax.axis_index("y") + chunk) % 4
    return column + jnp.where(
        core == 0, place * 256 + far_x * 64, far_y * 256 + place * 64 + 32
    )


def order_body(mine, theirs, gain, gate, up, down, near, far, gains, rows, picks):
    units = gate.shape[0]

    @pl.when(pl.program_id(0) == 0)
    def _():
        rows[...] = jnp.zeros_like(rows)
        place = lax.broadcasted_iota(jnp.int32, (1024, 512), 0)
        picks[0] = (place == mine[...]).astype(bf16)
        picks[1] = (place == theirs[...]).astype(bf16)

    for j, weight in enumerate((gate, up, down)):
        rows[PAD * j : PAD * j + units, :] = weight[...]
    rest, row = gain[0], lax.broadcasted_iota(jnp.int32, (16, gain.shape[2]), 0)
    split = jnp.zeros(row.shape, f32)
    for i in range(3):
        part = rest.astype(bf16).astype(f32)
        rest = rest - part
        split = jnp.where(row == i, part, split)
    rows[3 * PAD :, :] = split.astype(bf16)
    mine = jnp.dot(rows[...], picks[0], preferred_element_type=f32)
    theirs = jnp.dot(rows[: 3 * PAD, :], picks[1], preferred_element_type=f32)
    for chosen, out in ((mine, near), (theirs, far)):
        chosen = chosen[: 3 * PAD].astype(bf16)
        for k in range(4):
            for j in range(3):
                out[k, j] = chosen[PAD * j : PAD * (j + 1), 128 * k : 128 * (k + 1)]
    line = jnp.sum(mine[3 * PAD : 3 * PAD + 8], axis=0, keepdims=True)
    line = jnp.broadcast_to(line, (128, line.shape[1]))
    for k in range(4):
        gains[k] = line[:, 128 * k : 128 * (k + 1)].T


def order_weights(gain, gate, up, down):
    core = lax.axis_index("c")
    units = gate.shape[0]
    whole = pl.BlockSpec((1, 512), lambda z: (0, 0))
    piece = pl.BlockSpec((units, 1024), lambda z: (0, z))
    side = pl.BlockSpec((4, 3, PAD, 128), lambda z: (0, 0, 0, z))
    shape = jax.ShapeDtypeStruct((4, 3, PAD, 512), bf16)
    return pl.pallas_call(
        order_body,
        grid=(4,),
        in_specs=[
            whole,
            whole,
            pl.BlockSpec((1, 1, 1024), lambda z: (z, 0, 0)),
            piece,
            piece,
            piece,
        ],
        out_specs=[side, side, pl.BlockSpec((4, 128, 128), lambda z: (0, z, 0))],
        out_shape=[shape, shape, jax.ShapeDtypeStruct((4, 512, 128), f32)],
        scratch_shapes=[pltpu.VMEM((3 * PAD + 16, 1024), bf16), pltpu.VMEM((2, 1024, 512), bf16)],
        cost_estimate=pl.CostEstimate(flops=5 * 10**9, bytes_accessed=6 * 10**6, transcendentals=0),
        compiler_params=pltpu.CompilerParams(vmem_limit_bytes=20 * 2**20),
        name="order",
    )(sources(core), sources(1 - core), gain.reshape(4, 1, 1024), *(in_hbm(w) for w in (gate, up, down)))


def product_body(*refs, parts, starts, more):
    chunks = len(starts)
    pieces, refs = refs[: len(parts)], refs[len(parts) :]
    nears, fars, gains = refs[:chunks], refs[chunks : 2 * chunks], refs[2 * chunks : 3 * chunks]
    before, out, away, normed = refs[3 * chunks :] if more else (None, refs[-2], None, refs[-1])
    squares = 0.0
    for piece, (chunk, first) in zip(pieces, parts, strict=True):
        count, rows = piece.shape
        value = piece[...].astype(f32)
        squares = squares + jnp.sum(value * value, axis=0, keepdims=True)
        gain = gains[chunk][0, first : first + count, :]
        gain = jnp.concatenate([gain] * (rows // 128), axis=1)
        normed[512 * chunk + first : 512 * chunk + first + count, :] = (value * gain).astype(bf16)
    for side, weights in enumerate((nears, fars)):
        weights = jnp.concatenate([w[0].reshape(2 * PAD, 512) for w in weights], axis=1)
        total = jnp.dot(weights, normed[...], preferred_element_type=f32)
        where = slice(2 * PAD * side, 2 * PAD * (side + 1))
        if more:
            total = before[where, :] + total
            away[where, :] = total.astype(bf16)
        out[where, :] = total
    squares = jnp.broadcast_to(squares, (8, squares.shape[1]))
    where = slice(4 * PAD, 4 * PAD + 8)
    if more:
        squares = before[where, :] + squares
        high = squares.astype(bf16).astype(f32)
        away[4 * PAD :, :] = jnp.concatenate([high, squares - high], axis=0).astype(bf16)
    out[where, :] = squares


def products(pieces, chunks, near, far, gains, before=None):
    rows = pieces[0][0].shape[1]
    parts = tuple((chunks.index(k), first) for _, k, first in pieces)
    operands = [p for p, _, _ in pieces]
    specs = [pl.BlockSpec(p.shape, lambda i: (0, 0)) for p in operands]
    for weights in (near, far):
        for k in chunks:
            operands.append(weights)
            specs.append(pl.BlockSpec((1, 2, PAD, 512), lambda i, k=k: (k, 0, 0, 0)))
    for k in chunks:
        operands.append(gains)
        specs.append(pl.BlockSpec((1, 512, 128), lambda i, k=k: (k, 0, 0)))
    outs = [jax.ShapeDtypeStruct((4 * PAD + 8, rows), f32)]
    if before is not None:
        operands.append(before)
        specs.append(pl.BlockSpec(before.shape, lambda i: (0, 0)))
        outs.append(jax.ShapeDtypeStruct((4 * PAD + 16, rows), bf16))
    return pl.pallas_call(
        functools.partial(product_body, parts=parts, starts=chunks, more=before is not None),
        grid=(1,),
        in_specs=specs,
        out_specs=[pl.BlockSpec(o.shape, lambda i: (0, 0)) for o in outs],
        out_shape=outs,
        scratch_shapes=[pltpu.VMEM((512 * len(chunks), rows), bf16)],
        cost_estimate=pl.CostEstimate(
            flops=len(chunks) * 4 * 10**8, bytes_accessed=len(chunks) * 10**6, transcendentals=0
        ),
        compiler_params=pltpu.CompilerParams(vmem_limit_bytes=16 * 2**20),
        name="products",
    )(*operands)


def chunk_copies(source, target, sems, outward=False):
    copies = []
    for i in range(target.shape[0] // 8):
        rows = pl.ds(8 * i, 8)
        ends = (target.at[rows], source.at[rows]) if outward else (source.at[rows], target.at[rows])
        copies.append(pltpu.make_async_copy(*ends, sems.at[i]))
    return copies


def readout_body(*refs):
    arrived, refs = refs[:4], refs[4:]
    past, floor, gain, mixed, forget, value, query, gate, states, sems = refs
    copies = chunk_copies(past, states, sems)
    for copy in copies:
        copy.start()
    heads, width = past.shape[1:3]
    inner = heads * width
    total = arrived[0][...].astype(f32)
    for piece in arrived[1:]:
        total = total + piece[...].astype(f32)
    squares = total[:, 4 * inner : 4 * inner + 1] + total[:, 4 * inner + 64 : 4 * inner + 65]
    total = total[:, : 4 * inner] * lax.rsqrt(squares / D + epsilon)
    query[...] = jax.nn.silu(total[:, :inner])
    value[...] = total[:, 2 * inner : 3 * inner]
    gate[...] = jax.nn.silu(total[:, 3 * inner :])
    bound = floor[...]
    forget[...] = bound + (1.0 - bound) * jax.nn.sigmoid(total[:, inner : 2 * inner])
    for i, copy in enumerate(copies):
        copy.wait()
        here = slice(8 * i, 8 * (i + 1))
        for h in range(heads):
            lanes = slice(width * h, width * (h + 1))
            keep, ask = forget[here, lanes], query[here, lanes]
            both = keep * ask
            high = both.astype(bf16).astype(f32)
            both = jnp.concatenate([high, both - high], axis=0).astype(bf16)
            sums = []
            for j in range(8):
                state = states[8 * i + j, h]
                top = state.astype(bf16)
                low = (state - top.astype(f32)).astype(bf16)
                dots = jnp.dot(both, top, preferred_element_type=f32) + jnp.dot(
                    both, low, preferred_element_type=f32
                )
                sums.append(dots[j : j + 1] + dots[8 + j : 8 + j + 1])
            share = jnp.sum((1.0 - keep) * ask, axis=1, keepdims=True)
            r = jnp.concatenate(sums, axis=0) + share * value[here, lanes]
            r = r * lax.rsqrt(jnp.mean(r * r, axis=1, keepdims=True) + epsilon) * gain[...]
            query[here, lanes] = r * gate[here, lanes]
    mixed[...] = query[...].astype(bf16)


def read_out(arrived, past, floor, gain):
    count, heads, width, _ = past.shape
    inner = heads * width
    rows = pltpu.VMEM((count, inner), f32)
    table = pltpu.HBM((count, inner), f32)
    return pl.pallas_call(
        readout_body,
        in_specs=[
            *[pl.BlockSpec(piece.shape, lambda: (0, 0)) for piece in arrived],
            pl.BlockSpec(memory_space=pl.ANY),
            pl.BlockSpec((1, inner), lambda: (0, 0)),
            pl.BlockSpec((1, width), lambda: (0, 0)),
        ],
        out_shape=[jax.ShapeDtypeStruct((count, inner), bf16), table, table],
        scratch_shapes=[
            rows,
            rows,
            pltpu.VMEM(past.shape, f32),
            pltpu.SemaphoreType.DMA((count // 8,)),
        ],
        compiler_params=pltpu.CompilerParams(vmem_limit_bytes=14 * 2**20),
        name="readout",
    )(*arrived, in_hbm(past), floor.reshape(1, -1), gain.reshape(1, -1))


def state_body(forget, value, past, new, columns, states, arrivals, departures):
    copies = chunk_copies(past, states, arrivals)
    for copy in copies:
        copy.start()
    count, heads, width, _ = past.shape
    for h in range(heads):
        table = forget[:, width * h : width * (h + 1)]
        columns[h] = jnp.concatenate([table] * (width // count), axis=0).T
    leaving = chunk_copies(new, states, departures, outward=True)
    for i, copy in enumerate(copies):
        copy.wait()
        for h in range(heads):
            near = columns[h]
            for j in range(8 * i, 8 * (i + 1)):
                keep = jnp.broadcast_to(near[:, j : j + 1], (width, width))
                added = value[j : j + 1, width * h : width * (h + 1)]
                states[j, h] = added + keep * (states[j, h] - added)
        leaving[i].start()
    for copy in leaving:
        copy.wait()


def update_state(forget, value, past):
    count, heads, width, _ = past.shape
    whole = pl.BlockSpec(forget.shape, lambda: (0, 0))
    sems = pltpu.SemaphoreType.DMA((count // 8,))
    return pl.pallas_call(
        state_body,
        in_specs=[whole, whole, pl.BlockSpec(memory_space=pl.ANY)],
        out_specs=pl.BlockSpec(memory_space=pl.ANY),
        out_shape=jax.ShapeDtypeStruct(past.shape, f32),
        scratch_shapes=[
            pltpu.VMEM((heads, width, width), f32),
            pltpu.VMEM(past.shape, f32),
            sems,
            sems,
        ],
        compiler_params=pltpu.CompilerParams(vmem_limit_bytes=12 * 2**20),
        cost_estimate=pl.CostEstimate(
            flops=4 * 10**9, bytes_accessed=8 * 10**6, transcendentals=0
        ),
        name="state",
    )(in_hbm(forget), in_hbm(value), in_hbm(past))


def project_body(gain, *refs):
    pieces, weights, outs = refs[:4], refs[4:8], refs[8:12]
    block, rows_scratch, sums_scratch = refs[12:]
    x, core = lax.axis_index("x"), lax.axis_index("c")
    width, rows = pieces[0].shape[0] // 2, pieces[0].shape[1]
    for k, piece in enumerate(pieces):
        first = lax.rem(x + k, 4) * 2 * width
        for side in range(2):
            row = pl.multiple_of(first + lax.rem(core + side, 2) * width, width)
            block[pl.ds(row, width), :] = piece[width * side : width * (side + 1), :]
    value = block[...].astype(f32)
    normed = (value * jnp.concatenate([gain[...]] * (rows // 128), axis=1)).astype(bf16)
    rows_scratch[...] = normed.T
    squares = jnp.sum(value * value, axis=0, keepdims=True)
    high = squares.astype(bf16).astype(f32)
    line = lax.broadcasted_iota(jnp.int32, (128, rows), 0)
    sums_scratch[...] = jnp.where(line < 64, high, squares - high).astype(bf16).T
    own = outs[0].shape[1]
    z, y = lax.axis_index("z"), lax.axis_index("y")
    starts = []
    for k in range(4):
        for m in range(4):
            ahead = jnp.where(core == 0, k, m), jnp.where(core == 0, m, k)
            owner = lax.rem(z + ahead[0], 4) * 4 + lax.rem(y + ahead[1], 4)
            starts.append(pl.multiple_of(owner * own, own))
    normed = jnp.concatenate([rows_scratch[pl.ds(row, own), :] for row in starts], axis=0)
    for i, w in enumerate(weights):
        part = jnp.dot(normed, w[...], preferred_element_type=f32).astype(bf16)
        for k, out in enumerate(outs):
            here = part[4 * own * k : 4 * own * (k + 1)]
            out[:, :, 256 * i : 256 * (i + 1)] = here.reshape(4, own, 256)
    for k, out in enumerate(outs):
        for m in range(4):
            out[m, :, 1024:1152] = sums_scratch[pl.ds(starts[4 * k + m], own), :]


def project(pieces, gain, weights, own_rows):
    rows, width = pieces[0].shape[1], gain.shape[0]
    operands = [jnp.broadcast_to(gain[:, None], (width, 128)), *pieces, *weights]
    return pl.pallas_call(
        project_body,
        in_specs=[pl.BlockSpec(v.shape, lambda: (0, 0)) for v in operands],
        out_shape=[jax.ShapeDtypeStruct((4, own_rows, 4 * width + 128), bf16)] * 4,
        scratch_shapes=[
            pltpu.VMEM((width, rows), bf16),
            pltpu.VMEM((rows, width), bf16),
            pltpu.VMEM((rows, 128), bf16),
        ],
        compiler_params=pltpu.CompilerParams(vmem_limit_bytes=14 * 2**20),
        name="project",
    )(*operands)


def output_body(gathered, weight, mine, theirs, block):
    place = lax.axis_index("x"), lax.axis_index("c")
    width = mine.shape[1]
    block[...] = lax.dot_general(
        weight[...].T, gathered[...], (((1,), (1,)), ((), ())), preferred_element_type=f32
    )
    for k in range(4):
        first = lax.rem(place[0] + k, 4) * 2 * width
        for side, out in enumerate((mine, theirs)):
            row = pl.multiple_of(first + lax.rem(place[1] + side, 2) * width, width)
            out[k] = block[pl.ds(row, width), :].astype(bf16)


def project_out(gathered, weight):
    rows, width = gathered.shape[0], weight.shape[1]
    shape = jax.ShapeDtypeStruct((4, width // 8, rows), bf16)
    return pl.pallas_call(
        output_body,
        in_specs=[pl.BlockSpec(v.shape, lambda: (0, 0)) for v in (gathered, weight)],
        out_shape=[shape, shape],
        scratch_shapes=[pltpu.VMEM((width, rows), f32)],
        compiler_params=pltpu.CompilerParams(vmem_limit_bytes=10 * 2**20),
        name="output",
    )(gathered, weight)


def half_step(own, near_w, far_w, gains, near):
    width, rows = own.shape
    half = near.shape[0] // 2
    top, low = slice(0, half), slice(half, 2 * half)
    left_top = shift(near[top], 1)
    right_low = shift(near[low], -1)
    left_low = shift(near[low], 1)
    right_top = shift(near[top], -1)
    left_top, right_low, far_w = lax.optimization_barrier((left_top, right_low, far_w))
    far_top = shift(left_top, 1)
    far_low = shift(right_low, -1)
    early = [
        (near, 0, 0),
        (left_top, 3, 0),
        (right_low, 1, half),
        (left_low, 3, half),
        (right_top, 1, 0),
    ]
    (acc,) = products(early, [0, 3, 1], near_w, far_w, gains)
    late = [(far_top, 2, 0), (far_low, 2, half)]
    acc, away = products(late, [2], near_w, far_w, gains, acc)
    got = other_core(away).astype(f32)
    squares = acc[4 * PAD] + got[4 * PAD] + got[4 * PAD + 8]
    scale = lax.rsqrt(squares / D + epsilon)[None, :]
    own_acc = acc[: 2 * PAD] + got[2 * PAD : 4 * PAD]
    far_acc = acc[2 * PAD : 4 * PAD] + got[: 2 * PAD]
    hidden = jnp.concatenate(
        [
            (jax.nn.silu(scale * a[:PAD]) * (scale * a[PAD:])).astype(bf16)
            for a in (own_acc, far_acc)
        ],
        axis=0,
    )
    deep = jnp.concatenate([near_w[:, 2], far_w[:, 2]], axis=1)

    sums, arrived = {}, []
    for k in (1, 3, 2, 0):
        sums[k] = lax.dot_general(
            deep[k], hidden, (((0,), (0,)), ((), ())), preferred_element_type=f32
        ).astype(bf16)
        if k:
            arrived.append(shift(sums[k], k))
    total = sums[0].astype(f32)
    for piece in arrived:
        total = total + piece.astype(f32)
    total = total.astype(bf16)
    total = plane_exchange(total.reshape(16, width, rows)).astype(f32).sum(axis=0)
    return lax.optimization_barrier((own.astype(f32) + 0.5 * total).astype(bf16))


def plane_gather(own):
    return plane_exchange(jnp.broadcast_to(own, (16, *own.shape))).reshape(-1, own.shape[1])


def per_device(
    tokens,
    past_state,
    pre_gain,
    pre_gate,
    pre_up,
    pre_down,
    mix_gain,
    query_weight,
    forget_weight,
    value_weight,
    output_gate_weight,
    forget_floor,
    head_gain,
    proj_out,
    post_gain,
    post_gate,
    post_up,
    post_down,
):
    tokens = tokens.T
    near = plane_gather(tokens)
    near_w, far_w, gains = order_weights(pre_gain, pre_gate.T, pre_up.T, pre_down)
    near, near_w, far_w = lax.optimization_barrier((near, near_w, far_w))
    first = half_step(tokens, near_w, other_core(far_w), gains, near)

    width = mix_gain.shape[0] // lax.axis_size(KV)
    own_rows, _, _, _ = past_state.shape
    gains = lax.dynamic_slice_in_dim(mix_gain, lax.axis_index(KV) * width, width, 0)
    pair = jnp.concatenate([first, other_core(first)], axis=0)
    pieces = [pair] + [shift_x(pair, -k) for k in (1, 2, 3)]
    weight_list = (query_weight, forget_weight, value_weight, output_gate_weight)
    sent = project(pieces, gains, weight_list, own_rows)
    blocks = list(sent)
    blocks[0], post_gate, post_up, post_down = lax.optimization_barrier(
        (blocks[0], post_gate, post_up, post_down)
    )
    near_w, far_w, gains = order_weights(post_gain, post_gate.T, post_up.T, post_down)
    summed = blocks[0].astype(f32)
    passed = [shift_kv(blocks[k], k, 0) for k in (2, 1, 3)]
    passed, near_w = lax.optimization_barrier((passed, near_w))
    for piece in passed:
        summed = summed + piece.astype(f32)
    summed = summed.astype(bf16)
    arrived = [summed[0]] + [shift_kv(summed[m], m, 1) for m in (2, 1, 3)]
    mixed_in, forget, value = read_out(arrived, past_state, forget_floor, head_gain)
    gathered = copy_for_each(mixed_in, KV).reshape(-1, mixed_in.shape[1])
    mine, theirs = project_out(gathered, proj_out)
    mixed = (mine.astype(f32) + other_core(theirs).astype(f32)).astype(bf16)
    mixed_sum = mixed[0].astype(f32)
    for piece in [shift_x(mixed[k], k) for k in (2, 1, 3)]:
        mixed_sum = mixed_sum + piece.astype(f32)
    second = lax.optimization_barrier((first.astype(f32) + mixed_sum).astype(bf16))
    near = plane_gather(second)
    near, far_w = lax.optimization_barrier((near, far_w))
    far_w = other_core(far_w)
    new_state = update_state(forget, value, past_state)
    result = half_step(second, near_w, far_w, gains, near)
    return (result.T, new_state)


def solution(mesh):
    torus = Mesh(mesh.devices.reshape(4, 4, 4, 2), ALL)
    return jax.shard_map(
        per_device,
        mesh=torus,
        in_specs=(
            P(None, ALL),
            P(KV, TP, None, None),
            P(),
            P(None, ALL),
            P(None, ALL),
            P(ALL, None),
            P(),
            P(KV, TP),
            P(KV, TP),
            P(KV, TP),
            P(KV, TP),
            P(TP),
            P(),
            P(TP, KV),
            P(),
            P(None, ALL),
            P(None, ALL),
            P(ALL, None),
        ),
        out_specs=(P(None, ALL), P(KV, TP, None, None)),
        check_vma=False,
    )
```
